128 devices in a mesh: sp: 16 (over z, x), tp: 8 (over y, core).
Axes of the slice: x: 4, y: 4, z: 4, core: 2. Of those that a mesh axis runs over, the one named last changes fastest.
Arguments:
- queries: bfloat16 [8192, 3072], P('sp', 'tp'), may hold values from -6 to 6
- latent: bfloat16 [8192, 1024], P('sp'), may hold values from -6 to 6
- rope_key: bfloat16 [8192, 64], P('sp'), may hold values from -6 to 6
- key_weight: bfloat16 [1024, 2048], P(None, 'tp'), as said below
- value_weight: bfloat16 [1024, 2048], P(None, 'tp'), as said below
- log_sums: float32 [16, 8192], P('tp', 'sp'), as said below
- attn_out: bfloat16 [8192, 2048], P('sp', 'tp'), as said below
- out_grad: bfloat16 [8192, 2048], P('sp', 'tp'), may hold values from -6 to 6
Outputs:
- d_queries: bfloat16 [8192, 3072], P('sp', 'tp')
- d_latent: float32 [8192, 1024], P('sp')
- d_rope: float32 [8192, 64], P('sp')
- d_value_weight: float32 [1024, 2048], P('sp', 'tp')
The draws below stay inside these ranges and needn't reach their ends.
Inputs may be any that keep to these rules, and one draw needn't show every extreme that they name: `key_weight`: independent entries of order one multiplied by 1024^(-1/2). `value_weight`: independent entries of order one multiplied by 1024^(-1/2). log_sums[h, i] is the logarithm of the sum over j <= i of exp(scores[h, i, j]) of the forward pass. attn_out is the forward pass output: head h of row i is the sum over j <= i of exp(scores - log_sums) rounded to bfloat16, times head h of values row j, rounded to bfloat16.
All inputs are finite; a program needn't handle non-finite values.
Results may differ from the reference program's by a relative error of at most 0.018.
Values may be sent and summed in bfloat16 or wider, within the bound.
A program may use at most 192 MiB of HBM per device.

```python
import jax
import jax.numpy as jnp
from jax import lax

HEADS = 16
NOPE = 128
ROPE = 64
VDIM = 128
LATENT = 1024
TOKENS = 8192


def rough_normal(key, shape):
    return jnp.clip(jax.random.normal(key, shape, jnp.float32), -6.0, 6.0)


def base_inputs(key):
    queries = rough_normal(jax.random.fold_in(key, 101), (TOKENS, HEADS * (NOPE + ROPE)))
    latent = rough_normal(jax.random.fold_in(key, 102), (TOKENS, LATENT))
    rope_key = rough_normal(jax.random.fold_in(key, 103), (TOKENS, ROPE))
    key_weight = rough_normal(jax.random.fold_in(key, 104), (LATENT, HEADS * NOPE)) * LATENT ** (-0.5)
    value_weight = rough_normal(jax.random.fold_in(key, 105), (LATENT, HEADS * VDIM)) * LATENT ** (-0.5)
    return (queries.astype(jnp.bfloat16), latent.astype(jnp.bfloat16), rope_key.astype(jnp.bfloat16), key_weight.astype(jnp.bfloat16), value_weight.astype(jnp.bfloat16))


def forward_outputs(key):
    queries, latent, rope_key, key_weight, value_weight = base_inputs(key)
    head_width = NOPE + ROPE
    score_scale = head_width ** (-0.5)
    key_nope = jnp.dot(latent, key_weight, preferred_element_type=jnp.float32).astype(jnp.bfloat16)
    values = jnp.dot(latent, value_weight, preferred_element_type=jnp.float32).astype(jnp.bfloat16)
    query_heads = queries.reshape(TOKENS, HEADS, head_width).transpose(1, 0, 2)
    key_heads = key_nope.reshape(TOKENS, HEADS, NOPE).transpose(1, 0, 2)
    value_heads = values.reshape(TOKENS, HEADS, VDIM).transpose(1, 0, 2)
    positions = jnp.arange(TOKENS, dtype=jnp.int32)
    causal = positions[None, :] <= positions[:, None]

    def one_head(operands):
        query_h, key_h, value_h = operands
        scores = score_scale * (jnp.dot(query_h[:, :NOPE], key_h.T, preferred_element_type=jnp.float32) + jnp.dot(query_h[:, NOPE:], rope_key.T, preferred_element_type=jnp.float32))
        masked = jnp.where(causal, scores, -jnp.inf)
        log_sum = jax.nn.logsumexp(masked, axis=1)
        attn_probs = jnp.exp(masked - log_sum[:, None]).astype(jnp.bfloat16)
        return (log_sum, jnp.dot(attn_probs, value_h, preferred_element_type=jnp.float32).astype(jnp.bfloat16))
    log_sums, out_heads = lax.map(one_head, (query_heads, key_heads, value_heads))
    return (log_sums, out_heads.transpose(1, 0, 2).reshape(TOKENS, HEADS * VDIM))


def draw_queries(key, part):
    return base_inputs(key)[0]


def draw_latent(key, part):
    return base_inputs(key)[1]


def draw_rope_key(key, part):
    return base_inputs(key)[2]


def draw_key_weight(key, part):
    return base_inputs(key)[3]


def draw_value_weight(key, part):
    return base_inputs(key)[4]


def draw_log_sums(key, part):
    return forward_outputs(key)[0]


def draw_attn_out(key, part):
    return forward_outputs(key)[1]


def strengthened(result, key, source, target, shards_of, factor):
    owner, partner = [(jnp.arange(result.shape[dim]) // (result.shape[dim] // shards_of)).reshape([-1 if axis == dim else 1 for axis in range(result.ndim)]) for dim in (source, target)]
    chosen = jax.random.permutation(key, shards_of)[partner]
    strong = (owner == chosen) | (owner == (partner + shards_of // 2) % shards_of)
    return jnp.where(strong, factor * result, result)


def shard_levels(own_key, dims, pieces, low, top_value):
    loudness = 1.0
    for axis_at, blocks in pieces:
        steps = jax.random.uniform(jax.random.fold_in(jax.random.fold_in(own_key, 6), axis_at), (blocks,), jnp.float32, low / len(pieces), top_value / len(pieces))
        loudness = loudness * jnp.repeat(jnp.exp(steps), dims[axis_at] // blocks).reshape((-1,) + (1,) * (len(dims) - 1 - axis_at))
    return loudness


def noise_with(rng, extent, deviation, reach, split, heavy, kind=jnp.bfloat16):
    drawn = deviation * jax.random.normal(rng, extent, jnp.float32)
    if split:
        drawn = drawn * shard_levels(rng, extent, split, -0.22, 0.18)
    return jnp.clip(strengthened(drawn, jax.random.fold_in(rng, 3), *heavy), -reach, reach).astype(kind)


def setup_inputs(seed: int = 0) -> dict:
    keys = jax.random.split(jax.random.key(seed), 9)
    return {
        "queries": draw_queries(jax.random.fold_in(keys[8], 71), 0),
        "latent": draw_latent(jax.random.fold_in(keys[8], 71), 0),
        "rope_key": draw_rope_key(jax.random.fold_in(keys[8], 71), 0),
        "key_weight": draw_key_weight(jax.random.fold_in(keys[8], 71), 0),
        "value_weight": draw_value_weight(jax.random.fold_in(keys[8], 71), 0),
        "log_sums": draw_log_sums(jax.random.fold_in(keys[8], 71), 0),
        "attn_out": draw_attn_out(jax.random.fold_in(keys[8], 71), 0),
        "out_grad": noise_with(keys[7], (TOKENS, HEADS * VDIM), 1.0, 6.0, ((0, 16), (1, 8)), (0, 1, 16, 2.0)),
    }


def reference(queries, latent, rope_key, key_weight, value_weight, log_sums, attn_out, out_grad):
    tok_count = queries.shape[0]
    head_width = NOPE + ROPE
    score_scale = head_width ** -0.5
    key_nope = jnp.dot(latent, key_weight, preferred_element_type=jnp.float32).astype(jnp.bfloat16)
    values = jnp.dot(latent, value_weight, preferred_element_type=jnp.float32).astype(jnp.bfloat16)
    query_heads = queries.reshape(tok_count, HEADS, head_width).transpose(1, 0, 2)
    key_heads = key_nope.reshape(tok_count, HEADS, NOPE).transpose(1, 0, 2)
    value_heads = values.reshape(tok_count, HEADS, VDIM).transpose(1, 0, 2)
    grad_heads = out_grad.reshape(tok_count, HEADS, VDIM).transpose(1, 0, 2)
    out_heads = attn_out.reshape(tok_count, HEADS, VDIM).transpose(1, 0, 2)
    row_terms = jnp.sum(out_heads.astype(jnp.float32) * grad_heads.astype(jnp.float32), axis=-1)
    positions = jnp.arange(tok_count, dtype=jnp.int32)
    causal = positions[None, :] <= positions[:, None]

    def one_head(operands):
        query_h, key_h, value_h, grad_h, lse_h, delta_h = operands
        scores = score_scale * (jnp.dot(query_h[:, :NOPE], key_h.T, preferred_element_type=jnp.float32)
                                + jnp.dot(query_h[:, NOPE:], rope_key.T, preferred_element_type=jnp.float32))
        attn_probs = jnp.exp(jnp.where(causal, scores - lse_h[:, None], -1e30))
        probs_b = attn_probs.astype(jnp.bfloat16)
        value_grad = jnp.dot(probs_b.T, grad_h, preferred_element_type=jnp.float32)
        prob_grad = jnp.dot(grad_h, value_h.T, preferred_element_type=jnp.float32)
        score_grad = (attn_probs * (prob_grad - delta_h[:, None])).astype(jnp.bfloat16)
        query_grad = score_scale * jnp.concatenate(
            [jnp.dot(score_grad, key_h, preferred_element_type=jnp.float32),
             jnp.dot(score_grad, rope_key, preferred_element_type=jnp.float32)], axis=1)
        key_grad = score_scale * jnp.dot(score_grad.T, query_h[:, :NOPE], preferred_element_type=jnp.float32)
        rope_grad = score_scale * jnp.dot(score_grad.T, query_h[:, NOPE:], preferred_element_type=jnp.float32)
        return query_grad, key_grad, rope_grad, value_grad

    query_grad, key_grad, rope_grad, value_grad = lax.map(
        one_head, (query_heads, key_heads, value_heads, grad_heads, log_sums, row_terms))
    d_queries = query_grad.transpose(1, 0, 2).reshape(tok_count, HEADS * head_width).astype(jnp.bfloat16)
    key_grad_b = key_grad.transpose(1, 0, 2).reshape(tok_count, HEADS * NOPE).astype(jnp.bfloat16)
    value_grad_b = value_grad.transpose(1, 0, 2).reshape(tok_count, HEADS * VDIM).astype(jnp.bfloat16)
    d_latent = (jnp.dot(key_grad_b, key_weight.T, preferred_element_type=jnp.float32)
                + jnp.dot(value_grad_b, value_weight.T, preferred_element_type=jnp.float32))
    d_rope = jnp.sum(rope_grad, axis=0)
    d_value_weight = jnp.dot(latent.T, value_grad_b, preferred_element_type=jnp.float32)
    return (d_queries, d_latent, d_rope, d_value_weight)
```

```python
import jax
import jax.numpy as jnp
from jax import lax
from jax.experimental import pallas as pl
from jax.experimental.pallas import tpu as pltpu
from jax.sharding import PartitionSpec as P

NOPE = 128
ROPE = 64
HEAD = NOPE + ROPE
VDIM = 128
ROWS = 512
LATENT = 1024
WIDE = 1152
SCALE = HEAD**-0.5
LOG2E = 1.4426950408889634
BF16 = jnp.bfloat16
F32 = jnp.float32
MESH = pl.DeviceIdType.MESH
NT = (((1,), (1,)), ((), ()))

LSE_AT, GRAD_AT, DELTA_AT, PACK = 192, 208, 336, 352


def dot(a, b):
    return jnp.dot(a, b, preferred_element_type=F32)


def dot_nt(a, b):
    return lax.dot_general(a, b, NT, preferred_element_type=F32)


def in_three(row):
    high = row.astype(BF16).astype(F32)
    middle = (row - high).astype(BF16).astype(F32)
    low = row - high - middle
    at = lax.broadcasted_iota(jnp.int32, (16, row.shape[1]), 0)
    parts = jnp.where(at == 0, high, jnp.where(at == 1, middle, jnp.where(at == 2, low, 0.0)))
    return parts.astype(BF16)


def three_ones(width):
    at = lax.broadcasted_iota(jnp.int32, (ROWS, width), 1)
    return jnp.where(at < 3, 1.0, 0.0).astype(BF16)


def kernel(
    q, lat, rope, kw, vw, lse, ao, go,
    dq_out, dlat_out, drope_out, dw_out,
    qb, pk, kts, vs, kt, vv, kaug, vaug, dk, dv, dq, ps, dss,
    dqs, dqr, xs, rel, fin, dqh, dqf, gs, gf, kvb, latt,
    part, half, hr, ys, yr, ag, dws, dwr, dws2, dwr2,
    s_pk, s_kt, s_v, r_q, r_kt, r_v, s_fw, s_d, r_d, s_x, r_rel, r_fin, s_h, r_h, s_g, r_g,
    s_l, r_l, s_y, r_y, s_ag, s_agp, r_ag, s_w, r_w, s_w2, r_w2,
):
    sp, tp = lax.axis_index("sp"), lax.axis_index("tp")
    z, x, y, c = sp // 4, sp % 4, tp // 2, tp % 2
    core_of_z = ((z + 1) // 2) % 2
    slot_of_z = z // 2
    partner = (sp, 2 * y + 1 - c)

    def key_z(core, slot):
        return core + slot * (3 - 2 * core)

    def x_peer(j):
        return (4 * z + (x + j) % 4, tp)

    def z_peer(j):
        return (4 * ((z + j) % 4) + x, tp)

    def y_peer(j):
        return (sp, 2 * ((y + j) % 4) + c)

    def remote(src, dst, send, recv, to):
        return pltpu.make_async_remote_copy(
            src_ref=src, dst_ref=dst, send_sem=send, recv_sem=recv, device_id=to, device_id_type=MESH
        )

    def arrived(ref, recv):
        remote(ref, ref, s_l.at[0], recv, partner).wait_recv()

    barrier = pltpu.get_barrier_semaphore()
    peers = [partner]
    for j in (1, 2, 3):
        peers += [x_peer(j), y_peer(j)]
        peers += [(4 * ((z + j) % 4) + x, 2 * y + core) for core in (0, 1)]
    for peer in peers:
        pl.semaphore_signal(barrier, inc=1, device_id=peer, device_id_type=MESH)

    def to_head(e, src, dst, send, recv):
        head_z = 2 * c + e
        own = (head_z == z) & (core_of_z == c)
        copy = remote(src, dst, send, recv, (4 * head_z + x, 2 * y + core_of_z))
        return own, copy, pltpu.make_async_copy(src, dst, recv)

    def start_to_head(args):
        own, copy, local = to_head(*args)

        @pl.when(own)
        def _():
            local.start()

        @pl.when(jnp.logical_not(own))
        def _():
            copy.start()

    def sent_to_head(args):
        own, copy, _ = to_head(*args)

        @pl.when(jnp.logical_not(own))
        def _():
            copy.wait_send()

    qt = q[...].T
    got = go[...].T
    aot = ao[...].T
    first = []
    for e in (0, 1):
        grad = got[e * VDIM : (e + 1) * VDIM]
        delta = jnp.sum(
            grad.astype(F32) * aot[e * VDIM : (e + 1) * VDIM].astype(F32), axis=0, keepdims=True
        )
        pk[e, 0:LSE_AT] = qt[e * HEAD : (e + 1) * HEAD]
        pk[e, LSE_AT:GRAD_AT] = in_three(lse[e : e + 1, :] * (-1.0 / SCALE))
        pk[e, GRAD_AT:DELTA_AT] = grad
        pk[e, DELTA_AT:PACK] = in_three(-delta)
        args = (e, pk.at[e], qb.at[sp], s_pk.at[e], r_q.at[sp])
        if e == 0:
            pl.semaphore_wait(barrier, len(peers))
        start_to_head(args)
        first.append(args)

    keys = dot(lat[...], kw[...]).astype(BF16)
    for e in (0, 1):
        kts[e] = jnp.concatenate([keys[:, e * NOPE : (e + 1) * NOPE], rope[...]], axis=1).T
        args = (e, kts.at[e], kt.at[slot_of_z], s_kt.at[e], r_kt.at[slot_of_z])
        start_to_head(args)
        first.append(args)
    values = dot(lat[...], vw[...]).astype(BF16)
    for e in (0, 1):
        vs[e] = values[:, e * VDIM : (e + 1) * VDIM]
        args = (e, vs.at[e], vv.at[slot_of_z], s_v.at[e], r_v.at[slot_of_z])
        start_to_head(args)
        first.append(args)

    dk[...] = jnp.zeros_like(dk)
    dv[...] = jnp.zeros_like(dv)
    for s in (0, 1):
        kaug[s, :, HEAD:256] = three_ones(256 - HEAD)
        vaug[s, :, VDIM:256] = three_ones(256 - VDIM)

    def zero(b, _):
        dq[b] = jnp.zeros((HEAD, ROWS), F32)
        return 0

    lax.fori_loop(0, 16, zero, 0)

    def step(t):
        near = t < 4
        far = t >= 12
        mid = jnp.logical_not(near | far)
        pair = t % 2
        slot = jnp.where(mid, (t - 4) // 4, pair)
        other = jnp.where(near, t // 2, jnp.where(far, (t - 12) // 2, ((t - 4) // 2) % 2))
        dx = jnp.where(near, 0, jnp.where(far, 2, jnp.where(pair == 0, 3, 1)))
        core = jnp.where(other == 0, c, 1 - c)
        block = 4 * key_z(core, slot) + (x + dx) % 4
        return block, dx, other, slot

    def forwards(t):
        b, dx, other, slot = step(t)
        mine = other == 0
        plus = mine & ((dx == 0) | ((dx == 3) & (slot == 0)))
        minus = mine & ((dx == 0) | ((dx == 1) & (slot == 1)))
        return [
            (plus, remote(qb.at[b], qb.at[b], s_fw.at[0, b], r_q.at[b], x_peer(1))),
            (minus, remote(qb.at[b], qb.at[b], s_fw.at[1, b], r_q.at[b], x_peer(3))),
            (mine, remote(qb.at[b], qb.at[b], s_fw.at[2, b], r_q.at[b], partner)),
        ]

    def take(t):
        b = step(t)[0]
        arrived(qb.at[b], r_q.at[b])
        for holds, copy in forwards(t):

            @pl.when(holds)
            def _():
                copy.start()

    def tile(b, s, masked):
        raw = dot(kaug[s, :, 0:GRAD_AT], qb[b, 0:GRAD_AT]) * (SCALE * LOG2E)
        if masked:
            key_row = lax.broadcasted_iota(jnp.int32, (ROWS, ROWS), 0)
            query_row = lax.broadcasted_iota(jnp.int32, (ROWS, ROWS), 1)
            raw = jnp.where(key_row <= query_row, raw, -1e30)
        probs = jnp.exp2(raw)
        diff = dot(vaug[s, :, 0 : VDIM + 16], qb[b, GRAD_AT:PACK])
        grads = (probs * diff).astype(BF16)
        dv[s] += dot_nt(probs.astype(BF16), qb[b, GRAD_AT:DELTA_AT])
        dk[s] += dot_nt(grads, qb[b, 0:LSE_AT])
        dq[b] += dot(kt[s], grads)

    def to_partner(i, b):
        return remote(dqs.at[i], dqr.at[i], s_d.at[i], r_d.at[i], partner)

    def share_index(dx, slot):
        return 2 * dx + slot

    take(0)
    take(1)
    for s in (0, 1):
        arrived(kt.at[s], r_kt.at[s])
        arrived(vv.at[s], r_v.at[s])
        kaug[s, :, 0:HEAD] = kt[s].T
        vaug[s, :, 0:VDIM] = vv[s]
    own_block = [4 * key_z(c, s) + x for s in (0, 1)]

    def diagonal(s, _):
        tile(4 * key_z(c, s) + x, s, True)
        return 0

    lax.fori_loop(0, 2, diagonal, 0)
    tile(own_block[1], 0, False)

    def later(t, _):
        take(t)
        b, dx, other, slot = step(t)

        def pair(s, _):
            @pl.when(b > 4 * key_z(c, s) + x)
            def _():
                tile(b, s, False)

            return 0

        lax.fori_loop(0, 2, pair, 0)

        @pl.when(other == 1)
        def _():
            i = share_index(dx, slot)
            dqs[i] = dq[b].astype(BF16)
            to_partner(i, b).start()

        return 0

    lax.fori_loop(2, 16, later, 0)

    def to_owner(s, src, dst, send, recv):
        token_z = key_z(c, s)
        own = (token_z == z) & (z // 2 == c)
        copy = remote(src, dst, send, recv, (4 * token_z + x, 2 * y + z // 2))
        return own, copy, pltpu.make_async_copy(src, dst, recv)

    def start_to_owner(args):
        own, copy, local = to_owner(*args)

        @pl.when(own)
        def _():
            local.start()

        @pl.when(jnp.logical_not(own))
        def _():
            copy.start()

    def sent_to_owner(args):
        own, copy, _ = to_owner(*args)

        @pl.when(jnp.logical_not(own))
        def _():
            copy.wait_send()

    e_mine = z % 2
    back = []
    for s in (0, 1):
        gs[s, :, 0:NOPE] = (dk[s, :, 0:NOPE] * SCALE).astype(BF16)
        gs[s, :, NOPE : NOPE + VDIM] = dv[s].astype(BF16)
        rope_part = (dk[s, :, NOPE:HEAD] * SCALE).astype(BF16)
        gs[s, :, 256:384] = jnp.concatenate([rope_part, jnp.zeros((ROWS, ROPE), BF16)], axis=1)
        args = (s, gs.at[s], gf.at[e_mine], s_g.at[s], r_g.at[e_mine])
        start_to_owner(args)
        back.append(args)

    def add_share(dx, s):
        i = 2 * dx + s
        arrived(dqr.at[i], r_d.at[i])
        b = 4 * key_z(c, s) + (x + dx) % 4
        return dq[b] + dqr[i].astype(F32)

    returned = []

    def send_x(i, value, dst, recv, to):
        xs[i] = value.astype(BF16)
        copy = remote(xs.at[i], dst, s_x.at[i], recv, to)
        copy.start()
        returned.append(copy)

    send_x(0, add_share(2, 0), rel.at[0], r_rel.at[0], x_peer(3))
    send_x(1, add_share(2, 1), rel.at[1], r_rel.at[1], x_peer(1))
    send_x(2, add_share(3, 1), fin.at[1, 1], r_fin.at[1, 1], x_peer(3))
    send_x(3, add_share(1, 0), fin.at[0, 0], r_fin.at[0, 0], x_peer(1))
    via_minus, via_plus = add_share(3, 0), add_share(1, 1)
    arrived(rel.at[0], r_rel.at[0])
    send_x(4, via_minus + rel[0].astype(F32), fin.at[1, 0], r_fin.at[1, 0], x_peer(3))
    arrived(rel.at[1], r_rel.at[1])
    send_x(5, via_plus + rel[1].astype(F32), fin.at[0, 1], r_fin.at[0, 1], x_peer(1))

    latt[...] = lat[...].T

    for e in (0, 1):
        arrived(gf.at[e], r_g.at[e])
        kvb[:, e * NOPE : (e + 1) * NOPE] = gf[e, :, 0:NOPE]
        kvb[:, 256 + e * VDIM : 256 + (e + 1) * VDIM] = gf[e, :, NOPE : NOPE + VDIM]

    def latent_rows(first_row):
        rows = pl.ds(pl.multiple_of(first_row, 256), 256)
        grads = dot_nt(kvb[rows, 0:256], kw[...]) + dot_nt(kvb[rows, 256:512], vw[...])
        ropes = gf[0, rows, 256:384].astype(F32) + gf[1, rows, 256:384].astype(F32)
        return grads, ropes

    grads, ropes = latent_rows(256 * (1 - c))
    half[:, 0:LATENT] = grads.astype(BF16)
    half[:, LATENT:WIDE] = ropes.astype(BF16)
    to_half = remote(half, hr, s_l.at[0], r_l.at[0], partner)
    to_half.start()
    grads, ropes = latent_rows(256 * c)
    part[:, 0:LATENT] = grads
    part[:, LATENT:WIDE] = ropes
    arrived(hr, r_l.at[0])
    part[...] += hr[...].astype(F32)
    ys[...] = part[...].astype(BF16)
    sends = [to_half]
    for j in (2, 1, 3):
        yj = (y + j) % 4
        copy = remote(
            ys.at[pl.ds(pl.multiple_of(64 * yj, 64), 64)], yr.at[y], s_y.at[yj], r_y.at[y], y_peer(j)
        )
        copy.start()
        sends.append(copy)

    for b in range(16):
        dws[b % 4, b // 4] = dot(latt[64 * b : 64 * (b + 1)], kvb[:, 256:512]).astype(BF16)
    for j in (2, 1, 3):
        xj = (x + j) % 4
        copy = remote(dws.at[xj], dwr.at[x], s_w.at[xj], r_w.at[x], x_peer(j))
        copy.start()
        sends.append(copy)

    total = part[pl.ds(pl.multiple_of(64 * y, 64), 64)]
    for j in (1, 3, 2):
        yj = (y + j) % 4
        arrived(yr.at[yj], r_y.at[yj])
        total += yr[yj].astype(F32)
    ag[4 * c + y] = total.astype(BF16)
    for j in (2, 1, 3):
        copy = remote(ag.at[4 * c + y], ag.at[4 * c + y], s_ag.at[j], r_ag.at[4 * c + y], y_peer(j))
        copy.start()
        sends.append(copy)
    copy = remote(ag.at[4 * c + y], ag.at[4 * c + y], s_agp.at[0], r_ag.at[4 * c + y], partner)
    copy.start()
    sends.append(copy)

    for s in (0, 1):
        home = add_share(0, s)
        for side in (0, 1):
            arrived(fin.at[side, s], r_fin.at[side, s])
            home += fin[side, s].astype(F32)
        dqh[s] = (home * SCALE).astype(BF16)
        args = (s, dqh.at[s], dqf.at[e_mine], s_h.at[s], r_h.at[e_mine])
        start_to_owner(args)
        back.append(args)

    weight = dws[x].astype(F32)
    for j in (1, 3, 2):
        xj = (x + j) % 4
        arrived(dwr.at[xj], r_w.at[xj])
        weight += dwr[xj].astype(F32)
    dws2[...] = weight.astype(BF16)
    for j in (2, 1, 3):
        zj = (z + j) % 4
        copy = remote(dws2.at[zj], dwr2.at[z], s_w2.at[zj], r_w2.at[z], z_peer(j))
        copy.start()
        sends.append(copy)

    def latent_out(i):
        dlat_out[pl.ds(pl.multiple_of(64 * i, 64), 64), :] = ag[i, :, 0:LATENT].astype(F32)
        drope_out[pl.ds(pl.multiple_of(64 * i, 64), 64), :] = ag[i, :, LATENT : LATENT + ROPE].astype(F32)

    latent_out(4 * c + y)
    for j in (1, 3, 2):
        i = 4 * c + (y + j) % 4
        arrived(ag.at[i], r_ag.at[i])
        copy = remote(ag.at[i], ag.at[i], s_agp.at[j], r_ag.at[i], partner)
        copy.start()
        sends.append(copy)
        latent_out(i)

    weight = dws2[z].astype(F32)
    for j in (1, 3, 2):
        zj = (z + j) % 4
        arrived(dwr2.at[zj], r_w2.at[zj])
        weight += dwr2[zj].astype(F32)
    dw_out[...] = weight

    for e in (0, 1):
        arrived(dqf.at[e], r_h.at[e])
    dq_out[...] = jnp.concatenate([dqf[0], dqf[1]], axis=0).T

    for j in (0, 1, 3, 2):
        i = 4 * (1 - c) + (y + j) % 4
        arrived(ag.at[i], r_ag.at[i])
        latent_out(i)

    for args in first:
        sent_to_head(args)
    for args in back:
        sent_to_owner(args)
    for copy in returned + sends:
        copy.wait_send()

    def sent(t, _):
        for holds, copy in forwards(t):

            @pl.when(holds)
            def _():
                copy.wait_send()

        b, dx, other, slot = step(t)

        @pl.when(other == 1)
        def _():
            to_partner(share_index(dx, slot), b).wait_send()

        return 0

    lax.fori_loop(0, 16, sent, 0)


def per_device(q, lat, rope, kw, vw, lse, ao, go):
    vmem = pl.BlockSpec(memory_space=pltpu.VMEM)

    def buf(*shape, dtype=BF16):
        return pltpu.VMEM(shape, dtype)

    def sem(*shape):
        return pltpu.SemaphoreType.DMA(shape)

    scratch = [
        buf(16, PACK, ROWS), buf(2, PACK, ROWS), buf(2, HEAD, ROWS), buf(2, ROWS, VDIM),
        buf(2, HEAD, ROWS), buf(2, ROWS, VDIM), buf(2, ROWS, 256), buf(2, ROWS, 256),
        buf(2, ROWS, HEAD, dtype=F32), buf(2, ROWS, VDIM, dtype=F32), buf(16, HEAD, ROWS, dtype=F32),
        buf(16, 128), buf(16, 128),
        buf(8, HEAD, ROWS), buf(8, HEAD, ROWS), buf(6, HEAD, ROWS), buf(2, HEAD, ROWS), buf(2, 2, HEAD, ROWS),
        buf(2, HEAD, ROWS), buf(2, HEAD, ROWS), buf(2, ROWS, 384), buf(2, ROWS, 384), buf(ROWS, 512),
        buf(LATENT, ROWS),
        buf(256, WIDE, dtype=F32), buf(256, WIDE), buf(256, WIDE), buf(256, WIDE), buf(4, 64, WIDE), buf(8, 64, WIDE),
        buf(4, 4, 64, 256), buf(4, 4, 64, 256), buf(4, 64, 256), buf(4, 64, 256),
        sem(2), sem(2), sem(2), sem(16), sem(2), sem(2), sem(3, 16), sem(8), sem(8), sem(6), sem(2), sem(2, 2),
        sem(2), sem(2), sem(2), sem(2),
        sem(1), sem(1), sem(4), sem(4), sem(4), sem(4), sem(8), sem(4), sem(4), sem(4), sem(4),
    ]
    return pl.pallas_call(
        kernel,
        in_specs=[vmem] * 8,
        out_specs=[vmem] * 4,
        out_shape=[
            jax.ShapeDtypeStruct((ROWS, 2 * HEAD), BF16),
            jax.ShapeDtypeStruct((ROWS, LATENT), F32),
            jax.ShapeDtypeStruct((ROWS, ROPE), F32),
            jax.ShapeDtypeStruct((64, 256), F32),
        ],
        scratch_shapes=scratch,
        compiler_params=pltpu.CompilerParams(
            collective_id=0, has_side_effects=True, vmem_limit_bytes=60000 * 1024
        ),
        name="latent_attention_backward",
    )(q, lat, rope, kw, vw, lse, ao, go)


def solution(mesh):
    placed = (
        P("sp", "tp"),
        P("sp", None),
        P("sp", None),
        P(None, "tp"),
        P(None, "tp"),
        P("tp", "sp"),
        P("sp", "tp"),
        P("sp", "tp"),
    )
    return jax.shard_map(
        per_device,
        mesh=mesh,
        in_specs=placed,
        out_specs=(P("sp", "tp"), P("sp", None), P("sp", None), P("sp", "tp")),
        check_vma=False,
    )
```

```python
import jax
import jax.numpy as jnp
from jax import lax
from jax.experimental import pallas as pl
from jax.experimental.pallas import tpu as pltpu
from jax.sharding import PartitionSpec as P

NOPE = 128
ROPE = 64
HEAD = NOPE + ROPE
VDIM = 128
ROWS = 512
LATENT = 1024
WIDE = 1152
SCALE = HEAD**-0.5
LOG2E = 1.4426950408889634
BF16 = jnp.bfloat16
F32 = jnp.float32
MESH = pl.DeviceIdType.MESH
NT = (((1,), (1,)), ((), ()))

LSE_AT, GRAD_AT, PACK = 192, 208, 336
ONES_AT, VALUE_AT, KEY_PACK = 192, 224, 352


def dot(a, b):
    return jnp.dot(a, b, preferred_element_type=F32)


def dot_nt(a, b):
    return lax.dot_general(a, b, NT, preferred_element_type=F32)


def in_three(row):
    high = row.astype(BF16).astype(F32)
    middle = (row - high).astype(BF16).astype(F32)
    return high, middle, row - high - middle


def six_rows(first, second):
    at = lax.broadcasted_iota(jnp.int32, (16, first.shape[1]), 0)
    rows = jnp.zeros(at.shape, F32)
    for i, part in enumerate(in_three(first) + in_three(second)):
        rows = jnp.where(at == i, part, rows)
    return rows.astype(BF16)


def ones_rows(first):
    at = lax.broadcasted_iota(jnp.int32, (16, ROWS), 0)
    return jnp.where((at >= first) & (at < first + 3), 1.0, 0.0).astype(BF16)


def kernel(
    q_hbm, lat_hbm, rope_hbm, kw_hbm, vw_hbm, lse_hbm, ao_hbm, go_hbm,
    ag, dq_out, dw_out,
    q, lat, rope, kw, vw, lse, ao, go,
    qb, pk, kts, vts, kv, kaug, vaug, dk, dv, dq,
    dqs, dqr, xs, rel, fin, dqh, dqf, gs, gf, kvb, latt,
    part, half, hr, ys, yr, dws, dwr, dws2, dwr2,
    s_in, s_pk, s_kt, s_v, r_q, r_kt, r_v, s_fw, s_d, r_d, s_x, r_rel, r_fin, s_h, r_h, s_g, r_g,
    s_l, r_l, s_y, r_y, s_ag, s_agp, r_ag, s_w, r_w, s_w2, r_w2,
):
    sp, tp = lax.axis_index("sp"), lax.axis_index("tp")
    z, x, y, c = sp // 4, sp % 4, tp // 2, tp % 2
    core_of_z = ((z + 1) // 2) % 2
    slot_of_z = z // 2
    partner = (sp, 2 * y + 1 - c)

    def key_z(core, slot):
        return core + slot * (3 - 2 * core)

    def x_peer(j):
        return (4 * z + (x + j) % 4, tp)

    def z_peer(j):
        return (4 * ((z + j) % 4) + x, tp)

    def y_peer(j):
        return (sp, 2 * ((y + j) % 4) + c)

    def remote(src, dst, send, recv, to):
        return pltpu.make_async_remote_copy(
            src_ref=src, dst_ref=dst, send_sem=send, recv_sem=recv, device_id=to, device_id_type=MESH
        )

    def arrived(ref, recv, name="wait"):
        with jax.named_scope(name):
            remote(ref, ref, s_l.at[0], recv, partner).wait_recv()

    barrier = pltpu.get_barrier_semaphore()
    peers = [partner]
    for j in (1, 2, 3):
        peers += [x_peer(j), y_peer(j)]
        peers += [(4 * ((z + j) % 4) + x, 2 * y + core) for core in (0, 1)]
    for peer in peers:
        pl.semaphore_signal(barrier, inc=1, device_id=peer, device_id_type=MESH)

    pairs = [(q_hbm, q), (go_hbm, go), (ao_hbm, ao), (lse_hbm, lse), (lat_hbm, lat), (kw_hbm, kw), (vw_hbm, vw), (rope_hbm, rope)]
    loads = [pltpu.make_async_copy(src, dst, s_in.at[i]) for i, (src, dst) in enumerate(pairs)]
    for load in loads:
        load.start()

    dk[...] = jnp.zeros_like(dk)
    dv[...] = jnp.zeros_like(dv)
    for s in (0, 1):
        kv[s, ONES_AT : ONES_AT + 16] = ones_rows(0)
        kv[s, ONES_AT + 16 : VALUE_AT] = ones_rows(3)

    with jax.named_scope("inputs"):
        for load in loads:
            load.wait()
    with jax.named_scope("barrier"):
        pl.semaphore_wait(barrier, len(peers))

    def to_head(e, src, dst, send, recv):
        head_z = 2 * c + e
        own = (head_z == z) & (core_of_z == c)
        copy = remote(src, dst, send, recv, (4 * head_z + x, 2 * y + core_of_z))
        return own, copy, pltpu.make_async_copy(src, dst, recv)

    def start_to_head(args):
        own, copy, local = to_head(*args)

        @pl.when(own)
        def _():
            local.start()

        @pl.when(jnp.logical_not(own))
        def _():
            copy.start()

    def sent_to_head(args):
        own, copy, _ = to_head(*args)

        @pl.when(jnp.logical_not(own))
        def _():
            copy.wait_send()

    pack_args = [(e, pk.at[e], qb.at[sp], s_pk.at[e], r_q.at[sp]) for e in (0, 1)]
    key_args = [
        (e, kts.at[e], kv.at[slot_of_z, pl.ds(0, HEAD)], s_kt.at[e], r_kt.at[slot_of_z]) for e in (0, 1)
    ]
    value_args = [
        (e, vts.at[e], kv.at[slot_of_z, pl.ds(VALUE_AT, VDIM)], s_v.at[e], r_v.at[slot_of_z]) for e in (0, 1)
    ]

    def send_queries():
        qt = q[...].T
        got = go[...].T
        aot = ao[...].T
        for e in (0, 1):
            grad = got[e * VDIM : (e + 1) * VDIM]
            delta = jnp.sum(
                grad.astype(F32) * aot[e * VDIM : (e + 1) * VDIM].astype(F32), axis=0, keepdims=True
            )
            pk[e, 0:LSE_AT] = qt[e * HEAD : (e + 1) * HEAD]
            pk[e, LSE_AT:GRAD_AT] = six_rows(lse[e : e + 1, :] * (-1.0 / SCALE), -delta)
            pk[e, GRAD_AT:PACK] = grad
            start_to_head(pack_args[e])

    def send_keys():
        keys = dot(lat[...], kw[...]).astype(BF16).T
        for e in (0, 1):
            kts[e, 0:NOPE] = keys[e * NOPE : (e + 1) * NOPE]
            kts[e, NOPE:HEAD] = rope[...]
            start_to_head(key_args[e])
        values = dot(lat[...], vw[...]).astype(BF16).T
        for e in (0, 1):
            vts[e] = values[e * VDIM : (e + 1) * VDIM]
            start_to_head(value_args[e])

    @pl.when(z < 2)
    def _():
        send_keys()
        send_queries()

    @pl.when(z >= 2)
    def _():
        send_queries()
        send_keys()

    def zero(b, _):
        dq[b] = jnp.zeros((HEAD, ROWS), F32)
        return 0

    lax.fori_loop(0, 16, zero, 0)

    def step(t):
        near = t < 4
        far = t >= 12
        mid = jnp.logical_not(near | far)
        pair = t % 2
        slot = 1 - jnp.where(mid, (t - 4) // 4, (t % 4) // 2)
        other = jnp.where(mid, ((t - 4) // 2) % 2, pair)
        dx = jnp.where(near, 0, jnp.where(far, 2, jnp.where(pair == 0, 3, 1)))
        core = jnp.where(other == 0, c, 1 - c)
        block = 4 * key_z(core, slot) + (x + dx) % 4
        return block, dx, other, slot

    def forwards(t):
        b, dx, other, slot = step(t)
        mine = other == 0
        plus = mine & ((dx == 0) | ((dx == 3) & (slot == 0)))
        minus = mine & ((dx == 0) | ((dx == 1) & (slot == 1)))
        return [
            (plus, remote(qb.at[b], qb.at[b], s_fw.at[0, b], r_q.at[b], x_peer(1))),
            (minus, remote(qb.at[b], qb.at[b], s_fw.at[1, b], r_q.at[b], x_peer(3))),
            (mine, remote(qb.at[b], qb.at[b], s_fw.at[2, b], r_q.at[b], partner)),
        ]

    def take(t):
        b = step(t)[0]
        arrived(qb.at[b], r_q.at[b], "wait_query")
        for holds, copy in forwards(t):

            @pl.when(holds)
            def _():
                copy.start()

    def tile(b, s, masked):
        raw = dot(kaug[s], qb[b, 0:GRAD_AT]) * (SCALE * LOG2E)
        if masked:
            key_row = lax.broadcasted_iota(jnp.int32, (ROWS, ROWS), 0)
            query_row = lax.broadcasted_iota(jnp.int32, (ROWS, ROWS), 1)
            raw = jnp.where(key_row <= query_row, raw, -1e30)
        probs = jnp.exp2(raw)
        diff = dot(vaug[s], qb[b, LSE_AT:PACK])
        grads = (probs * diff).astype(BF16)
        dv[s] += dot_nt(probs.astype(BF16), qb[b, GRAD_AT:PACK])
        dk[s] += dot_nt(grads, qb[b, 0:LSE_AT])
        dq[b] += dot(kv[s, 0:HEAD], grads)

    def to_partner(i):
        return remote(dqs.at[i], dqr.at[i], s_d.at[i], r_d.at[i], partner)

    def share(t):
        b, dx, other, slot = step(t)

        @pl.when(other == 1)
        def _():
            i = 2 * dx + slot
            dqs[i] = dq[b].astype(BF16)
            to_partner(i).start()

    def own_block(s):
        return 4 * key_z(c, s) + x

    def take_keys(s):
        arrived(kv.at[s, pl.ds(0, HEAD)], r_kt.at[s], "wait_keys")
        arrived(kv.at[s, pl.ds(VALUE_AT, VDIM)], r_v.at[s], "wait_values")
        kaug[s] = kv[s, 0:GRAD_AT].T
        vaug[s] = kv[s, GRAD_AT:KEY_PACK].T

    def tiles(t):
        b = step(t)[0]

        def pair(s, _):
            @pl.when(b > own_block(s))
            def _():
                tile(b, s, False)

            return 0

        with jax.named_scope("pair"):
            lax.fori_loop(0, 2, pair, 0)

    def early(t, _):
        take(t)
        with jax.named_scope("early"):
            tile(step(t)[0], 0, False)
        return 0

    def diagonal(s, _):
        tile(own_block(s), s, True)
        return 0

    def later(t, _):
        take(t)
        tiles(t)
        share(t)
        return 0

    take_keys(0)
    lax.fori_loop(0, 2, early, 0)
    take(2)
    take_keys(1)
    with jax.named_scope("diagonal"):
        lax.fori_loop(0, 2, diagonal, 0)

    @pl.when(step(1)[0] > own_block(1))
    def _():
        tile(step(1)[0], 1, False)

    share(1)
    lax.fori_loop(3, 16, later, 0)

    def to_owner(s, src, dst, send, recv):
        token_z = key_z(c, s)
        own = (token_z == z) & (z // 2 == c)
        copy = remote(src, dst, send, recv, (4 * token_z + x, 2 * y + z // 2))
        return own, copy, pltpu.make_async_copy(src, dst, recv)

    def start_to_owner(args):
        own, copy, local = to_owner(*args)

        @pl.when(own)
        def _():
            local.start()

        @pl.when(jnp.logical_not(own))
        def _():
            copy.start()

    def sent_to_owner(args):
        own, copy, _ = to_owner(*args)

        @pl.when(jnp.logical_not(own))
        def _():
            copy.wait_send()

    e_mine = z % 2
    back = []
    for s in (0, 1):
        gs[s, 0:ROWS] = (dk[s, :, 0:NOPE] * SCALE).astype(BF16)
        gs[s, ROWS : 2 * ROWS] = dv[s].astype(BF16)
        rope_part = (dk[s, :, NOPE:HEAD] * SCALE).astype(BF16)
        gs[s, 2 * ROWS : 2 * ROWS + 256] = jnp.concatenate([rope_part[0:256], rope_part[256:512]], axis=1)
        args = (s, gs.at[s], gf.at[e_mine], s_g.at[s], r_g.at[e_mine])
        start_to_owner(args)
        back.append(args)

    def add_share(dx, s):
        i = 2 * dx + s
        arrived(dqr.at[i], r_d.at[i], "wait_share")
        b = 4 * key_z(c, s) + (x + dx) % 4
        return dq[b] + dqr[i].astype(F32)

    returned = []

    def send_x(i, value, dst, recv, to):
        xs[i] = value.astype(BF16)
        copy = remote(xs.at[i], dst, s_x.at[i], recv, to)
        copy.start()
        returned.append(copy)

    send_x(0, add_share(2, 0), rel.at[0], r_rel.at[0], x_peer(3))
    send_x(1, add_share(2, 1), rel.at[1], r_rel.at[1], x_peer(1))
    send_x(2, add_share(3, 1), fin.at[1, 1], r_fin.at[1, 1], x_peer(3))
    send_x(3, add_share(1, 0), fin.at[0, 0], r_fin.at[0, 0], x_peer(1))

    def relay_queries():
        via_minus, via_plus = add_share(3, 0), add_share(1, 1)
        arrived(rel.at[0], r_rel.at[0], "wait_relay")
        send_x(4, via_minus + rel[0].astype(F32), fin.at[1, 0], r_fin.at[1, 0], x_peer(3))
        arrived(rel.at[1], r_rel.at[1], "wait_relay")
        send_x(5, via_plus + rel[1].astype(F32), fin.at[0, 1], r_fin.at[0, 1], x_peer(1))

    latt[...] = lat[...].T

    for e in (0, 1):
        arrived(gf.at[e], r_g.at[e], "wait_grads")
        kvb[:, e * NOPE : (e + 1) * NOPE] = gf[e, 0:ROWS]
        kvb[:, 256 + e * VDIM : 256 + (e + 1) * VDIM] = gf[e, ROWS : 2 * ROWS]

    both_ropes = gf[0, 2 * ROWS : 2 * ROWS + 256].astype(F32) + gf[1, 2 * ROWS : 2 * ROWS + 256].astype(F32)

    def latent_rows(which):
        rows = pl.ds(pl.multiple_of(256 * which, 256), 256)
        grads = dot_nt(kvb[rows, 0:256], kw[...]) + dot_nt(kvb[rows, 256:512], vw[...])
        ropes = jnp.where(which == 0, both_ropes[:, 0:ROPE], both_ropes[:, ROPE : 2 * ROPE])
        return grads, jnp.concatenate([ropes, jnp.zeros_like(ropes)], axis=1)

    grads, ropes = latent_rows(1 - c)
    half[:, 0:LATENT] = grads.astype(BF16)
    half[:, LATENT:WIDE] = ropes.astype(BF16)
    to_half = remote(half, hr, s_l.at[0], r_l.at[0], partner)
    to_half.start()
    grads, ropes = latent_rows(c)
    part[:, 0:LATENT] = grads
    part[:, LATENT:WIDE] = ropes
    arrived(hr, r_l.at[0], "wait_half")
    part[...] += hr[...].astype(F32)
    ys[...] = part[...].astype(BF16)
    sends = [to_half]
    for j in (2, 1, 3):
        yj = (y + j) % 4
        copy = remote(
            ys.at[pl.ds(pl.multiple_of(64 * yj, 64), 64)], yr.at[y], s_y.at[yj], r_y.at[y], y_peer(j)
        )
        copy.start()
        sends.append(copy)

    relay_queries()
    for b in range(16):
        dws[b % 4, b // 4] = dot(latt[64 * b : 64 * (b + 1)], kvb[:, 256:512]).astype(BF16)
    for j in (2, 1, 3):
        xj = (x + j) % 4
        copy = remote(dws.at[xj], dwr.at[x], s_w.at[xj], r_w.at[x], x_peer(j))
        copy.start()
        sends.append(copy)

    total = part[pl.ds(pl.multiple_of(64 * y, 64), 64)]
    for j in (1, 3, 2):
        yj = (y + j) % 4
        arrived(yr.at[yj], r_y.at[yj], "wait_sum")
        total += yr[yj].astype(F32)
    ag[4 * c + y] = total.astype(BF16)
    for j in (2, 1, 3):
        copy = remote(ag.at[4 * c + y], ag.at[4 * c + y], s_ag.at[j], r_ag.at[4 * c + y], y_peer(j))
        copy.start()
        sends.append(copy)
    copy = remote(ag.at[4 * c + y], ag.at[4 * c + y], s_agp.at[0], r_ag.at[4 * c + y], partner)
    copy.start()
    sends.append(copy)

    for s in (0, 1):
        home = add_share(0, s)
        for side in (0, 1):
            arrived(fin.at[side, s], r_fin.at[side, s], "wait_home")
            home += fin[side, s].astype(F32)
        dqh[s] = (home * SCALE).astype(BF16)
        args = (s, dqh.at[s], dqf.at[e_mine], s_h.at[s], r_h.at[e_mine])
        start_to_owner(args)
        back.append(args)

    weight = dws[x].astype(F32)
    for j in (1, 3, 2):
        xj = (x + j) % 4
        arrived(dwr.at[xj], r_w.at[xj], "wait_weight")
        weight += dwr[xj].astype(F32)
    dws2[...] = weight.astype(BF16)
    for j in (2, 1, 3):
        zj = (z + j) % 4
        copy = remote(dws2.at[zj], dwr2.at[z], s_w2.at[zj], r_w2.at[z], z_peer(j))
        copy.start()
        sends.append(copy)

    for j in (1, 3, 2):
        i = 4 * c + (y + j) % 4
        arrived(ag.at[i], r_ag.at[i], "wait_chunk")
        copy = remote(ag.at[i], ag.at[i], s_agp.at[j], r_ag.at[i], partner)
        copy.start()
        sends.append(copy)

    weight = dws2[z].astype(F32)
    for j in (1, 3, 2):
        zj = (z + j) % 4
        arrived(dwr2.at[zj], r_w2.at[zj], "wait_weight")
        weight += dwr2[zj].astype(F32)
    dw_out[...] = weight

    for e in (0, 1):
        arrived(dqf.at[e], r_h.at[e], "wait_queries")
    dq_out[...] = jnp.concatenate([dqf[0], dqf[1]], axis=0).T

    for j in (0, 1, 3, 2):
        i = 4 * (1 - c) + (y + j) % 4
        arrived(ag.at[i], r_ag.at[i], "wait_other_chunk")

    for args in pack_args + key_args + value_args:
        sent_to_head(args)
    for args in back:
        sent_to_owner(args)
    for copy in returned + sends:
        copy.wait_send()

    def sent(t, _):
        for holds, copy in forwards(t):

            @pl.when(holds)
            def _():
                copy.wait_send()

        b, dx, other, slot = step(t)

        @pl.when(other == 1)
        def _():
            to_partner(2 * dx + slot).wait_send()

        return 0

    lax.fori_loop(0, 16, sent, 0)


def finish(ag, dq, dw, dlat_out, drope_out, dq_out, dw_out):
    for i in range(8):
        rows = slice(64 * i, 64 * (i + 1))
        dlat_out[rows] = ag[i, :, 0:LATENT].astype(F32)
    ropes = jnp.concatenate([ag[i, :, LATENT:WIDE] for i in range(8)], axis=0).T
    drope_out[...] = ropes[0:ROPE].astype(F32)
    dq_out[...] = dq[...]
    dw_out[...] = dw[...]


def per_device(q, lat, rope, kw, vw, lse, ao, go):
    vmem = pl.BlockSpec(memory_space=pltpu.VMEM)
    anywhere = pl.BlockSpec(memory_space=pl.ANY)

    def buf(*shape, dtype=BF16):
        return pltpu.VMEM(shape, dtype)

    def sem(*shape):
        return pltpu.SemaphoreType.DMA(shape)

    scratch = [
        buf(ROWS, 2 * HEAD), buf(ROWS, LATENT), buf(ROPE, ROWS), buf(LATENT, 256), buf(LATENT, 256),
        buf(2, ROWS, dtype=F32), buf(ROWS, 256), buf(ROWS, 256),
        buf(16, PACK, ROWS), buf(2, PACK, ROWS), buf(2, HEAD, ROWS), buf(2, VDIM, ROWS),
        buf(2, KEY_PACK, ROWS), buf(2, ROWS, GRAD_AT), buf(2, ROWS, KEY_PACK - GRAD_AT),
        buf(2, ROWS, HEAD, dtype=F32), buf(2, ROWS, VDIM, dtype=F32), buf(16, HEAD, ROWS, dtype=F32),
        buf(8, HEAD, ROWS), buf(8, HEAD, ROWS), buf(6, HEAD, ROWS), buf(2, HEAD, ROWS), buf(2, 2, HEAD, ROWS),
        buf(2, HEAD, ROWS), buf(2, HEAD, ROWS), buf(2, 1280, 128), buf(2, 1280, 128), buf(ROWS, 512),
        buf(LATENT, ROWS),
        buf(256, WIDE, dtype=F32), buf(256, WIDE), buf(256, WIDE), buf(256, WIDE), buf(4, 64, WIDE),
        buf(4, 4, 64, 256), buf(4, 4, 64, 256), buf(4, 64, 256), buf(4, 64, 256),
        sem(8), sem(2), sem(2), sem(2), sem(16), sem(2), sem(2), sem(3, 16), sem(8), sem(8), sem(6), sem(2), sem(2, 2),
        sem(2), sem(2), sem(2), sem(2),
        sem(1), sem(1), sem(4), sem(4), sem(4), sem(4), sem(8), sem(4), sem(4), sem(4), sem(4),
    ]
    ag, dq, dw = pl.pallas_call(
        kernel,
        in_specs=[anywhere] * 8,
        out_specs=[vmem] * 3,
        out_shape=[
            jax.ShapeDtypeStruct((8, 64, WIDE), BF16),
            jax.ShapeDtypeStruct((ROWS, 2 * HEAD), BF16),
            jax.ShapeDtypeStruct((64, 256), F32),
        ],
        scratch_shapes=scratch,
        compiler_params=pltpu.CompilerParams(
            collective_id=0, has_side_effects=True, vmem_limit_bytes=58000 * 1024
        ),
        name="latent_attention_backward",
    )(q, lat, rope.T, kw, vw, lse, ao, go)
    dlat, drope, dq, dw = pl.pallas_call(
        finish,
        in_specs=[vmem] * 3,
        out_specs=[vmem] * 4,
        out_shape=[
            jax.ShapeDtypeStruct((ROWS, LATENT), F32),
            jax.ShapeDtypeStruct((ROPE, ROWS), F32),
            jax.ShapeDtypeStruct((ROWS, 2 * HEAD), BF16),
            jax.ShapeDtypeStruct((64, 256), F32),
        ],
        name="finish",
    )(ag, dq, dw)
    return dq, dlat, drope.T, dw


def solution(mesh):
    placed = (
        P("sp", "tp"),
        P("sp", None),
        P("sp", None),
        P(None, "tp"),
        P(None, "tp"),
        P("tp", "sp"),
        P("sp", "tp"),
        P("sp", "tp"),
    )
    return jax.shard_map(
        per_device,
        mesh=mesh,
        in_specs=placed,
        out_specs=(P("sp", "tp"), P("sp", None), P("sp", None), P("sp", "tp")),
        check_vma=False,
    )
```

```python
import jax
import jax.numpy as jnp
from jax import lax
from jax.experimental import pallas as pl
from jax.experimental.pallas import tpu as pltpu
from jax.sharding import PartitionSpec as P

NOPE = 128
ROPE = 64
HEAD = NOPE + ROPE
VDIM = 128
ROWS = 512
LATENT = 1024
CHUNK = 64
PIECE = 160
DONE = 544
HALF = 256
SCALE = HEAD**-0.5
LOG2E = 1.4426950408889634
BF16 = jnp.bfloat16
F32 = jnp.float32
MESH = pl.DeviceIdType.MESH
NT = (((1,), (1,)), ((), ()))

LSE_AT, GRAD_AT, PACK = 192, 208, 336
ONES_AT, VALUE_AT, KEY_PACK = 192, 224, 352


def dot(a, b):
    return jnp.dot(a, b, preferred_element_type=F32)


def dot_nt(a, b):
    return lax.dot_general(a, b, NT, preferred_element_type=F32)


def in_three(row):
    high = row.astype(BF16).astype(F32)
    middle = (row - high).astype(BF16).astype(F32)
    return high, middle, row - high - middle


def six_rows(first, second):
    at = lax.broadcasted_iota(jnp.int32, (16, first.shape[1]), 0)
    rows = jnp.zeros(at.shape, F32)
    for i, part in enumerate(in_three(first) + in_three(second)):
        rows = jnp.where(at == i, part, rows)
    return rows.astype(BF16)


def ones_rows(first):
    at = lax.broadcasted_iota(jnp.int32, (16, ROWS), 0)
    return jnp.where((at >= first) & (at < first + 3), 1.0, 0.0).astype(BF16)


def kernel(
    q_hbm, lat_hbm, rope_hbm, kw_hbm, vw_hbm, lse_hbm, ao_hbm, go_hbm,
    ag_out, dq_out, dw_out,
    q, lat, rope, kw, vw, lse, ao, go,
    qb, pk, kts, vts, kv, kaug, vaug, dk, dv, dq,
    dqs, dqr, xs, rel, fin, dqh, dqf, gs, gf, lt, wt,
    dwh, dwhr, dwx, dwxr, dwz, dwf, ag, dqo, dwo,
    s_in, s_pk, s_kt, s_v, r_q, r_kt, r_v, s_fw, s_d, r_d, s_x, r_rel, r_fin, s_h, r_h, s_g, r_g,
    s_lt, r_lt, s_wt, r_wt, s_ag, r_ag, s_wh, r_wh, s_wx, r_wx, s_wz, r_wz, s_out,
):
    sp, tp = lax.axis_index("sp"), lax.axis_index("tp")
    z, x, y, c = sp // 4, sp % 4, tp // 2, tp % 2
    core_of_z = ((z + 1) // 2) % 2
    slot_of_z = z // 2
    partner = (sp, 2 * y + 1 - c)

    def key_z(core, slot):
        return core + slot * (3 - 2 * core)

    def x_peer(j):
        return (4 * z + (x + j) % 4, tp)

    def z_peer(j):
        return (4 * ((z + j) % 4) + x, tp)

    def y_peer(j):
        return (sp, 2 * ((y + j) % 4) + c)

    def remote(src, dst, send, recv, to):
        return pltpu.make_async_remote_copy(
            src_ref=src, dst_ref=dst, send_sem=send, recv_sem=recv, device_id=to, device_id_type=MESH
        )

    def arrived(ref, recv, name="wait"):
        with jax.named_scope(name):
            remote(ref, ref, s_in.at[0], recv, partner).wait_recv()

    def left(ref, send):
        remote(ref, ref, send, s_in.at[0], partner).wait_send()

    barrier = pltpu.get_barrier_semaphore()
    peers = [partner]
    for j in (1, 2, 3):
        peers += [x_peer(j)]
        peers += [(sp, 2 * ((y + j) % 4) + core) for core in (0, 1)]
        peers += [(4 * ((z + j) % 4) + x, 2 * y + core) for core in (0, 1)]
    for peer in peers:
        pl.semaphore_signal(barrier, inc=1, device_id=peer, device_id_type=MESH)

    pairs = [(q_hbm, q), (go_hbm, go), (ao_hbm, ao), (lse_hbm, lse), (lat_hbm, lat), (kw_hbm, kw), (vw_hbm, vw), (rope_hbm, rope)]
    loads = [pltpu.make_async_copy(src, dst, s_in.at[i]) for i, (src, dst) in enumerate(pairs)]
    for load in loads:
        load.start()

    dk[...] = jnp.zeros_like(dk)
    dv[...] = jnp.zeros_like(dv)
    for s in (0, 1):
        kv[s, ONES_AT : ONES_AT + 16] = ones_rows(0)
        kv[s, ONES_AT + 16 : VALUE_AT] = ones_rows(3)

    with jax.named_scope("inputs"):
        for load in loads:
            load.wait()
    with jax.named_scope("barrier"):
        pl.semaphore_wait(barrier, len(peers))

    def to_head(e, src, dst, send, recv):
        head_z = 2 * c + e
        own = (head_z == z) & (core_of_z == c)
        copy = remote(src, dst, send, recv, (4 * head_z + x, 2 * y + core_of_z))
        return own, copy, pltpu.make_async_copy(src, dst, recv)

    def start_to_head(args):
        own, copy, local = to_head(*args)

        @pl.when(own)
        def _():
            local.start()

        @pl.when(jnp.logical_not(own))
        def _():
            copy.start()

    def sent_to_head(args):
        own, copy, _ = to_head(*args)

        @pl.when(jnp.logical_not(own))
        def _():
            copy.wait_send()

    def half(ref, b, h):
        return ref.at[b, :, pl.ds(HALF * h, HALF)]

    pack_args = [
        (e, half(pk, e, h), half(qb, sp, h), s_pk.at[e, h], r_q.at[sp, h]) for h in (0, 1) for e in (0, 1)
    ]
    key_args = [
        (e, kts.at[e], kv.at[slot_of_z, pl.ds(0, HEAD)], s_kt.at[e], r_kt.at[slot_of_z]) for e in (0, 1)
    ]
    value_args = [
        (e, vts.at[e], kv.at[slot_of_z, pl.ds(VALUE_AT, VDIM)], s_v.at[e], r_v.at[slot_of_z]) for e in (0, 1)
    ]

    latent_args = [(e, lat, lt.at[slot_of_z], s_lt.at[e], r_lt.at[slot_of_z]) for e in (0, 1)]

    def send_queries():
        qt = q[...].T
        got = go[...].T
        aot = ao[...].T
        for e in (0, 1):
            grad = got[e * VDIM : (e + 1) * VDIM]
            delta = jnp.sum(
                grad.astype(F32) * aot[e * VDIM : (e + 1) * VDIM].astype(F32), axis=0, keepdims=True
            )
            pk[e, 0:LSE_AT] = qt[e * HEAD : (e + 1) * HEAD]
            pk[e, LSE_AT:GRAD_AT] = six_rows(lse[e : e + 1, :] * (-1.0 / SCALE), -delta)
            pk[e, GRAD_AT:PACK] = grad
        for args in pack_args:
            start_to_head(args)

    def send_keys():
        keys = dot(lat[...], kw[...]).astype(BF16).T
        for e in (0, 1):
            kts[e, 0:NOPE] = keys[e * NOPE : (e + 1) * NOPE]
            kts[e, NOPE:HEAD] = rope[...]
            start_to_head(key_args[e])
        values = dot(lat[...], vw[...]).astype(BF16).T
        for e in (0, 1):
            vts[e] = values[e * VDIM : (e + 1) * VDIM]
            start_to_head(value_args[e])

    @pl.when(z < 2)
    def _():
        send_keys()
        send_queries()

    @pl.when(z >= 2)
    def _():
        send_queries()
        send_keys()

    def weight_copy(kind, dy, p):
        at = 2 * ((y + dy) % 4) + c
        to = (y_peer(1), y_peer(3), partner)[kind]
        return remote(wt.at[at, p], wt.at[at, p], s_wt.at[0], r_wt.at[3 if kind == 2 else 2 if dy else p], to)

    def send_weight(*args):
        copy = weight_copy(*args)
        copy.start()

    def take_weights(p):
        arrived(wt.at[0], r_wt.at[p], "wait_weights")
        for dy in (1, 3):
            send_weight(2, dy, p)
        send_weight(p, 3 - 2 * p, p)

    for p, weights in ((0, kw), (1, vw)):
        wt[tp, p] = weights[...].T
        for kind in (0, 1, 2):
            send_weight(kind, 0, p)

    def zero(b, _):
        dq[b] = jnp.zeros((HEAD, ROWS), F32)
        return 0

    lax.fori_loop(0, 16, zero, 0)

    def step(t):
        near = t < 4
        far = t >= 12
        mid = jnp.logical_not(near | far)
        pair = t % 2
        slot = 1 - jnp.where(mid, (t - 4) // 4, (t % 4) // 2)
        other = jnp.where(mid, ((t - 4) // 2) % 2, pair)
        dx = jnp.where(near, 0, jnp.where(far, 2, jnp.where(pair == 0, 3, 1)))
        core = jnp.where(other == 0, c, 1 - c)
        block = 4 * key_z(core, slot) + (x + dx) % 4
        return block, dx, other, slot

    def forwards(t, h):
        b, dx, other, slot = step(t)
        block = half(qb, b, h)
        mine = other == 0
        plus = mine & ((dx == 0) | ((dx == 3) & (slot == 0)))
        minus = mine & ((dx == 0) | ((dx == 1) & (slot == 1)))
        return [
            (plus, remote(block, block, s_fw.at[0], r_q.at[b, h], x_peer(1))),
            (minus, remote(block, block, s_fw.at[1], r_q.at[b, h], x_peer(3))),
            (mine, remote(block, block, s_fw.at[2], r_q.at[b, h], partner)),
        ]

    def take(t):
        b = step(t)[0]
        for h in (0, 1):
            arrived(half(qb, b, h), r_q.at[b, h], "wait_query")
            for holds, copy in forwards(t, h):

                @pl.when(holds)
                def _():
                    copy.start()

    def tile(b, s, masked):
        raw = dot(kaug[s], qb[b, 0:GRAD_AT]) * (SCALE * LOG2E)
        if masked:
            key_row = lax.broadcasted_iota(jnp.int32, (ROWS, ROWS), 0)
            query_row = lax.broadcasted_iota(jnp.int32, (ROWS, ROWS), 1)
            raw = jnp.where(key_row <= query_row, raw, -1e30)
        probs = jnp.exp2(raw)
        diff = dot(vaug[s], qb[b, LSE_AT:PACK])
        grads = (probs * diff).astype(BF16)
        dv[s] += dot_nt(probs.astype(BF16), qb[b, GRAD_AT:PACK])
        dk[s] += dot_nt(grads, qb[b, 0:LSE_AT])
        dq[b] += dot(kv[s, 0:HEAD], grads)

    def to_partner(i):
        return remote(dqs.at[i], dqr.at[i], s_d.at[0], r_d.at[i], partner)

    def share(t):
        b, dx, other, slot = step(t)

        @pl.when(other == 1)
        def _():
            i = 2 * dx + slot
            dqs[i] = dq[b].astype(BF16)
            to_partner(i).start()

    def own_block(s):
        return 4 * key_z(c, s) + x

    def take_keys(s):
        arrived(kv.at[s, pl.ds(0, HEAD)], r_kt.at[s], "wait_keys")
        arrived(kv.at[s, pl.ds(VALUE_AT, VDIM)], r_v.at[s], "wait_values")
        kaug[s] = kv[s, 0:GRAD_AT].T
        vaug[s] = kv[s, GRAD_AT:KEY_PACK].T

    def tiles(t):
        b = step(t)[0]

        def pair(s, _):
            @pl.when(b > own_block(s))
            def _():
                tile(b, s, False)

            return 0

        with jax.named_scope("pair"):
            lax.fori_loop(0, 2, pair, 0)

    def early(t, _):
        @pl.when(t > 0)
        def _():
            take(t)

        with jax.named_scope("early"):
            tile(step(t)[0], 0, False)
        return 0

    def diagonal(s, _):
        tile(own_block(s), s, True)
        return 0

    def later(t, _):
        take(t)

        @pl.when(t == 5)
        def _():
            take_weights(0)

        @pl.when(t == 8)
        def _():
            take_weights(1)

        tiles(t)
        share(t)
        return 0

    def piece(s, j):
        i = (4 * c + y + j) % 8
        token_z = key_z(c, s)
        to = (4 * token_z + x, 2 * (i % 4) + i // 4)
        src, dst = gs.at[s, i], gf.at[4 * y + z]
        return (
            (token_z == z) if j == 0 else None,
            remote(src, dst, s_g.at[s], r_g.at[y], to),
            pltpu.make_async_copy(src, dst, r_g.at[y]),
        )

    def by_piece(s, j, local_op, remote_op):
        own, copy, local = piece(s, j)
        if own is None:
            remote_op(copy)
            return

        @pl.when(own)
        def _():
            local_op(local)

        @pl.when(jnp.logical_not(own))
        def _():
            remote_op(copy)

    def send_grads(s):
        gs[s, :, 0:CHUNK] = (dk[s, :, 0:NOPE] * SCALE).astype(BF16).reshape(8, CHUNK, NOPE)
        gs[s, :, CHUNK : 2 * CHUNK] = dv[s].astype(BF16).reshape(8, CHUNK, VDIM)
        ropes = (dk[s, :, NOPE:HEAD] * SCALE).astype(BF16).reshape(8, 2, 32, ROPE)
        gs[s, :, 2 * CHUNK : PIECE] = jnp.concatenate([ropes[:, 0], ropes[:, 1]], axis=2)
        for j in range(8):
            by_piece(s, j, lambda local: local.start(), lambda copy: copy.start())

    def to_owner(s, src, dst, send, recv):
        token_z = key_z(c, s)
        own = (token_z == z) & (z // 2 == c)
        copy = remote(src, dst, send, recv, (4 * token_z + x, 2 * y + z // 2))
        return own, copy, pltpu.make_async_copy(src, dst, recv)

    def start_to_owner(args):
        own, copy, local = to_owner(*args)

        @pl.when(own)
        def _():
            local.start()

        @pl.when(jnp.logical_not(own))
        def _():
            copy.start()

    def sent_to_owner(args):
        own, copy, _ = to_owner(*args)

        @pl.when(jnp.logical_not(own))
        def _():
            copy.wait_send()

    e_mine = z % 2
    back = []

    def add_share(dx, s):
        i = 2 * dx + s
        arrived(dqr.at[i], r_d.at[i], "wait_share")
        b = 4 * key_z(c, s) + (x + dx) % 4
        return dq[b] + dqr[i].astype(F32)

    def send_x(i, value, dst, recv, to):
        xs[i] = value.astype(BF16)
        copy = remote(xs.at[i], dst, s_x.at[0], recv, to)
        copy.start()

    def to_hbm(i):
        pltpu.make_async_copy(ag.at[i], ag_out.at[i], s_out.at[2]).start()

    take(0)
    take_keys(0)
    lax.fori_loop(0, 2, early, 0)
    for args in latent_args:
        start_to_head(args)
    take(2)
    take_keys(1)
    with jax.named_scope("diagonal"):
        lax.fori_loop(0, 2, diagonal, 0)

    @pl.when(step(1)[0] > own_block(1))
    def _():
        tile(step(1)[0], 1, False)

    share(1)
    lax.fori_loop(3, 14, later, 0)

    send_grads(1)
    send_x(1, add_share(2, 1), rel.at[1], r_rel.at[1], x_peer(1))
    send_x(2, add_share(3, 1), fin.at[1, 1], r_fin.at[1], x_peer(3))
    send_x(3, add_share(1, 0), fin.at[0, 0], r_fin.at[0], x_peer(1))
    lax.fori_loop(14, 16, later, 0)
    send_grads(0)
    send_x(0, add_share(2, 0), rel.at[0], r_rel.at[0], x_peer(3))

    arrived(wt.at[0], r_wt.at[2], "wait_weights")
    for p in (0, 1):
        send_weight(2, 2, p)

    for args in pack_args + key_args + value_args + latent_args:
        sent_to_head(args)

    left(qb.at[pl.ds(0, 3)], s_fw.at[0])
    left(qb.at[pl.ds(0, 3)], s_fw.at[1])
    left(qb.at[pl.ds(0, 8)], s_fw.at[2])
    left(dqs, s_d.at[0])

    def relay_plus():
        value = add_share(1, 1)
        arrived(rel.at[1], r_rel.at[1], "wait_relay")
        send_x(5, value + rel[1].astype(F32), fin.at[1, 0], r_fin.at[1], x_peer(1))

    def relay_minus():
        value = add_share(3, 0)
        arrived(rel.at[0], r_rel.at[0], "wait_relay")
        send_x(4, value + rel[0].astype(F32), fin.at[0, 1], r_fin.at[0], x_peer(3))

    relay_plus()
    relay_minus()

    arrived(wt.at[pl.ds(0, 4)], r_wt.at[3], "wait_weights")
    latent = jnp.zeros((CHUNK, LATENT), F32)
    ropes = jnp.zeros((32, 2 * ROPE), F32)
    for j in (0, 1, 3, 2):
        yj = (y + j) % 4
        arrived(gf.at[pl.ds(4 * yj, 4)], r_g.at[yj], "wait_grads")
        for u in range(4):
            ropes += gf[4 * yj + u, 2 * CHUNK : PIECE].astype(F32)
        for core in (0, 1):
            first, second = 4 * yj + 2 * core, 4 * yj + 2 * core + 1
            for p in (0, 1):
                rows = slice(p * CHUNK, (p + 1) * CHUNK)
                grads = jnp.concatenate([gf[first, rows], gf[second, rows]], axis=1)
                latent += dot(grads, wt[2 * yj + core, p])
    mine = 4 * c + y
    for i in range(8):
        ag[mine, CHUNK * i : CHUNK * (i + 1)] = latent[:, 128 * i : 128 * (i + 1)].astype(BF16)
    ag[mine, 8 * CHUNK : DONE] = ropes.astype(BF16)
    for j in (2, 1, 3):
        remote(ag.at[mine], ag.at[mine], s_ag.at[0], r_ag.at[mine], y_peer(j)).start()
    remote(ag.at[mine], ag.at[mine], s_ag.at[0], r_ag.at[mine], partner).start()
    to_hbm(mine)

    for s in (0, 1):
        arrived(lt.at[s], r_lt.at[s], "wait_latent")
    weight = dot(gs[0, :, CHUNK : 2 * CHUNK].reshape(ROWS, VDIM).T, lt[0])
    weight += dot(gs[1, :, CHUNK : 2 * CHUNK].reshape(ROWS, VDIM).T, lt[1])
    for core in (0, 1):
        dwh[core] = weight[:, 512 * core : 512 * (core + 1)].astype(BF16).T
    to_half = remote(dwh.at[1 - c], dwhr, s_wh.at[0], r_wh.at[0], partner)
    to_half.start()

    arrived(dwhr, r_wh.at[0], "wait_weight")
    weight = (dwh[c].astype(F32) + dwhr[...].astype(F32)).astype(BF16)
    for i in range(8):
        dwx[i % 4, i // 4] = weight[64 * i : 64 * (i + 1)]
    for j in (2, 1, 3):
        xj = (x + j) % 4
        copy = remote(dwx.at[xj], dwxr.at[x], s_wx.at[0], r_wx.at[0], x_peer(j))
        copy.start()

    for s in (0, 1):
        home = add_share(0, s)
        arrived(fin.at[s], r_fin.at[s], "wait_home")
        home += fin[s, 0].astype(F32) + fin[s, 1].astype(F32)
        dqh[s] = (home * SCALE).astype(BF16)
        args = (s, dqh.at[s], dqf.at[e_mine], s_h.at[s], r_h.at[e_mine])
        start_to_owner(args)
        back.append(args)

    weight = dwx[x].astype(F32)
    arrived(dwxr.at[pl.ds(0, 3)], r_wx.at[0], "wait_weight")
    for j in (1, 3, 2):
        weight += dwxr[(x + j) % 4].astype(F32)
    dwz[...] = weight.astype(BF16)

    def weight_home(i):
        row_z = 2 * c + i
        own = (row_z == z) & (z // 2 == c)
        src, dst = dwz.at[i], dwf.at[z % 2]
        copy = remote(src, dst, s_wz.at[i], r_wz.at[z % 2], (4 * row_z + x, 2 * y + z // 2))
        return own, copy, pltpu.make_async_copy(src, dst, r_wz.at[z % 2])

    for i in (0, 1):
        own, copy, local = weight_home(i)

        @pl.when(own)
        def _():
            local.start()

        @pl.when(jnp.logical_not(own))
        def _():
            copy.start()

    for s in (0, 1):
        own = key_z(c, s) == z

        @pl.when(own)
        def _():
            left(gs.at[s, pl.ds(0, 7)], s_g.at[s])

        @pl.when(jnp.logical_not(own))
        def _():
            left(gs.at[s], s_g.at[s])

    left(wt.at[pl.ds(0, 7)], s_wt.at[0])
    left(xs, s_x.at[0])
    left(dwx.at[pl.ds(0, 3)], s_wx.at[0])

    for j in (1, 3, 2):
        i = 4 * c + (y + j) % 4
        arrived(ag.at[i], r_ag.at[i], "wait_chunk")
        remote(ag.at[i], ag.at[i], s_ag.at[0], r_ag.at[i], partner).start()
        to_hbm(i)

    for e in (0, 1):
        arrived(dwf.at[e], r_wz.at[e], "wait_weight")
        dwo[:, e * VDIM : (e + 1) * VDIM] = dwf[e].astype(F32)
    for e in (0, 1):
        arrived(dqf.at[e], r_h.at[e], "wait_queries")
    dqo[...] = jnp.concatenate([dqf[0], dqf[1]], axis=0).T
    stores = [pltpu.make_async_copy(dqo, dq_out, s_out.at[0]), pltpu.make_async_copy(dwo, dw_out, s_out.at[1])]
    for store in stores:
        store.start()
    for i in (0, 1):
        own, copy, _ = weight_home(i)

        @pl.when(jnp.logical_not(own))
        def _():
            copy.wait_send()

    for args in back:
        sent_to_owner(args)
    for j in (0, 1, 3, 2):
        i = 4 * (1 - c) + (y + j) % 4
        arrived(ag.at[i], r_ag.at[i], "wait_other_chunk")
        to_hbm(i)

    with jax.named_scope("last"):
        to_half.wait_send()
        left(ag.at[pl.ds(0, 7)], s_ag.at[0])
        for store in stores:
            store.wait()
        pltpu.make_async_copy(ag, ag_out, s_out.at[2]).wait()


def finish(ag_hbm, dq_hbm, dw_hbm, dlat_hbm, drope_hbm, dq_out, dw_out, ag, dq, dw, dlat, drope, s_in, s_out):
    loads = [pltpu.make_async_copy(ag_hbm.at[i], ag.at[i], s_in.at[i]) for i in range(8)]
    loads += [pltpu.make_async_copy(dq_hbm, dq, s_in.at[8]), pltpu.make_async_copy(dw_hbm, dw, s_in.at[9])]
    for load in loads:
        load.start()
    stores = []
    for i in range(8):
        loads[i].wait()
        rows = pl.ds(CHUNK * i, CHUNK)
        for j in range(8):
            dlat[rows, 128 * j : 128 * (j + 1)] = ag[i, CHUNK * j : CHUNK * (j + 1)].astype(F32)
        stores.append(pltpu.make_async_copy(dlat.at[rows], dlat_hbm.at[rows], s_out.at[i]))
        stores[-1].start()
    for i, src, dst in ((8, dq, dq_out), (9, dw, dw_out)):
        loads[i].wait()
        stores.append(pltpu.make_async_copy(src, dst, s_out.at[i]))
        stores[-1].start()
    ropes = []
    for i in range(8):
        pairs = ag[i, 8 * CHUNK : DONE].T.astype(F32)
        ropes += [pairs[0:ROPE], pairs[ROPE : 2 * ROPE]]
    drope[...] = jnp.concatenate(ropes, axis=1)
    stores.append(pltpu.make_async_copy(drope, drope_hbm, s_out.at[10]))
    stores[-1].start()
    for store in stores:
        store.wait()


def per_device(q, lat, rope, kw, vw, lse, ao, go):
    vmem = pl.BlockSpec(memory_space=pltpu.VMEM)
    anywhere = pl.BlockSpec(memory_space=pl.ANY)

    def buf(*shape, dtype=BF16):
        return pltpu.VMEM(shape, dtype)

    def sem(*shape):
        return pltpu.SemaphoreType.DMA(shape)

    scratch = [
        buf(ROWS, 2 * HEAD), buf(ROWS, LATENT), buf(ROPE, ROWS), buf(LATENT, 256), buf(LATENT, 256),
        buf(2, ROWS, dtype=F32), buf(ROWS, 256), buf(ROWS, 256),
        buf(16, PACK, ROWS), buf(2, PACK, ROWS), buf(2, HEAD, ROWS), buf(2, VDIM, ROWS),
        buf(2, KEY_PACK, ROWS), buf(2, ROWS, GRAD_AT), buf(2, ROWS, KEY_PACK - GRAD_AT),
        buf(2, ROWS, HEAD, dtype=F32), buf(2, ROWS, VDIM, dtype=F32), buf(16, HEAD, ROWS, dtype=F32),
        buf(8, HEAD, ROWS), buf(8, HEAD, ROWS), buf(6, HEAD, ROWS), buf(2, HEAD, ROWS), buf(2, 2, HEAD, ROWS),
        buf(2, HEAD, ROWS), buf(2, HEAD, ROWS), buf(2, 8, PIECE, 128), buf(16, PIECE, 128),
        buf(2, ROWS, LATENT), buf(8, 2, 256, LATENT),
        buf(2, 512, VDIM), buf(512, VDIM), buf(4, 2, 64, VDIM), buf(4, 2, 64, VDIM), buf(2, 64, VDIM), buf(2, 64, VDIM),
        buf(8, DONE, 128), buf(ROWS, 2 * HEAD), buf(64, 256, dtype=F32),
        sem(8), sem(2, 2), sem(2), sem(2), sem(16, 2), sem(2), sem(2), sem(3), sem(1), sem(8), sem(1), sem(2),
        sem(2), sem(2), sem(2), sem(2), sem(4),
        sem(2), sem(2), sem(1), sem(4), sem(1), sem(8), sem(1), sem(1), sem(1), sem(1), sem(2), sem(2), sem(3),
    ]
    ag, dq, dw = pl.pallas_call(
        kernel,
        in_specs=[anywhere] * 8,
        out_specs=[anywhere] * 3,
        out_shape=[
            jax.ShapeDtypeStruct((8, DONE, 128), BF16),
            jax.ShapeDtypeStruct((ROWS, 2 * HEAD), BF16),
            jax.ShapeDtypeStruct((64, 256), F32),
        ],
        scratch_shapes=scratch,
        compiler_params=pltpu.CompilerParams(
            collective_id=0, has_side_effects=True, vmem_limit_bytes=58000 * 1024
        ),
        name="latent_attention_backward",
    )(q, lat, rope.T, kw, vw, lse, ao, go)
    dlat, drope, dq, dw = pl.pallas_call(
        finish,
        in_specs=[anywhere] * 3,
        out_specs=[anywhere] * 4,
        out_shape=[
            jax.ShapeDtypeStruct((ROWS, LATENT), F32),
            jax.ShapeDtypeStruct((ROPE, ROWS), F32),
            jax.ShapeDtypeStruct((ROWS, 2 * HEAD), BF16),
            jax.ShapeDtypeStruct((64, 256), F32),
        ],
        scratch_shapes=[
            buf(8, DONE, 128), buf(ROWS, 2 * HEAD), buf(64, 256, dtype=F32),
            buf(ROWS, LATENT, dtype=F32), buf(ROPE, ROWS, dtype=F32), sem(10), sem(11),
        ],
        compiler_params=pltpu.CompilerParams(vmem_limit_bytes=58000 * 1024),
        name="finish",
    )(ag, dq, dw)
    return dq, dlat, drope.T, dw


def solution(mesh):
    placed = (
        P("sp", "tp"),
        P("sp", None),
        P("sp", None),
        P(None, "tp"),
        P(None, "tp"),
        P("tp", "sp"),
        P("sp", "tp"),
        P("sp", "tp"),
    )
    return jax.shard_map(
        per_device,
        mesh=mesh,
        in_specs=placed,
        out_specs=(P("sp", "tp"), P("sp", None), P("sp", None), P("sp", "tp")),
        check_vma=False,
    )
```

```python
import jax
import jax.numpy as jnp
from jax import lax
from jax.experimental import pallas as pl
from jax.experimental.pallas import tpu as pltpu
from jax.sharding import PartitionSpec as P

NOPE = 128
ROPE = 64
HEAD = NOPE + ROPE
VDIM = 128
ROWS = 512
LATENT = 1024
CHUNK = 64
PIECE = 160
DONE = 544
HALF = 256
SCALE = HEAD**-0.5
LOG2E = 1.4426950408889634
BF16 = jnp.bfloat16
F32 = jnp.float32
MESH = pl.DeviceIdType.MESH
NT = (((1,), (1,)), ((), ()))

LSE_AT, GRAD_AT, PACK = 192, 208, 336
ONES_AT, VALUE_AT, KEY_PACK = 192, 224, 352


def dot(a, b):
    return jnp.dot(a, b, preferred_element_type=F32)


def dot_nt(a, b):
    return lax.dot_general(a, b, NT, preferred_element_type=F32)


def in_three(row):
    high = row.astype(BF16).astype(F32)
    middle = (row - high).astype(BF16).astype(F32)
    return high, middle, row - high - middle


def six_rows(first, second):
    at = lax.broadcasted_iota(jnp.int32, (16, first.shape[1]), 0)
    rows = jnp.zeros(at.shape, F32)
    for i, part in enumerate(in_three(first) + in_three(second)):
        rows = jnp.where(at == i, part, rows)
    return rows.astype(BF16)


def ones_rows(first):
    at = lax.broadcasted_iota(jnp.int32, (16, ROWS), 0)
    return jnp.where((at >= first) & (at < first + 3), 1.0, 0.0).astype(BF16)


def kernel(
    q_hbm, lat_hbm, rope_hbm, kw_hbm, vw_hbm, lse_hbm, ao_hbm, go_hbm,
    ag_out, dq_out, dw_out,
    q, lat, rope, kw, vw, lse, ao, go,
    qb, pk, kts, vts, kv, kaug, vaug, dk, dv, dq,
    dqs, dqr, xs, rel, fin, dqh, dqf, gs, gf, lt, wt,
    dwh, dwhr, dwx, dwxr, dwz, dwf, ag, dqo, dwo,
    s_in, s_pk, s_kt, s_v, r_q, r_kt, r_v, s_fw, s_d, r_d, s_x, r_rel, r_fin, s_h, r_h, s_g, r_g,
    s_lt, r_lt, s_wt, r_wt, s_ag, r_ag, s_wh, r_wh, s_wx, r_wx, s_wz, r_wz, s_out,
):
    sp, tp = lax.axis_index("sp"), lax.axis_index("tp")
    z, x, y, c = sp // 4, sp % 4, tp // 2, tp % 2
    core_of_z = ((z + 1) // 2) % 2
    slot_of_z = z // 2
    partner = (sp, 2 * y + 1 - c)

    def key_z(core, slot):
        return core + slot * (3 - 2 * core)

    def x_peer(j):
        return (4 * z + (x + j) % 4, tp)

    def z_peer(j):
        return (4 * ((z + j) % 4) + x, tp)

    def y_peer(j):
        return (sp, 2 * ((y + j) % 4) + c)

    def remote(src, dst, send, recv, to):
        return pltpu.make_async_remote_copy(
            src_ref=src, dst_ref=dst, send_sem=send, recv_sem=recv, device_id=to, device_id_type=MESH
        )

    def arrived(ref, recv, name="wait"):
        with jax.named_scope(name):
            remote(ref, ref, s_in.at[0], recv, partner).wait_recv()

    def left(ref, send):
        remote(ref, ref, send, s_in.at[0], partner).wait_send()

    barrier = pltpu.get_barrier_semaphore()
    peers = [partner]
    for j in (1, 2, 3):
        peers += [x_peer(j)]
        peers += [(sp, 2 * ((y + j) % 4) + core) for core in (0, 1)]
        peers += [(4 * ((z + j) % 4) + x, 2 * y + core) for core in (0, 1)]
    for peer in peers:
        pl.semaphore_signal(barrier, inc=1, device_id=peer, device_id_type=MESH)

    def load(i):
        pairs = ((q_hbm, q), (go_hbm, go), (ao_hbm, ao), (lse_hbm, lse), (lat_hbm, lat), (kw_hbm, kw), (rope_hbm, rope), (vw_hbm, vw))
        return pltpu.make_async_copy(*pairs[i], s_in.at[i])

    @pl.when(z < 2)
    def _():
        for i in (4, 5, 6, 7, 0, 1, 2, 3):
            load(i).start()

    @pl.when(z >= 2)
    def _():
        for i in range(8):
            load(i).start()

    dk[...] = jnp.zeros_like(dk)
    dv[...] = jnp.zeros_like(dv)
    for s in (0, 1):
        kv[s, ONES_AT : ONES_AT + 16] = ones_rows(0)
        kv[s, ONES_AT + 16 : VALUE_AT] = ones_rows(3)

    def to_head(e, src, dst, send, recv):
        head_z = 2 * c + e
        own = (head_z == z) & (core_of_z == c)
        copy = remote(src, dst, send, recv, (4 * head_z + x, 2 * y + core_of_z))
        return own, copy, pltpu.make_async_copy(src, dst, recv)

    def start_to_head(args):
        own, copy, local = to_head(*args)

        @pl.when(own)
        def _():
            local.start()

        @pl.when(jnp.logical_not(own))
        def _():
            copy.start()

    def sent_to_head(args):
        own, copy, _ = to_head(*args)

        @pl.when(jnp.logical_not(own))
        def _():
            copy.wait_send()

    def half(ref, b, h):
        return ref.at[b, :, pl.ds(HALF * h, HALF)]

    pack_args = [
        (e, half(pk, e, h), half(qb, sp, h), s_pk.at[e, h], r_q.at[sp, h]) for h in (0, 1) for e in (0, 1)
    ]
    key_args = [
        (e, kts.at[e], kv.at[slot_of_z, pl.ds(0, HEAD)], s_kt.at[e], r_kt.at[slot_of_z]) for e in (0, 1)
    ]
    value_args = [
        (e, vts.at[e], kv.at[slot_of_z, pl.ds(VALUE_AT, VDIM)], s_v.at[e], r_v.at[slot_of_z]) for e in (0, 1)
    ]

    latent_args = [(e, lat, lt.at[slot_of_z], s_lt.at[e], r_lt.at[slot_of_z]) for e in (0, 1)]

    def pack_queries():
        for i in range(4):
            load(i).wait()
        qt = q[...].T
        got = go[...].T
        aot = ao[...].T
        for e in (0, 1):
            grad = got[e * VDIM : (e + 1) * VDIM]
            delta = jnp.sum(
                grad.astype(F32) * aot[e * VDIM : (e + 1) * VDIM].astype(F32), axis=0, keepdims=True
            )
            pk[e, 0:LSE_AT] = qt[e * HEAD : (e + 1) * HEAD]
            pk[e, LSE_AT:GRAD_AT] = six_rows(lse[e : e + 1, :] * (-1.0 / SCALE), -delta)
            pk[e, GRAD_AT:PACK] = grad

    def pack_keys():
        for i in range(4, 8):
            load(i).wait()
        keys = dot(lat[...], kw[...]).astype(BF16).T
        for e in (0, 1):
            kts[e, 0:NOPE] = keys[e * NOPE : (e + 1) * NOPE]
            kts[e, NOPE:HEAD] = rope[...]
        values = dot(lat[...], vw[...]).astype(BF16).T
        for e in (0, 1):
            vts[e] = values[e * VDIM : (e + 1) * VDIM]

    def send_queries():
        for args in pack_args:
            start_to_head(args)

    def send_keys():
        for args in key_args + value_args:
            start_to_head(args)

    def weight_copy(kind, dy, p):
        at = 2 * ((y + dy) % 4) + c
        to = (y_peer(1), y_peer(3), partner)[kind]
        return remote(wt.at[at, p], wt.at[at, p], s_wt.at[0], r_wt.at[3 if kind == 2 else 2 if dy else p], to)

    def send_weight(*args):
        copy = weight_copy(*args)
        copy.start()

    def take_weights(p):
        arrived(wt.at[0], r_wt.at[p], "wait_weights")
        for dy in (1, 3):
            send_weight(2, dy, p)
        send_weight(p, 3 - 2 * p, p)

    def send_own_weights(p):
        wt[tp, p] = (kw, vw)[p][...].T
        for kind in (0, 1, 2):
            send_weight(kind, 0, p)

    @pl.when(z < 2)
    def _():
        pack_keys()

    @pl.when(z >= 2)
    def _():
        pack_queries()

    with jax.named_scope("barrier"):
        pl.semaphore_wait(barrier, len(peers))

    @pl.when(z < 2)
    def _():
        send_keys()
        send_own_weights(0)
        pack_queries()
        send_queries()

    @pl.when(z >= 2)
    def _():
        send_queries()
        pack_keys()
        send_keys()
        send_own_weights(0)

    send_own_weights(1)

    def zero(b, _):
        dq[b] = jnp.zeros((HEAD, ROWS), F32)
        return 0

    lax.fori_loop(0, 16, zero, 0)

    def step(t):
        near = t < 4
        far = t >= 12
        mid = jnp.logical_not(near | far)
        pair = t % 2
        slot = 1 - jnp.where(mid, (t - 4) // 4, (t % 4) // 2)
        other = jnp.where(mid, ((t - 4) // 2) % 2, pair)
        dx = jnp.where(near, 0, jnp.where(far, 2, jnp.where(pair == 0, 3, 1)))
        core = jnp.where(other == 0, c, 1 - c)
        block = 4 * key_z(core, slot) + (x + dx) % 4
        return block, dx, other, slot

    def forwards(t, h):
        b, dx, other, slot = step(t)
        block = half(qb, b, h)
        mine = other == 0
        plus = mine & ((dx == 0) | ((dx == 3) & (slot == 0)))
        minus = mine & ((dx == 0) | ((dx == 1) & (slot == 1)))
        return [
            (plus, remote(block, block, s_fw.at[0], r_q.at[b, h], x_peer(1))),
            (minus, remote(block, block, s_fw.at[1], r_q.at[b, h], x_peer(3))),
            (mine, remote(block, block, s_fw.at[2], r_q.at[b, h], partner)),
        ]

    def take(t):
        b = step(t)[0]
        for h in (0, 1):
            arrived(half(qb, b, h), r_q.at[b, h], "wait_query")
            for holds, copy in forwards(t, h):

                @pl.when(holds)
                def _():
                    copy.start()

    def tile(b, s, masked):
        raw = dot(kaug[s], qb[b, 0:GRAD_AT]) * (SCALE * LOG2E)
        if masked:
            key_row = lax.broadcasted_iota(jnp.int32, (ROWS, ROWS), 0)
            query_row = lax.broadcasted_iota(jnp.int32, (ROWS, ROWS), 1)
            raw = jnp.where(key_row <= query_row, raw, -1e30)
        probs = jnp.exp2(raw)
        diff = dot(vaug[s], qb[b, LSE_AT:PACK])
        grads = (probs * diff).astype(BF16)
        dv[s] += dot_nt(probs.astype(BF16), qb[b, GRAD_AT:PACK])
        dk[s] += dot_nt(grads, qb[b, 0:LSE_AT])
        dq[b] += dot(kv[s, 0:HEAD], grads)

    def to_partner(i):
        return remote(dqs.at[i], dqr.at[i], s_d.at[0], r_d.at[i], partner)

    def share(t):
        b, dx, other, slot = step(t)

        i = 2 * dx + slot
        dqs[i] = dq[b].astype(BF16)
        to_partner(i).start()

    def own_block(s):
        return 4 * key_z(c, s) + x

    def take_keys(s):
        arrived(kv.at[s, pl.ds(0, HEAD)], r_kt.at[s], "wait_keys")
        arrived(kv.at[s, pl.ds(VALUE_AT, VDIM)], r_v.at[s], "wait_values")
        kaug[s] = kv[s, 0:GRAD_AT].T
        vaug[s] = kv[s, GRAD_AT:KEY_PACK].T

    def both_tiles(b):
        probs = [jnp.exp2(dot(kaug[s], qb[b, 0:GRAD_AT]) * (SCALE * LOG2E)) for s in (0, 1)]
        grads = [(probs[s] * dot(vaug[s], qb[b, LSE_AT:PACK])).astype(BF16) for s in (0, 1)]
        for s in (0, 1):
            dv[s] += dot_nt(probs[s].astype(BF16), qb[b, GRAD_AT:PACK])
            dk[s] += dot_nt(grads[s], qb[b, 0:LSE_AT])
        dq[b] += dot(kv[0, 0:HEAD], grads[0]) + dot(kv[1, 0:HEAD], grads[1])

    def tiles(b):
        with jax.named_scope("pair"):

            @pl.when(b > own_block(1))
            def _():
                both_tiles(b)

            @pl.when((b > own_block(0)) & (b < own_block(1)))
            def _():
                tile(b, 0, False)

    def early(t, _):
        @pl.when(t > 0)
        def _():
            take(t)

        with jax.named_scope("early"):
            tile(step(t)[0], 0, False)
        return 0

    def diagonal(s, _):
        tile(own_block(s), s, True)
        return 0

    def later(p, _):
        far = p >= 6
        even = jnp.logical_not(far) & (p % 2 == 0)
        odd = jnp.logical_not(far) & (p % 2 == 1)
        slot = step(2 * p)[3]

        @pl.when(even)
        def _():
            for h in (0, 1):
                for i, back_slot in ((0, 0), (1, 1)):
                    b = step(2 * p + i)[0]
                    block = half(qb, b, h)
                    arrived(block, r_q.at[b, h], "wait_query")

                    @pl.when(slot == back_slot)
                    def _():
                        remote(block, block, s_fw.at[i], r_q.at[b, h], x_peer(1 + 2 * i)).start()

                    remote(block, block, s_fw.at[2], r_q.at[b, h], partner).start()

        @pl.when(odd)
        def _():
            for i in (0, 1):
                b = step(2 * p + i)[0]
                for h in (0, 1):
                    arrived(half(qb, b, h), r_q.at[b, h], "wait_query")

        @pl.when(far)
        def _():
            b = step(2 * p)[0]
            for h in (0, 1):
                block = half(qb, b, h)
                arrived(block, r_q.at[b, h], "wait_query")
                remote(block, block, s_fw.at[2], r_q.at[b, h], partner).start()

        @pl.when(p == 2)
        def _():
            take_weights(0)

        @pl.when(p == 4)
        def _():
            take_weights(1)

        def member(i, _):
            b = step(2 * p + i)[0]

            @pl.when(far & (i == 1))
            def _():
                for h in (0, 1):
                    arrived(half(qb, b, h), r_q.at[b, h], "wait_query")

            tiles(b)
            return 0

        lax.fori_loop(0, 2, member, 0)

        @pl.when(odd)
        def _():
            share(2 * p)

        @pl.when(odd | far)
        def _():
            share(2 * p + 1)

        return 0

    def rest(i, _):
        b = step(1 + 2 * i)[0]

        @pl.when(b > own_block(1 - i))
        def _():
            tile(b, 1 - i, False)

        return 0

    def piece(s, j):
        i = (4 * c + y + j) % 8
        token_z = key_z(c, s)
        to = (4 * token_z + x, 2 * (i % 4) + i // 4)
        src, dst = gs.at[s, i], gf.at[4 * y + z]
        return (
            (token_z == z) if j == 0 else None,
            remote(src, dst, s_g.at[s], r_g.at[y], to),
            pltpu.make_async_copy(src, dst, r_g.at[y]),
        )

    def by_piece(s, j, local_op, remote_op):
        own, copy, local = piece(s, j)
        if own is None:
            remote_op(copy)
            return

        @pl.when(own)
        def _():
            local_op(local)

        @pl.when(jnp.logical_not(own))
        def _():
            remote_op(copy)

    def send_grads(s):
        gs[s, :, 0:CHUNK] = (dk[s, :, 0:NOPE] * SCALE).astype(BF16).reshape(8, CHUNK, NOPE)
        gs[s, :, CHUNK : 2 * CHUNK] = dv[s].astype(BF16).reshape(8, CHUNK, VDIM)
        ropes = (dk[s, :, NOPE:HEAD] * SCALE).astype(BF16).reshape(8, 2, 32, ROPE)
        gs[s, :, 2 * CHUNK : PIECE] = jnp.concatenate([ropes[:, 0], ropes[:, 1]], axis=2)
        for j in range(8):
            by_piece(s, j, lambda local: local.start(), lambda copy: copy.start())

    def to_owner(s, src, dst, send, recv):
        token_z = key_z(c, s)
        own = (token_z == z) & (z // 2 == c)
        copy = remote(src, dst, send, recv, (4 * token_z + x, 2 * y + z // 2))
        return own, copy, pltpu.make_async_copy(src, dst, recv)

    def start_to_owner(args):
        own, copy, local = to_owner(*args)

        @pl.when(own)
        def _():
            local.start()

        @pl.when(jnp.logical_not(own))
        def _():
            copy.start()

    def sent_to_owner(args):
        own, copy, _ = to_owner(*args)

        @pl.when(jnp.logical_not(own))
        def _():
            copy.wait_send()

    e_mine = z % 2
    back = []

    def add_share(dx, s):
        i = 2 * dx + s
        arrived(dqr.at[i], r_d.at[i], "wait_share")
        b = 4 * key_z(c, s) + (x + dx) % 4
        return dq[b] + dqr[i].astype(F32)

    def send_x(i, value, dst, recv, to):
        xs[i] = value.astype(BF16)
        copy = remote(xs.at[i], dst, s_x.at[0], recv, to)
        copy.start()

    def to_hbm(i):
        pltpu.make_async_copy(ag.at[i], ag_out.at[i], s_out.at[2]).start()

    take(0)
    take_keys(0)
    lax.fori_loop(0, 2, early, 0)
    for args in latent_args:
        start_to_head(args)
    take(2)
    take_keys(1)
    with jax.named_scope("diagonal"):
        lax.fori_loop(0, 2, diagonal, 0)

    take(3)
    lax.fori_loop(0, 2, rest, 0)
    share(1)
    share(3)
    lax.fori_loop(2, 7, later, 0)

    send_grads(1)
    send_x(1, add_share(2, 1), rel.at[1], r_rel.at[1], x_peer(1))
    send_x(2, add_share(3, 1), fin.at[1, 1], r_fin.at[1], x_peer(3))
    send_x(3, add_share(1, 0), fin.at[0, 0], r_fin.at[0], x_peer(1))
    lax.fori_loop(7, 8, later, 0)
    send_grads(0)
    send_x(0, add_share(2, 0), rel.at[0], r_rel.at[0], x_peer(3))

    arrived(wt.at[0], r_wt.at[2], "wait_weights")
    for p in (0, 1):
        send_weight(2, 2, p)

    for args in pack_args + key_args + value_args + latent_args:
        sent_to_head(args)

    left(qb.at[pl.ds(0, 3)], s_fw.at[0])
    left(qb.at[pl.ds(0, 3)], s_fw.at[1])
    left(qb.at[pl.ds(0, 8)], s_fw.at[2])
    left(dqs, s_d.at[0])

    def relay_plus():
        value = add_share(1, 1)
        arrived(rel.at[1], r_rel.at[1], "wait_relay")
        send_x(5, value + rel[1].astype(F32), fin.at[1, 0], r_fin.at[1], x_peer(1))

    def relay_minus():
        value = add_share(3, 0)
        arrived(rel.at[0], r_rel.at[0], "wait_relay")
        send_x(4, value + rel[0].astype(F32), fin.at[0, 1], r_fin.at[0], x_peer(3))

    relay_plus()
    relay_minus()

    arrived(wt.at[pl.ds(0, 4)], r_wt.at[3], "wait_weights")
    latent = jnp.zeros((CHUNK, LATENT), F32)
    ropes = jnp.zeros((32, 2 * ROPE), F32)
    for j in (0, 1, 3, 2):
        yj = (y + j) % 4
        arrived(gf.at[pl.ds(4 * yj, 4)], r_g.at[yj], "wait_grads")
        for u in range(4):
            ropes += gf[4 * yj + u, 2 * CHUNK : PIECE].astype(F32)
        for core in (0, 1):
            first, second = 4 * yj + 2 * core, 4 * yj + 2 * core + 1
            for p in (0, 1):
                rows = slice(p * CHUNK, (p + 1) * CHUNK)
                grads = jnp.concatenate([gf[first, rows], gf[second, rows]], axis=1)
                latent += dot(grads, wt[2 * yj + core, p])
    mine = 4 * c + y
    for i in range(8):
        ag[mine, CHUNK * i : CHUNK * (i + 1)] = latent[:, 128 * i : 128 * (i + 1)].astype(BF16)
    ag[mine, 8 * CHUNK : DONE] = ropes.astype(BF16)
    for j in (2, 1, 3):
        remote(ag.at[mine], ag.at[mine], s_ag.at[0], r_ag.at[mine], y_peer(j)).start()
    remote(ag.at[mine], ag.at[mine], s_ag.at[0], r_ag.at[mine], partner).start()
    to_hbm(mine)

    for s in (0, 1):
        arrived(lt.at[s], r_lt.at[s], "wait_latent")
    weight = dot(gs[0, :, CHUNK : 2 * CHUNK].reshape(ROWS, VDIM).T, lt[0])
    weight += dot(gs[1, :, CHUNK : 2 * CHUNK].reshape(ROWS, VDIM).T, lt[1])
    for core in (0, 1):
        dwh[core] = weight[:, 512 * core : 512 * (core + 1)].astype(BF16).T
    to_half = remote(dwh.at[1 - c], dwhr, s_wh.at[0], r_wh.at[0], partner)
    to_half.start()

    arrived(dwhr, r_wh.at[0], "wait_weight")
    weight = (dwh[c].astype(F32) + dwhr[...].astype(F32)).astype(BF16)
    for i in range(8):
        dwx[i % 4, i // 4] = weight[64 * i : 64 * (i + 1)]
    for j in (2, 1, 3):
        xj = (x + j) % 4
        copy = remote(dwx.at[xj], dwxr.at[x], s_wx.at[0], r_wx.at[0], x_peer(j))
        copy.start()

    for s in (0, 1):
        home = add_share(0, s)
        arrived(fin.at[s], r_fin.at[s], "wait_home")
        home += fin[s, 0].astype(F32) + fin[s, 1].astype(F32)
        dqh[s] = (home * SCALE).astype(BF16)
        args = (s, dqh.at[s], dqf.at[e_mine], s_h.at[s], r_h.at[e_mine])
        start_to_owner(args)
        back.append(args)

    weight = dwx[x].astype(F32)
    arrived(dwxr.at[pl.ds(0, 3)], r_wx.at[0], "wait_weight")
    for j in (1, 3, 2):
        weight += dwxr[(x + j) % 4].astype(F32)
    dwz[...] = weight.astype(BF16)

    def weight_home(i):
        row_z = 2 * c + i
        own = (row_z == z) & (z // 2 == c)
        src, dst = dwz.at[i], dwf.at[z % 2]
        copy = remote(src, dst, s_wz.at[i], r_wz.at[z % 2], (4 * row_z + x, 2 * y + z // 2))
        return own, copy, pltpu.make_async_copy(src, dst, r_wz.at[z % 2])

    for i in (0, 1):
        own, copy, local = weight_home(i)

        @pl.when(own)
        def _():
            local.start()

        @pl.when(jnp.logical_not(own))
        def _():
            copy.start()

    for s in (0, 1):
        own = key_z(c, s) == z

        @pl.when(own)
        def _():
            left(gs.at[s, pl.ds(0, 7)], s_g.at[s])

        @pl.when(jnp.logical_not(own))
        def _():
            left(gs.at[s], s_g.at[s])

    left(wt.at[pl.ds(0, 7)], s_wt.at[0])
    left(xs, s_x.at[0])
    left(dwx.at[pl.ds(0, 3)], s_wx.at[0])

    for j in (1, 3, 2):
        i = 4 * c + (y + j) % 4
        arrived(ag.at[i], r_ag.at[i], "wait_chunk")
        remote(ag.at[i], ag.at[i], s_ag.at[0], r_ag.at[i], partner).start()
        to_hbm(i)

    for e in (0, 1):
        arrived(dwf.at[e], r_wz.at[e], "wait_weight")
        dwo[:, e * VDIM : (e + 1) * VDIM] = dwf[e].astype(F32)
    for e in (0, 1):
        arrived(dqf.at[e], r_h.at[e], "wait_queries")
    dqo[...] = jnp.concatenate([dqf[0], dqf[1]], axis=0).T
    stores = [pltpu.make_async_copy(dqo, dq_out, s_out.at[0]), pltpu.make_async_copy(dwo, dw_out, s_out.at[1])]
    for store in stores:
        store.start()
    for i in (0, 1):
        own, copy, _ = weight_home(i)

        @pl.when(jnp.logical_not(own))
        def _():
            copy.wait_send()

    for args in back:
        sent_to_owner(args)
    for j in (0, 1, 3, 2):
        i = 4 * (1 - c) + (y + j) % 4
        arrived(ag.at[i], r_ag.at[i], "wait_other_chunk")
        to_hbm(i)

    with jax.named_scope("last"):
        to_half.wait_send()
        left(ag.at[pl.ds(0, 7)], s_ag.at[0])
        for store in stores:
            store.wait()
        pltpu.make_async_copy(ag, ag_out, s_out.at[2]).wait()


def finish(ag_hbm, dq_hbm, dw_hbm, dlat_hbm, drope_hbm, dq_out, dw_out, ag, dq, dw, dlat, drope, s_in, s_out):
    loads = [pltpu.make_async_copy(ag_hbm.at[i], ag.at[i], s_in.at[i]) for i in range(8)]
    loads += [pltpu.make_async_copy(dq_hbm, dq, s_in.at[8]), pltpu.make_async_copy(dw_hbm, dw, s_in.at[9])]
    for load in loads:
        load.start()
    stores = []
    for i in range(8):
        loads[i].wait()
        rows = pl.ds(CHUNK * i, CHUNK)
        for j in range(8):
            dlat[rows, 128 * j : 128 * (j + 1)] = ag[i, CHUNK * j : CHUNK * (j + 1)].astype(F32)
        stores.append(pltpu.make_async_copy(dlat.at[rows], dlat_hbm.at[rows], s_out.at[i]))
        stores[-1].start()
    for i, src, dst in ((8, dq, dq_out), (9, dw, dw_out)):
        loads[i].wait()
        stores.append(pltpu.make_async_copy(src, dst, s_out.at[i]))
        stores[-1].start()
    ropes = []
    for i in range(8):
        pairs = ag[i, 8 * CHUNK : DONE].T.astype(F32)
        ropes += [pairs[0:ROPE], pairs[ROPE : 2 * ROPE]]
    drope[...] = jnp.concatenate(ropes, axis=1)
    stores.append(pltpu.make_async_copy(drope, drope_hbm, s_out.at[10]))
    stores[-1].start()
    for store in stores:
        store.wait()


def per_device(q, lat, rope, kw, vw, lse, ao, go):
    vmem = pl.BlockSpec(memory_space=pltpu.VMEM)
    anywhere = pl.BlockSpec(memory_space=pl.ANY)

    def buf(*shape, dtype=BF16):
        return pltpu.VMEM(shape, dtype)

    def sem(*shape):
        return pltpu.SemaphoreType.DMA(shape)

    scratch = [
        buf(ROWS, 2 * HEAD), buf(ROWS, LATENT), buf(ROPE, ROWS), buf(LATENT, 256), buf(LATENT, 256),
        buf(2, ROWS, dtype=F32), buf(ROWS, 256), buf(ROWS, 256),
        buf(16, PACK, ROWS), buf(2, PACK, ROWS), buf(2, HEAD, ROWS), buf(2, VDIM, ROWS),
        buf(2, KEY_PACK, ROWS), buf(2, ROWS, GRAD_AT), buf(2, ROWS, KEY_PACK - GRAD_AT),
        buf(2, ROWS, HEAD, dtype=F32), buf(2, ROWS, VDIM, dtype=F32), buf(16, HEAD, ROWS, dtype=F32),
        buf(8, HEAD, ROWS), buf(8, HEAD, ROWS), buf(6, HEAD, ROWS), buf(2, HEAD, ROWS), buf(2, 2, HEAD, ROWS),
        buf(2, HEAD, ROWS), buf(2, HEAD, ROWS), buf(2, 8, PIECE, 128), buf(16, PIECE, 128),
        buf(2, ROWS, LATENT), buf(8, 2, 256, LATENT),
        buf(2, 512, VDIM), buf(512, VDIM), buf(4, 2, 64, VDIM), buf(4, 2, 64, VDIM), buf(2, 64, VDIM), buf(2, 64, VDIM),
        buf(8, DONE, 128), buf(ROWS, 2 * HEAD), buf(64, 256, dtype=F32),
        sem(8), sem(2, 2), sem(2), sem(2), sem(16, 2), sem(2), sem(2), sem(3), sem(1), sem(8), sem(1), sem(2),
        sem(2), sem(2), sem(2), sem(2), sem(4),
        sem(2), sem(2), sem(1), sem(4), sem(1), sem(8), sem(1), sem(1), sem(1), sem(1), sem(2), sem(2), sem(3),
    ]
    ag, dq, dw = pl.pallas_call(
        kernel,
        in_specs=[anywhere] * 8,
        out_specs=[anywhere] * 3,
        out_shape=[
            jax.ShapeDtypeStruct((8, DONE, 128), BF16),
            jax.ShapeDtypeStruct((ROWS, 2 * HEAD), BF16),
            jax.ShapeDtypeStruct((64, 256), F32),
        ],
        scratch_shapes=scratch,
        compiler_params=pltpu.CompilerParams(
            collective_id=0, has_side_effects=True, vmem_limit_bytes=58000 * 1024
        ),
        name="latent_attention_backward",
    )(q, lat, rope.T, kw, vw, lse, ao, go)
    dlat, drope, dq, dw = pl.pallas_call(
        finish,
        in_specs=[anywhere] * 3,
        out_specs=[anywhere] * 4,
        out_shape=[
            jax.ShapeDtypeStruct((ROWS, LATENT), F32),
            jax.ShapeDtypeStruct((ROPE, ROWS), F32),
            jax.ShapeDtypeStruct((ROWS, 2 * HEAD), BF16),
            jax.ShapeDtypeStruct((64, 256), F32),
        ],
        scratch_shapes=[
            buf(8, DONE, 128), buf(ROWS, 2 * HEAD), buf(64, 256, dtype=F32),
            buf(ROWS, LATENT, dtype=F32), buf(ROPE, ROWS, dtype=F32), sem(10), sem(11),
        ],
        compiler_params=pltpu.CompilerParams(vmem_limit_bytes=58000 * 1024),
        name="finish",
    )(ag, dq, dw)
    return dq, dlat, drope.T, dw


def solution(mesh):
    placed = (
        P("sp", "tp"),
        P("sp", None),
        P("sp", None),
        P(None, "tp"),
        P(None, "tp"),
        P("tp", "sp"),
        P("sp", "tp"),
        P("sp", "tp"),
    )
    return jax.shard_map(
        per_device,
        mesh=mesh,
        in_specs=placed,
        out_specs=(P("sp", "tp"), P("sp", None), P("sp", None), P("sp", "tp")),
        check_vma=False,
    )
```

```python
import jax
import jax.numpy as jnp
from jax import lax
from jax.experimental import pallas as pl
from jax.experimental.pallas import tpu as pltpu
from jax.sharding import PartitionSpec as P

NOPE = 128
ROPE = 64
HEAD = NOPE + ROPE
VDIM = 128
ROWS = 512
LATENT = 1024
CHUNK = 64
PIECE = 160
DONE = 544
HALF = 256
SCALE = HEAD**-0.5
LOG2E = 1.4426950408889634
BF16 = jnp.bfloat16
F32 = jnp.float32
MESH = pl.DeviceIdType.MESH
NT = (((1,), (1,)), ((), ()))

LSE_AT, GRAD_AT, PACK = 192, 208, 336
ONES_AT, VALUE_AT, KEY_PACK = 192, 224, 352


def dot(a, b):
    return jnp.dot(a, b, preferred_element_type=F32)


def dot_nt(a, b):
    return lax.dot_general(a, b, NT, preferred_element_type=F32)


def in_three(row):
    high = row.astype(BF16).astype(F32)
    middle = (row - high).astype(BF16).astype(F32)
    return high, middle, row - high - middle


def six_rows(first, second):
    at = lax.broadcasted_iota(jnp.int32, (16, first.shape[1]), 0)
    rows = jnp.zeros(at.shape, F32)
    for i, part in enumerate(in_three(first) + in_three(second)):
        rows = jnp.where(at == i, part, rows)
    return rows.astype(BF16)


def ones_rows(first):
    at = lax.broadcasted_iota(jnp.int32, (16, ROWS), 0)
    return jnp.where((at >= first) & (at < first + 3), 1.0, 0.0).astype(BF16)


def kernel(
    q_hbm, lat_hbm, rope_hbm, kw_hbm, vw_hbm, lse_hbm, ao_hbm, go_hbm,
    ag_out, dq_out, dw_out,
    q, lat, rope, kw, vw, lse, ao, go,
    qb, pk, kts, vts, kv, kaug, vaug, dk, dv, dq,
    dqs, dqr, xs, rel, fin, dqh, dqf, gs, gf, lt, wt,
    dwh, dwhr, dwx, dwxr, dwz, dwf, ag, dqo, dwo,
    s_in, s_pk, s_kt, s_v, r_q, r_kt, r_v, s_fw, s_d, r_d, s_x, r_rel, r_fin, s_h, r_h, s_g, r_g,
    s_lt, r_lt, s_wt, r_wt, s_ag, r_ag, s_wh, r_wh, s_wx, r_wx, s_wz, r_wz, s_out,
):
    sp, tp = lax.axis_index("sp"), lax.axis_index("tp")
    z, x, y, c = sp // 4, sp % 4, tp // 2, tp % 2
    core_of_z = ((z + 1) // 2) % 2
    slot_of_z = z // 2
    partner = (sp, 2 * y + 1 - c)

    def key_z(core, slot):
        return core + slot * (3 - 2 * core)

    def x_peer(j):
        return (4 * z + (x + j) % 4, tp)

    def z_peer(j):
        return (4 * ((z + j) % 4) + x, tp)

    def y_peer(j):
        return (sp, 2 * ((y + j) % 4) + c)

    def remote(src, dst, send, recv, to):
        return pltpu.make_async_remote_copy(
            src_ref=src, dst_ref=dst, send_sem=send, recv_sem=recv, device_id=to, device_id_type=MESH
        )

    def arrived(ref, recv, name="wait"):
        with jax.named_scope(name):
            remote(ref, ref, s_in.at[0], recv, partner).wait_recv()

    def left(ref, send):
        remote(ref, ref, send, s_in.at[0], partner).wait_send()

    barrier = pltpu.get_barrier_semaphore()
    peers = [partner]
    for j in (1, 2, 3):
        peers += [x_peer(j)]
        peers += [(sp, 2 * ((y + j) % 4) + core) for core in (0, 1)]
        peers += [(4 * ((z + j) % 4) + x, 2 * y + core) for core in (0, 1)]
    for peer in peers:
        pl.semaphore_signal(barrier, inc=1, device_id=peer, device_id_type=MESH)

    def load(i):
        pairs = ((q_hbm, q), (go_hbm, go), (ao_hbm, ao), (lse_hbm, lse), (lat_hbm, lat), (kw_hbm, kw), (rope_hbm, rope), (vw_hbm, vw))
        return pltpu.make_async_copy(*pairs[i], s_in.at[i])

    @pl.when(z < 2)
    def _():
        for i in (4, 5, 6, 7, 0, 1, 2, 3):
            load(i).start()

    @pl.when(z >= 2)
    def _():
        for i in range(8):
            load(i).start()

    dk[...] = jnp.zeros_like(dk)
    dv[...] = jnp.zeros_like(dv)
    for s in (0, 1):
        kv[s, ONES_AT : ONES_AT + 16] = ones_rows(0)
        kv[s, ONES_AT + 16 : VALUE_AT] = ones_rows(3)

    def to_head(e, src, dst, send, recv):
        head_z = 2 * c + e
        own = (head_z == z) & (core_of_z == c)
        copy = remote(src, dst, send, recv, (4 * head_z + x, 2 * y + core_of_z))
        return own, copy, pltpu.make_async_copy(src, dst, recv)

    def start_to_head(args):
        own, copy, local = to_head(*args)

        @pl.when(own)
        def _():
            local.start()

        @pl.when(jnp.logical_not(own))
        def _():
            copy.start()

    def sent_to_head(args):
        own, copy, _ = to_head(*args)

        @pl.when(jnp.logical_not(own))
        def _():
            copy.wait_send()

    def half(ref, b, h):
        return ref.at[b, :, pl.ds(HALF * h, HALF)]

    pack_args = [
        (e, half(pk, e, h), half(qb, sp, h), s_pk.at[e, h], r_q.at[sp, h]) for h in (0, 1) for e in (0, 1)
    ]
    key_args = [
        (e, kts.at[e], kv.at[slot_of_z, pl.ds(0, HEAD)], s_kt.at[e], r_kt.at[slot_of_z]) for e in (0, 1)
    ]
    value_args = [
        (e, vts.at[e], kv.at[slot_of_z, pl.ds(VALUE_AT, VDIM)], s_v.at[e], r_v.at[slot_of_z]) for e in (0, 1)
    ]

    latent_args = [(e, lat, lt.at[slot_of_z], s_lt.at[e], r_lt.at[slot_of_z]) for e in (0, 1)]

    def pack_queries():
        for i in range(4):
            load(i).wait()
        qt = q[...].T
        got = go[...].T
        aot = ao[...].T
        for e in (0, 1):
            grad = got[e * VDIM : (e + 1) * VDIM]
            delta = jnp.sum(
                grad.astype(F32) * aot[e * VDIM : (e + 1) * VDIM].astype(F32), axis=0, keepdims=True
            )
            pk[e, 0:LSE_AT] = qt[e * HEAD : (e + 1) * HEAD]
            pk[e, LSE_AT:GRAD_AT] = six_rows(lse[e : e + 1, :] * (-1.0 / SCALE), -delta)
            pk[e, GRAD_AT:PACK] = grad

    def pack_keys():
        for i in range(4, 8):
            load(i).wait()
        keys = dot(lat[...], kw[...]).astype(BF16).T
        for e in (0, 1):
            kts[e, 0:NOPE] = keys[e * NOPE : (e + 1) * NOPE]
            kts[e, NOPE:HEAD] = rope[...]
        values = dot(lat[...], vw[...]).astype(BF16).T
        for e in (0, 1):
            vts[e] = values[e * VDIM : (e + 1) * VDIM]

    def send_queries():
        for args in pack_args:
            start_to_head(args)

    def send_keys():
        for args in key_args + value_args:
            start_to_head(args)

    def weight_copy(kind, dy, p):
        at = 2 * ((y + dy) % 4) + c
        to = (y_peer(1), y_peer(3), partner)[kind]
        return remote(wt.at[at, p], wt.at[at, p], s_wt.at[0], r_wt.at[3 if kind == 2 else 2 if dy else p], to)

    def send_weight(*args):
        copy = weight_copy(*args)
        copy.start()

    def take_weights(p):
        arrived(wt.at[0], r_wt.at[p], "wait_weights")
        for dy in (1, 3):
            send_weight(2, dy, p)
        send_weight(p, 3 - 2 * p, p)

    def send_own_weights(p):
        wt[tp, p] = (kw, vw)[p][...].T
        for kind in (0, 1, 2):
            send_weight(kind, 0, p)

    @pl.when(z < 2)
    def _():
        pack_keys()

    @pl.when(z >= 2)
    def _():
        pack_queries()

    with jax.named_scope("barrier"):
        pl.semaphore_wait(barrier, len(peers))

    @pl.when(z < 2)
    def _():
        send_keys()
        send_own_weights(0)
        pack_queries()
        send_queries()

    @pl.when(z >= 2)
    def _():
        send_queries()
        pack_keys()
        send_own_weights(0)
        send_own_weights(1)
        send_keys()

    @pl.when(z < 2)
    def _():
        send_own_weights(1)

    for args in latent_args:
        start_to_head(args)

    def zero(b, _):
        dq[b] = jnp.zeros((HEAD, ROWS), F32)
        return 0

    lax.fori_loop(0, 16, zero, 0)

    def step(t):
        near = t < 4
        far = t >= 12
        mid = jnp.logical_not(near | far)
        pair = t % 2
        slot = 1 - jnp.where(mid, (t - 4) // 4, (t % 4) // 2)
        other = jnp.where(mid, ((t - 4) // 2) % 2, pair)
        dx = jnp.where(near, 0, jnp.where(far, 2, jnp.where(pair == 0, 3, 1)))
        core = jnp.where(other == 0, c, 1 - c)
        block = 4 * key_z(core, slot) + (x + dx) % 4
        return block, dx, other, slot

    def forwards(t, h):
        b, dx, other, slot = step(t)
        block = half(qb, b, h)
        mine = other == 0
        plus = mine & ((dx == 0) | ((dx == 3) & (slot == 0)))
        minus = mine & ((dx == 0) | ((dx == 1) & (slot == 1)))
        return [
            (plus, remote(block, block, s_fw.at[0], r_q.at[b, h], x_peer(1))),
            (minus, remote(block, block, s_fw.at[1], r_q.at[b, h], x_peer(3))),
            (mine, remote(block, block, s_fw.at[2], r_q.at[b, h], partner)),
        ]

    def take(t):
        b = step(t)[0]
        for h in (0, 1):
            arrived(half(qb, b, h), r_q.at[b, h], "wait_query")
            for holds, copy in forwards(t, h):

                @pl.when(holds)
                def _():
                    copy.start()

    def tile(b, s, masked):
        raw = dot(kaug[s], qb[b, 0:GRAD_AT]) * (SCALE * LOG2E)
        if masked:
            key_row = lax.broadcasted_iota(jnp.int32, (ROWS, ROWS), 0)
            query_row = lax.broadcasted_iota(jnp.int32, (ROWS, ROWS), 1)
            raw = jnp.where(key_row <= query_row, raw, -1e30)
        probs = jnp.exp2(raw)
        diff = dot(vaug[s], qb[b, LSE_AT:PACK])
        grads = (probs * diff).astype(BF16)
        dv[s] += dot_nt(probs.astype(BF16), qb[b, GRAD_AT:PACK])
        dk[s] += dot_nt(grads, qb[b, 0:LSE_AT])
        dq[b] += dot(kv[s, 0:HEAD], grads)

    def to_partner(i):
        return remote(dqs.at[i], dqr.at[i], s_d.at[0], r_d.at[i], partner)

    def share(t):
        b, dx, other, slot = step(t)

        i = 2 * dx + slot
        dqs[i] = dq[b].astype(BF16)
        to_partner(i).start()

    def own_block(s):
        return 4 * key_z(c, s) + x

    def take_keys(s):
        arrived(kv.at[s, pl.ds(0, HEAD)], r_kt.at[s], "wait_keys")
        arrived(kv.at[s, pl.ds(VALUE_AT, VDIM)], r_v.at[s], "wait_values")
        kaug[s] = kv[s, 0:GRAD_AT].T
        vaug[s] = kv[s, GRAD_AT:KEY_PACK].T

    def both_tiles(b):
        probs = [jnp.exp2(dot(kaug[s], qb[b, 0:GRAD_AT]) * (SCALE * LOG2E)) for s in (0, 1)]
        grads = [(probs[s] * dot(vaug[s], qb[b, LSE_AT:PACK])).astype(BF16) for s in (0, 1)]
        for s in (0, 1):
            dv[s] += dot_nt(probs[s].astype(BF16), qb[b, GRAD_AT:PACK])
            dk[s] += dot_nt(grads[s], qb[b, 0:LSE_AT])
        dq[b] += dot(kv[0, 0:HEAD], grads[0]) + dot(kv[1, 0:HEAD], grads[1])

    def tiles(b):
        with jax.named_scope("pair"):

            @pl.when(b > own_block(1))
            def _():
                both_tiles(b)

            @pl.when((b > own_block(0)) & (b < own_block(1)))
            def _():
                tile(b, 0, False)

    def early(t, _):
        @pl.when(t > 0)
        def _():
            take(t)

        with jax.named_scope("early"):
            tile(step(t)[0], 0, False)
        return 0

    def diagonal(s, _):
        tile(own_block(s), s, True)
        return 0

    def later(p, _):
        far = p >= 6
        even = jnp.logical_not(far) & (p % 2 == 0)
        odd = jnp.logical_not(far) & (p % 2 == 1)
        slot = step(2 * p)[3]

        @pl.when(even)
        def _():
            for h in (0, 1):
                for i, back_slot in ((0, 0), (1, 1)):
                    b = step(2 * p + i)[0]
                    block = half(qb, b, h)
                    arrived(block, r_q.at[b, h], "wait_query")

                    @pl.when(slot == back_slot)
                    def _():
                        remote(block, block, s_fw.at[i], r_q.at[b, h], x_peer(1 + 2 * i)).start()

                    remote(block, block, s_fw.at[2], r_q.at[b, h], partner).start()

        @pl.when(odd)
        def _():
            for i in (0, 1):
                b = step(2 * p + i)[0]
                for h in (0, 1):
                    arrived(half(qb, b, h), r_q.at[b, h], "wait_query")

        @pl.when(far)
        def _():
            b = step(2 * p)[0]
            for h in (0, 1):
                block = half(qb, b, h)
                arrived(block, r_q.at[b, h], "wait_query")
                remote(block, block, s_fw.at[2], r_q.at[b, h], partner).start()

        @pl.when(p == 2)
        def _():
            take_weights(0)

        @pl.when(p == 4)
        def _():
            take_weights(1)

        def member(i, _):
            b = step(2 * p + i)[0]

            @pl.when(far & (i == 1))
            def _():
                for h in (0, 1):
                    arrived(half(qb, b, h), r_q.at[b, h], "wait_query")

            tiles(b)
            return 0

        lax.fori_loop(0, 2, member, 0)

        @pl.when(odd)
        def _():
            share(2 * p)

        @pl.when(odd | far)
        def _():
            share(2 * p + 1)

        return 0

    def rest(i, _):
        b = step(1 + 2 * i)[0]

        @pl.when(b > own_block(1 - i))
        def _():
            tile(b, 1 - i, False)

        return 0

    def piece(s, j):
        i = (4 * c + y + j) % 8
        token_z = key_z(c, s)
        to = (4 * token_z + x, 2 * (i % 4) + i // 4)
        src, dst = gs.at[s, i], gf.at[4 * y + z]
        return (
            (token_z == z) if j == 0 else None,
            remote(src, dst, s_g.at[s], r_g.at[y], to),
            pltpu.make_async_copy(src, dst, r_g.at[y]),
        )

    def by_piece(s, j, local_op, remote_op):
        own, copy, local = piece(s, j)
        if own is None:
            remote_op(copy)
            return

        @pl.when(own)
        def _():
            local_op(local)

        @pl.when(jnp.logical_not(own))
        def _():
            remote_op(copy)

    def send_grads(s):
        gs[s, :, 0:CHUNK] = (dk[s, :, 0:NOPE] * SCALE).astype(BF16).reshape(8, CHUNK, NOPE)
        gs[s, :, CHUNK : 2 * CHUNK] = dv[s].astype(BF16).reshape(8, CHUNK, VDIM)
        ropes = (dk[s, :, NOPE:HEAD] * SCALE).astype(BF16).reshape(8, 2, 32, ROPE)
        gs[s, :, 2 * CHUNK : PIECE] = jnp.concatenate([ropes[:, 0], ropes[:, 1]], axis=2)
        for j in range(8):
            by_piece(s, j, lambda local: local.start(), lambda copy: copy.start())

    def to_owner(s, src, dst, send, recv):
        token_z = key_z(c, s)
        own = (token_z == z) & (z // 2 == c)
        copy = remote(src, dst, send, recv, (4 * token_z + x, 2 * y + z // 2))
        return own, copy, pltpu.make_async_copy(src, dst, recv)

    def start_to_owner(args):
        own, copy, local = to_owner(*args)

        @pl.when(own)
        def _():
            local.start()

        @pl.when(jnp.logical_not(own))
        def _():
            copy.start()

    def sent_to_owner(args):
        own, copy, _ = to_owner(*args)

        @pl.when(jnp.logical_not(own))
        def _():
            copy.wait_send()

    e_mine = z % 2
    back = []

    def add_share(dx, s):
        i = 2 * dx + s
        arrived(dqr.at[i], r_d.at[i], "wait_share")
        b = 4 * key_z(c, s) + (x + dx) % 4
        return dq[b] + dqr[i].astype(F32)

    def send_x(i, value, dst, recv, to):
        xs[i] = value.astype(BF16)
        copy = remote(xs.at[i], dst, s_x.at[0], recv, to)
        copy.start()

    def to_hbm(i):
        pltpu.make_async_copy(ag.at[i], ag_out.at[i], s_out.at[2]).start()

    take(0)
    take_keys(0)
    lax.fori_loop(0, 2, early, 0)
    take(2)
    take_keys(1)
    with jax.named_scope("diagonal"):
        lax.fori_loop(0, 2, diagonal, 0)

    take(3)
    lax.fori_loop(0, 2, rest, 0)
    share(1)
    share(3)
    lax.fori_loop(2, 7, later, 0)

    send_grads(1)
    send_x(1, add_share(2, 1), rel.at[1], r_rel.at[1], x_peer(1))
    send_x(2, add_share(3, 1), fin.at[1, 1], r_fin.at[1], x_peer(3))
    send_x(3, add_share(1, 0), fin.at[0, 0], r_fin.at[0], x_peer(1))
    lax.fori_loop(7, 8, later, 0)
    send_grads(0)
    send_x(0, add_share(2, 0), rel.at[0], r_rel.at[0], x_peer(3))

    arrived(wt.at[0], r_wt.at[2], "wait_weights")
    for p in (0, 1):
        send_weight(2, 2, p)

    for args in pack_args + key_args + value_args + latent_args:
        sent_to_head(args)

    left(qb.at[pl.ds(0, 3)], s_fw.at[0])
    left(qb.at[pl.ds(0, 3)], s_fw.at[1])
    left(qb.at[pl.ds(0, 8)], s_fw.at[2])
    left(dqs, s_d.at[0])

    def relay_plus():
        value = add_share(1, 1)
        arrived(rel.at[1], r_rel.at[1], "wait_relay")
        send_x(5, value + rel[1].astype(F32), fin.at[1, 0], r_fin.at[1], x_peer(1))

    def relay_minus():
        value = add_share(3, 0)
        arrived(rel.at[0], r_rel.at[0], "wait_relay")
        send_x(4, value + rel[0].astype(F32), fin.at[0, 1], r_fin.at[0], x_peer(3))

    relay_plus()
    relay_minus()

    arrived(wt.at[pl.ds(0, 4)], r_wt.at[3], "wait_weights")
    latent = jnp.zeros((CHUNK, LATENT), F32)
    ropes = jnp.zeros((32, 2 * ROPE), F32)
    for j in (0, 1, 3, 2):
        yj = (y + j) % 4
        arrived(gf.at[pl.ds(4 * yj, 4)], r_g.at[yj], "wait_grads")
        for u in range(4):
            ropes += gf[4 * yj + u, 2 * CHUNK : PIECE].astype(F32)
        for core in (0, 1):
            first, second = 4 * yj + 2 * core, 4 * yj + 2 * core + 1
            for p in (0, 1):
                rows = slice(p * CHUNK, (p + 1) * CHUNK)
                grads = jnp.concatenate([gf[first, rows], gf[second, rows]], axis=1)
                latent += dot(grads, wt[2 * yj + core, p])
    mine = 4 * c + y
    for i in range(8):
        ag[mine, CHUNK * i : CHUNK * (i + 1)] = latent[:, 128 * i : 128 * (i + 1)].astype(BF16)
    ag[mine, 8 * CHUNK : DONE] = ropes.astype(BF16)
    for j in (2, 1, 3):
        remote(ag.at[mine], ag.at[mine], s_ag.at[0], r_ag.at[mine], y_peer(j)).start()
    remote(ag.at[mine], ag_out.at[mine], s_ag.at[0], r_ag.at[mine], partner).start()
    to_hbm(mine)

    for s in (0, 1):
        arrived(lt.at[s], r_lt.at[s], "wait_latent")
    weight = dot(gs[0, :, CHUNK : 2 * CHUNK].reshape(ROWS, VDIM).T, lt[0])
    weight += dot(gs[1, :, CHUNK : 2 * CHUNK].reshape(ROWS, VDIM).T, lt[1])
    for core in (0, 1):
        dwh[core] = weight[:, 512 * core : 512 * (core + 1)].astype(BF16).T
    to_half = remote(dwh.at[1 - c], dwhr, s_wh.at[0], r_wh.at[0], partner)
    to_half.start()

    arrived(dwhr, r_wh.at[0], "wait_weight")
    weight = (dwh[c].astype(F32) + dwhr[...].astype(F32)).astype(BF16)
    for i in range(8):
        dwx[i % 4, i // 4] = weight[64 * i : 64 * (i + 1)]
    for j in (2, 1, 3):
        xj = (x + j) % 4
        copy = remote(dwx.at[xj], dwxr.at[x], s_wx.at[0], r_wx.at[0], x_peer(j))
        copy.start()

    for s in (0, 1):
        home = add_share(0, s)
        arrived(fin.at[s], r_fin.at[s], "wait_home")
        home += fin[s, 0].astype(F32) + fin[s, 1].astype(F32)
        dqh[s] = (home * SCALE).astype(BF16)
        args = (s, dqh.at[s], dqf.at[e_mine], s_h.at[s], r_h.at[e_mine])
        start_to_owner(args)
        back.append(args)

    weight = dwx[x].astype(F32)
    arrived(dwxr.at[pl.ds(0, 3)], r_wx.at[0], "wait_weight")
    for j in (1, 3, 2):
        weight += dwxr[(x + j) % 4].astype(F32)
    dwz[...] = weight.astype(BF16)

    def weight_home(i):
        row_z = 2 * c + i
        own = (row_z == z) & (z // 2 == c)
        src, dst = dwz.at[i], dwf.at[z % 2]
        copy = remote(src, dst, s_wz.at[i], r_wz.at[z % 2], (4 * row_z + x, 2 * y + z // 2))
        return own, copy, pltpu.make_async_copy(src, dst, r_wz.at[z % 2])

    for i in (0, 1):
        own, copy, local = weight_home(i)

        @pl.when(own)
        def _():
            local.start()

        @pl.when(jnp.logical_not(own))
        def _():
            copy.start()

    for s in (0, 1):
        own = key_z(c, s) == z

        @pl.when(own)
        def _():
            left(gs.at[s, pl.ds(0, 7)], s_g.at[s])

        @pl.when(jnp.logical_not(own))
        def _():
            left(gs.at[s], s_g.at[s])

    left(wt.at[pl.ds(0, 7)], s_wt.at[0])
    left(xs, s_x.at[0])
    left(dwx.at[pl.ds(0, 3)], s_wx.at[0])

    for j in (1, 3, 2):
        i = 4 * c + (y + j) % 4
        arrived(ag.at[i], r_ag.at[i], "wait_chunk")
        remote(ag.at[i], ag_out.at[i], s_ag.at[0], r_ag.at[i], partner).start()
        to_hbm(i)

    for e in (0, 1):
        arrived(dwf.at[e], r_wz.at[e], "wait_weight")
        dwo[:, e * VDIM : (e + 1) * VDIM] = dwf[e].astype(F32)
    for e in (0, 1):
        arrived(dqf.at[e], r_h.at[e], "wait_queries")
    dqo[...] = jnp.concatenate([dqf[0], dqf[1]], axis=0).T
    stores = [pltpu.make_async_copy(dqo, dq_out, s_out.at[0]), pltpu.make_async_copy(dwo, dw_out, s_out.at[1])]
    for store in stores:
        store.start()
    for i in (0, 1):
        own, copy, _ = weight_home(i)

        @pl.when(jnp.logical_not(own))
        def _():
            copy.wait_send()

    for args in back:
        sent_to_owner(args)
    for j in (0, 1, 3, 2):
        i = 4 * (1 - c) + (y + j) % 4
        arrived(ag_out.at[i], r_ag.at[i], "wait_other_chunk")

    with jax.named_scope("last"):
        to_half.wait_send()
        left(ag.at[pl.ds(0, 7)], s_ag.at[0])
        for store in stores:
            store.wait()
        pltpu.make_async_copy(ag.at[pl.ds(0, 4)], ag_out.at[pl.ds(0, 4)], s_out.at[2]).wait()


def finish(ag_hbm, dq_hbm, dw_hbm, dlat_hbm, drope_hbm, dq_out, dw_out, ag, dq, dw, dlat, drope, s_in, s_out):
    loads = [pltpu.make_async_copy(ag_hbm.at[i], ag.at[i], s_in.at[i]) for i in range(8)]
    loads += [pltpu.make_async_copy(dq_hbm, dq, s_in.at[8]), pltpu.make_async_copy(dw_hbm, dw, s_in.at[9])]
    for load in loads:
        load.start()
    stores = []
    for i in range(8):
        loads[i].wait()
        rows = pl.ds(CHUNK * i, CHUNK)
        for j in range(8):
            dlat[rows, 128 * j : 128 * (j + 1)] = ag[i, CHUNK * j : CHUNK * (j + 1)].astype(F32)
        stores.append(pltpu.make_async_copy(dlat.at[rows], dlat_hbm.at[rows], s_out.at[i]))
        stores[-1].start()
    for i, src, dst in ((8, dq, dq_out), (9, dw, dw_out)):
        loads[i].wait()
        stores.append(pltpu.make_async_copy(src, dst, s_out.at[i]))
        stores[-1].start()
    ropes = []
    for i in range(8):
        pairs = ag[i, 8 * CHUNK : DONE].T.astype(F32)
        ropes += [pairs[0:ROPE], pairs[ROPE : 2 * ROPE]]
    drope[...] = jnp.concatenate(ropes, axis=1)
    stores.append(pltpu.make_async_copy(drope, drope_hbm, s_out.at[10]))
    stores[-1].start()
    for store in stores:
        store.wait()


def per_device(q, lat, rope, kw, vw, lse, ao, go):
    vmem = pl.BlockSpec(memory_space=pltpu.VMEM)
    anywhere = pl.BlockSpec(memory_space=pl.ANY)

    def buf(*shape, dtype=BF16):
        return pltpu.VMEM(shape, dtype)

    def sem(*shape):
        return pltpu.SemaphoreType.DMA(shape)

    scratch = [
        buf(ROWS, 2 * HEAD), buf(ROWS, LATENT), buf(ROPE, ROWS), buf(LATENT, 256), buf(LATENT, 256),
        buf(2, ROWS, dtype=F32), buf(ROWS, 256), buf(ROWS, 256),
        buf(16, PACK, ROWS), buf(2, PACK, ROWS), buf(2, HEAD, ROWS), buf(2, VDIM, ROWS),
        buf(2, KEY_PACK, ROWS), buf(2, ROWS, GRAD_AT), buf(2, ROWS, KEY_PACK - GRAD_AT),
        buf(2, ROWS, HEAD, dtype=F32), buf(2, ROWS, VDIM, dtype=F32), buf(16, HEAD, ROWS, dtype=F32),
        buf(8, HEAD, ROWS), buf(8, HEAD, ROWS), buf(6, HEAD, ROWS), buf(2, HEAD, ROWS), buf(2, 2, HEAD, ROWS),
        buf(2, HEAD, ROWS), buf(2, HEAD, ROWS), buf(2, 8, PIECE, 128), buf(16, PIECE, 128),
        buf(2, ROWS, LATENT), buf(8, 2, 256, LATENT),
        buf(2, 512, VDIM), buf(512, VDIM), buf(4, 2, 64, VDIM), buf(4, 2, 64, VDIM), buf(2, 64, VDIM), buf(2, 64, VDIM),
        buf(8, DONE, 128), buf(ROWS, 2 * HEAD), buf(64, 256, dtype=F32),
        sem(8), sem(2, 2), sem(2), sem(2), sem(16, 2), sem(2), sem(2), sem(3), sem(1), sem(8), sem(1), sem(2),
        sem(2), sem(2), sem(2), sem(2), sem(4),
        sem(2), sem(2), sem(1), sem(4), sem(1), sem(8), sem(1), sem(1), sem(1), sem(1), sem(2), sem(2), sem(3),
    ]
    ag, dq, dw = pl.pallas_call(
        kernel,
        in_specs=[anywhere] * 8,
        out_specs=[anywhere] * 3,
        out_shape=[
            jax.ShapeDtypeStruct((8, DONE, 128), BF16),
            jax.ShapeDtypeStruct((ROWS, 2 * HEAD), BF16),
            jax.ShapeDtypeStruct((64, 256), F32),
        ],
        scratch_shapes=scratch,
        compiler_params=pltpu.CompilerParams(
            collective_id=0, has_side_effects=True, vmem_limit_bytes=58000 * 1024
        ),
        name="latent_attention_backward",
    )(q, lat, rope.T, kw, vw, lse, ao, go)
    dlat, drope, dq, dw = pl.pallas_call(
        finish,
        in_specs=[anywhere] * 3,
        out_specs=[anywhere] * 4,
        out_shape=[
            jax.ShapeDtypeStruct((ROWS, LATENT), F32),
            jax.ShapeDtypeStruct((ROPE, ROWS), F32),
            jax.ShapeDtypeStruct((ROWS, 2 * HEAD), BF16),
            jax.ShapeDtypeStruct((64, 256), F32),
        ],
        scratch_shapes=[
            buf(8, DONE, 128), buf(ROWS, 2 * HEAD), buf(64, 256, dtype=F32),
            buf(ROWS, LATENT, dtype=F32), buf(ROPE, ROWS, dtype=F32), sem(10), sem(11),
        ],
        compiler_params=pltpu.CompilerParams(vmem_limit_bytes=58000 * 1024),
        name="finish",
    )(ag, dq, dw)
    return dq, dlat, drope.T, dw


def solution(mesh):
    placed = (
        P("sp", "tp"),
        P("sp", None),
        P("sp", None),
        P(None, "tp"),
        P(None, "tp"),
        P("tp", "sp"),
        P("sp", "tp"),
        P("sp", "tp"),
    )
    return jax.shard_map(
        per_device,
        mesh=mesh,
        in_specs=placed,
        out_specs=(P("sp", "tp"), P("sp", None), P("sp", None), P("sp", "tp")),
        check_vma=False,
    )
```

```python
import jax
import jax.numpy as jnp
from jax import lax
from jax.experimental import pallas as pl
from jax.experimental.pallas import tpu as pltpu
from jax.sharding import PartitionSpec as P

NOPE = 128
ROPE = 64
HEAD = NOPE + ROPE
VDIM = 128
ROWS = 512
LATENT = 1024
CHUNK = 64
PIECE = 160
DONE = 544
HALF = 256
SCALE = HEAD**-0.5
LOG2E = 1.4426950408889634
BF16 = jnp.bfloat16
F32 = jnp.float32
MESH = pl.DeviceIdType.MESH
NT = (((1,), (1,)), ((), ()))

LSE_AT, GRAD_AT, PACK = 192, 208, 336
ONES_AT, VALUE_AT, KEY_PACK = 192, 224, 352


def dot(a, b):
    return jnp.dot(a, b, preferred_element_type=F32)


def dot_nt(a, b):
    return lax.dot_general(a, b, NT, preferred_element_type=F32)


def in_three(row):
    high = row.astype(BF16).astype(F32)
    middle = (row - high).astype(BF16).astype(F32)
    return high, middle, row - high - middle


def six_rows(first, second):
    at = lax.broadcasted_iota(jnp.int32, (16, first.shape[1]), 0)
    rows = jnp.zeros(at.shape, F32)
    for i, part in enumerate(in_three(first) + in_three(second)):
        rows = jnp.where(at == i, part, rows)
    return rows.astype(BF16)


def ones_rows(first):
    at = lax.broadcasted_iota(jnp.int32, (16, ROWS), 0)
    return jnp.where((at >= first) & (at < first + 3), 1.0, 0.0).astype(BF16)


def kernel(
    q_hbm, lat_hbm, rope_hbm, kw_hbm, vw_hbm, lse_hbm, ao_hbm, go_hbm,
    ag_out, dq_out, dw_out,
    q, lat, rope, kw, vw, lse, ao, go,
    qb, pk, kts, vts, kv, kaug, vaug, dk, dv, dq,
    dqs, dqr, xs, rel, fin, dqh, dqf, gs, gf, lt, wt,
    dwh, dwhr, dwx, dwxr, dwz, dwf, ag, dqo, dwo,
    s_in, s_pk, s_kt, s_v, r_q, r_kt, r_v, s_fw, s_d, r_d, s_x, r_rel, r_fin, s_h, r_h, s_g, r_g,
    s_lt, r_lt, s_wt, r_wt, s_ag, r_ag, s_wh, r_wh, s_wx, r_wx, s_wz, r_wz, s_out,
):
    sp, tp = lax.axis_index("sp"), lax.axis_index("tp")
    z, x, y, c = sp // 4, sp % 4, tp // 2, tp % 2
    core_of_z = ((z + 1) // 2) % 2
    slot_of_z = z // 2
    partner = (sp, 2 * y + 1 - c)

    def key_z(core, slot):
        return core + slot * (3 - 2 * core)

    def x_peer(j):
        return (4 * z + (x + j) % 4, tp)

    def z_peer(j):
        return (4 * ((z + j) % 4) + x, tp)

    def y_peer(j):
        return (sp, 2 * ((y + j) % 4) + c)

    def remote(src, dst, send, recv, to):
        return pltpu.make_async_remote_copy(
            src_ref=src, dst_ref=dst, send_sem=send, recv_sem=recv, device_id=to, device_id_type=MESH
        )

    def arrived(ref, recv, name="wait"):
        with jax.named_scope(name):
            remote(ref, ref, s_in.at[0], recv, partner).wait_recv()

    def left(ref, send):
        remote(ref, ref, send, s_in.at[0], partner).wait_send()

    barrier = pltpu.get_barrier_semaphore()
    peers = [partner]
    for j in (1, 2, 3):
        peers += [x_peer(j)]
        peers += [(sp, 2 * ((y + j) % 4) + core) for core in (0, 1)]
        peers += [(4 * ((z + j) % 4) + x, 2 * y + core) for core in (0, 1)]
    for peer in peers:
        pl.semaphore_signal(barrier, inc=1, device_id=peer, device_id_type=MESH)

    def load(i):
        pairs = ((q_hbm, q), (go_hbm, go), (ao_hbm, ao), (lse_hbm, lse), (lat_hbm, lat), (kw_hbm, kw), (rope_hbm, rope), (vw_hbm, vw))
        return pltpu.make_async_copy(*pairs[i], s_in.at[i])

    @pl.when(z < 2)
    def _():
        for i in (4, 5, 6, 7, 0, 1, 2, 3):
            load(i).start()

    @pl.when(z >= 2)
    def _():
        for i in range(8):
            load(i).start()

    dk[...] = jnp.zeros_like(dk)
    dv[...] = jnp.zeros_like(dv)
    for s in (0, 1):
        kv[s, ONES_AT : ONES_AT + 16] = ones_rows(0)
        kv[s, ONES_AT + 16 : VALUE_AT] = ones_rows(3)

    def to_head(e, src, dst, send, recv):
        head_z = 2 * c + e
        own = (head_z == z) & (core_of_z == c)
        copy = remote(src, dst, send, recv, (4 * head_z + x, 2 * y + core_of_z))
        return own, copy, pltpu.make_async_copy(src, dst, recv)

    def start_to_head(args):
        own, copy, local = to_head(*args)

        @pl.when(own)
        def _():
            local.start()

        @pl.when(jnp.logical_not(own))
        def _():
            copy.start()

    def sent_to_head(args):
        own, copy, _ = to_head(*args)

        @pl.when(jnp.logical_not(own))
        def _():
            copy.wait_send()

    def half(ref, b, h):
        return ref.at[b, :, pl.ds(HALF * h, HALF)]

    pack_args = [
        (e, half(pk, e, h), half(qb, sp, h), s_pk.at[e, h], r_q.at[sp, h]) for h in (0, 1) for e in (0, 1)
    ]
    key_args = [
        (e, kts.at[e], kv.at[slot_of_z, pl.ds(0, HEAD)], s_kt.at[e], r_kt.at[slot_of_z]) for e in (0, 1)
    ]
    value_args = [
        (e, vts.at[e], kv.at[slot_of_z, pl.ds(VALUE_AT, VDIM)], s_v.at[e], r_v.at[slot_of_z]) for e in (0, 1)
    ]

    latent_args = [(e, lat, lt.at[slot_of_z], s_lt.at[e], r_lt.at[slot_of_z]) for e in (0, 1)]

    def pack_queries():
        for i in range(4):
            load(i).wait()
        qt = q[...].T
        got = go[...].T
        aot = ao[...].T
        for e in (0, 1):
            grad = got[e * VDIM : (e + 1) * VDIM]
            delta = jnp.sum(
                grad.astype(F32) * aot[e * VDIM : (e + 1) * VDIM].astype(F32), axis=0, keepdims=True
            )
            pk[e, 0:LSE_AT] = qt[e * HEAD : (e + 1) * HEAD]
            pk[e, LSE_AT:GRAD_AT] = six_rows(lse[e : e + 1, :] * (-1.0 / SCALE), -delta)
            pk[e, GRAD_AT:PACK] = grad

    def pack_keys():
        for i in range(4, 8):
            load(i).wait()
        keys = dot(lat[...], kw[...]).astype(BF16).T
        for e in (0, 1):
            kts[e, 0:NOPE] = keys[e * NOPE : (e + 1) * NOPE]
            kts[e, NOPE:HEAD] = rope[...]
        values = dot(lat[...], vw[...]).astype(BF16).T
        for e in (0, 1):
            vts[e] = values[e * VDIM : (e + 1) * VDIM]

    def send_queries():
        for args in pack_args:
            start_to_head(args)

    def send_keys():
        for args in key_args + value_args:
            start_to_head(args)

    def weight_copy(kind, dy, p):
        at = 2 * ((y + dy) % 4) + c
        to = (y_peer(1), y_peer(3), partner)[kind]
        return remote(wt.at[at, p], wt.at[at, p], s_wt.at[0], r_wt.at[3 if kind == 2 else 2 if dy else p], to)

    def send_weight(*args):
        copy = weight_copy(*args)
        copy.start()

    def take_weights(p):
        arrived(wt.at[0], r_wt.at[p], "wait_weights")
        for dy in (1, 3):
            send_weight(2, dy, p)
        send_weight(p, 3 - 2 * p, p)

    def send_own_weights(p):
        wt[tp, p] = (kw, vw)[p][...].T
        for kind in (0, 1, 2):
            send_weight(kind, 0, p)

    @pl.when(z < 2)
    def _():
        pack_keys()

    @pl.when(z >= 2)
    def _():
        pack_queries()

    with jax.named_scope("barrier"):
        pl.semaphore_wait(barrier, len(peers))

    @pl.when(z < 2)
    def _():
        send_keys()
        send_own_weights(0)
        pack_queries()
        send_queries()

    @pl.when(z >= 2)
    def _():
        send_queries()
        pack_keys()
        send_own_weights(0)
        send_own_weights(1)
        send_keys()

    @pl.when(z < 2)
    def _():
        send_own_weights(1)

    for args in latent_args:
        start_to_head(args)

    def zero(b, _):
        dq[b] = jnp.zeros((HEAD, ROWS), F32)
        return 0

    lax.fori_loop(0, 16, zero, 0)

    def step(t):
        near = t < 4
        far = t >= 12
        mid = jnp.logical_not(near | far)
        pair = t % 2
        slot = 1 - jnp.where(mid, (t - 4) // 4, (t % 4) // 2)
        other = jnp.where(mid, ((t - 4) // 2) % 2, pair)
        dx = jnp.where(near, 0, jnp.where(far, 2, jnp.where(pair == 0, 3, 1)))
        core = jnp.where(other == 0, c, 1 - c)
        block = 4 * key_z(core, slot) + (x + dx) % 4
        return block, dx, other, slot

    def forwards(t, h):
        b, dx, other, slot = step(t)
        block = half(qb, b, h)
        mine = other == 0
        plus = mine & ((dx == 0) | ((dx == 3) & (slot == 0)))
        minus = mine & ((dx == 0) | ((dx == 1) & (slot == 1)))
        return [
            (plus, remote(block, block, s_fw.at[0], r_q.at[b, h], x_peer(1))),
            (minus, remote(block, block, s_fw.at[1], r_q.at[b, h], x_peer(3))),
            (mine, remote(block, block, s_fw.at[2], r_q.at[b, h], partner)),
        ]

    def take(t):
        b = step(t)[0]
        for h in (0, 1):
            arrived(half(qb, b, h), r_q.at[b, h], "wait_query")
            for holds, copy in forwards(t, h):

                @pl.when(holds)
                def _():
                    copy.start()

    def tile(b, s, masked):
        raw = dot(kaug[s], qb[b, 0:GRAD_AT]) * (SCALE * LOG2E)
        if masked:
            key_row = lax.broadcasted_iota(jnp.int32, (ROWS, ROWS), 0)
            query_row = lax.broadcasted_iota(jnp.int32, (ROWS, ROWS), 1)
            raw = jnp.where(key_row <= query_row, raw, -1e30)
        probs = jnp.exp2(raw)
        diff = dot(vaug[s], qb[b, LSE_AT:PACK])
        grads = (probs * diff).astype(BF16)
        dv[s] += dot_nt(probs.astype(BF16), qb[b, GRAD_AT:PACK])
        dk[s] += dot_nt(grads, qb[b, 0:LSE_AT])
        dq[b] += dot(kv[s, 0:HEAD], grads)

    def to_partner(i):
        return remote(dqs.at[i], dqr.at[i], s_d.at[0], r_d.at[i], partner)

    def share(t):
        b, dx, other, slot = step(t)

        i = 2 * dx + slot
        dqs[i] = dq[b].astype(BF16)
        to_partner(i).start()

    def own_block(s):
        return 4 * key_z(c, s) + x

    def take_keys(s):
        arrived(kv.at[s, pl.ds(0, HEAD)], r_kt.at[s], "wait_keys")
        arrived(kv.at[s, pl.ds(VALUE_AT, VDIM)], r_v.at[s], "wait_values")
        kaug[s] = kv[s, 0:GRAD_AT].T
        vaug[s] = kv[s, GRAD_AT:KEY_PACK].T

    def both_tiles(b):
        probs = [jnp.exp2(dot(kaug[s], qb[b, 0:GRAD_AT]) * (SCALE * LOG2E)) for s in (0, 1)]
        grads = [(probs[s] * dot(vaug[s], qb[b, LSE_AT:PACK])).astype(BF16) for s in (0, 1)]
        for s in (0, 1):
            dv[s] += dot_nt(probs[s].astype(BF16), qb[b, GRAD_AT:PACK])
            dk[s] += dot_nt(grads[s], qb[b, 0:LSE_AT])
        dq[b] += dot(kv[0, 0:HEAD], grads[0]) + dot(kv[1, 0:HEAD], grads[1])

    def tiles(b):
        with jax.named_scope("pair"):

            @pl.when(b > own_block(1))
            def _():
                both_tiles(b)

            @pl.when((b > own_block(0)) & (b < own_block(1)))
            def _():
                tile(b, 0, False)

    def early(t, _):
        @pl.when(t > 0)
        def _():
            take(t)

        with jax.named_scope("early"):
            tile(step(t)[0], 0, False)
        return 0

    def diagonal(s, _):
        tile(own_block(s), s, True)
        return 0

    def later(p, _):
        far = p >= 6
        even = jnp.logical_not(far) & (p % 2 == 0)
        odd = jnp.logical_not(far) & (p % 2 == 1)
        slot = step(2 * p)[3]

        @pl.when(even)
        def _():
            for h in (0, 1):
                for i, back_slot in ((0, 0), (1, 1)):
                    b = step(2 * p + i)[0]
                    block = half(qb, b, h)
                    arrived(block, r_q.at[b, h], "wait_query")

                    @pl.when(slot == back_slot)
                    def _():
                        remote(block, block, s_fw.at[i], r_q.at[b, h], x_peer(1 + 2 * i)).start()

                    remote(block, block, s_fw.at[2], r_q.at[b, h], partner).start()

        @pl.when(odd)
        def _():
            for i in (0, 1):
                b = step(2 * p + i)[0]
                for h in (0, 1):
                    arrived(half(qb, b, h), r_q.at[b, h], "wait_query")

        @pl.when(far)
        def _():
            b = step(2 * p)[0]
            for h in (0, 1):
                block = half(qb, b, h)
                arrived(block, r_q.at[b, h], "wait_query")
                remote(block, block, s_fw.at[2], r_q.at[b, h], partner).start()

        @pl.when(p == 2)
        def _():
            take_weights(0)

        @pl.when(p == 4)
        def _():
            take_weights(1)

        def member(i, _):
            b = step(2 * p + i)[0]

            @pl.when(far & (i == 1))
            def _():
                for h in (0, 1):
                    arrived(half(qb, b, h), r_q.at[b, h], "wait_query")

            tiles(b)
            return 0

        lax.fori_loop(0, 2, member, 0)

        @pl.when(odd)
        def _():
            share(2 * p)

        @pl.when(odd | far)
        def _():
            share(2 * p + 1)

        return 0

    def rest(i, _):
        b = step(1 + 2 * i)[0]

        @pl.when(b > own_block(1 - i))
        def _():
            tile(b, 1 - i, False)

        return 0

    def piece(s, j):
        i = (4 * c + y + j) % 8
        token_z = key_z(c, s)
        to = (4 * token_z + x, 2 * (i % 4) + i // 4)
        src, dst = gs.at[s, i], gf.at[4 * y + z]
        return (
            (token_z == z) if j == 0 else None,
            remote(src, dst, s_g.at[s], r_g.at[y], to),
            pltpu.make_async_copy(src, dst, r_g.at[y]),
        )

    def by_piece(s, j, local_op, remote_op):
        own, copy, local = piece(s, j)
        if own is None:
            remote_op(copy)
            return

        @pl.when(own)
        def _():
            local_op(local)

        @pl.when(jnp.logical_not(own))
        def _():
            remote_op(copy)

    def send_grads(s):
        gs[s, :, 0:CHUNK] = (dk[s, :, 0:NOPE] * SCALE).astype(BF16).reshape(8, CHUNK, NOPE)
        gs[s, :, CHUNK : 2 * CHUNK] = dv[s].astype(BF16).reshape(8, CHUNK, VDIM)
        ropes = (dk[s, :, NOPE:HEAD] * SCALE).astype(BF16).reshape(8, 2, 32, ROPE)
        gs[s, :, 2 * CHUNK : PIECE] = jnp.concatenate([ropes[:, 0], ropes[:, 1]], axis=2)
        for j in (2, 6, 1, 5, 3, 7, 4, 0):
            by_piece(s, j, lambda local: local.start(), lambda copy: copy.start())

    def to_owner(s, src, dst, send, recv):
        token_z = key_z(c, s)
        own = (token_z == z) & (z // 2 == c)
        copy = remote(src, dst, send, recv, (4 * token_z + x, 2 * y + z // 2))
        return own, copy, pltpu.make_async_copy(src, dst, recv)

    def start_to_owner(args):
        own, copy, local = to_owner(*args)

        @pl.when(own)
        def _():
            local.start()

        @pl.when(jnp.logical_not(own))
        def _():
            copy.start()

    def sent_to_owner(args):
        own, copy, _ = to_owner(*args)

        @pl.when(jnp.logical_not(own))
        def _():
            copy.wait_send()

    e_mine = z % 2
    back = []

    def add_share(dx, s):
        i = 2 * dx + s
        arrived(dqr.at[i], r_d.at[i], "wait_share")
        b = 4 * key_z(c, s) + (x + dx) % 4
        return dq[b] + dqr[i].astype(F32)

    def send_x(i, value, dst, recv, to):
        xs[i] = value.astype(BF16)
        copy = remote(xs.at[i], dst, s_x.at[0], recv, to)
        copy.start()

    def to_hbm(i):
        pltpu.make_async_copy(ag.at[i], ag_out.at[i], s_out.at[2]).start()

    take(0)
    take_keys(0)
    lax.fori_loop(0, 2, early, 0)
    take(2)
    take_keys(1)
    with jax.named_scope("diagonal"):
        lax.fori_loop(0, 2, diagonal, 0)

    take(3)
    lax.fori_loop(0, 2, rest, 0)
    share(1)
    share(3)
    lax.fori_loop(2, 7, later, 0)

    send_grads(1)
    send_x(1, add_share(2, 1), rel.at[1], r_rel.at[1], x_peer(1))
    send_x(2, add_share(3, 1), fin.at[1, 1], r_fin.at[1], x_peer(3))
    send_x(3, add_share(1, 0), fin.at[0, 0], r_fin.at[0], x_peer(1))
    lax.fori_loop(7, 8, later, 0)
    send_grads(0)
    send_x(0, add_share(2, 0), rel.at[0], r_rel.at[0], x_peer(3))

    arrived(wt.at[0], r_wt.at[2], "wait_weights")
    for p in (0, 1):
        send_weight(2, 2, p)

    for args in pack_args + key_args + value_args + latent_args:
        sent_to_head(args)

    left(qb.at[pl.ds(0, 3)], s_fw.at[0])
    left(qb.at[pl.ds(0, 3)], s_fw.at[1])
    left(qb.at[pl.ds(0, 8)], s_fw.at[2])
    left(dqs, s_d.at[0])

    def relay_plus():
        value = add_share(1, 1)
        arrived(rel.at[1], r_rel.at[1], "wait_relay")
        send_x(5, value + rel[1].astype(F32), fin.at[1, 0], r_fin.at[1], x_peer(1))

    def relay_minus():
        value = add_share(3, 0)
        arrived(rel.at[0], r_rel.at[0], "wait_relay")
        send_x(4, value + rel[0].astype(F32), fin.at[0, 1], r_fin.at[0], x_peer(3))

    relay_plus()
    relay_minus()

    arrived(wt.at[pl.ds(0, 4)], r_wt.at[3], "wait_weights")
    latent = jnp.zeros((CHUNK, LATENT), F32)
    ropes = jnp.zeros((32, 2 * ROPE), F32)
    for j in (0, 1, 3, 2):
        yj = (y + j) % 4
        arrived(gf.at[pl.ds(4 * yj, 4)], r_g.at[yj], "wait_grads")
        for u in range(4):
            ropes += gf[4 * yj + u, 2 * CHUNK : PIECE].astype(F32)
        for core in (0, 1):
            first, second = 4 * yj + 2 * core, 4 * yj + 2 * core + 1
            for p in (0, 1):
                rows = slice(p * CHUNK, (p + 1) * CHUNK)
                grads = jnp.concatenate([gf[first, rows], gf[second, rows]], axis=1)
                latent += dot(grads, wt[2 * yj + core, p])
    mine = 4 * c + y
    for i in range(8):
        ag[mine, CHUNK * i : CHUNK * (i + 1)] = latent[:, 128 * i : 128 * (i + 1)].astype(BF16)
    ag[mine, 8 * CHUNK : DONE] = ropes.astype(BF16)
    for j in (2, 1, 3):
        remote(ag.at[mine], ag.at[mine], s_ag.at[0], r_ag.at[mine], y_peer(j)).start()
    remote(ag.at[mine], ag_out.at[mine], s_ag.at[0], r_ag.at[mine], partner).start()
    to_hbm(mine)

    for s in (0, 1):
        arrived(lt.at[s], r_lt.at[s], "wait_latent")
    weight = dot(gs[0, :, CHUNK : 2 * CHUNK].reshape(ROWS, VDIM).T, lt[0])
    weight += dot(gs[1, :, CHUNK : 2 * CHUNK].reshape(ROWS, VDIM).T, lt[1])
    for core in (0, 1):
        dwh[core] = weight[:, 512 * core : 512 * (core + 1)].astype(BF16).T
    to_half = remote(dwh.at[1 - c], dwhr, s_wh.at[0], r_wh.at[0], partner)
    to_half.start()

    arrived(dwhr, r_wh.at[0], "wait_weight")
    weight = (dwh[c].astype(F32) + dwhr[...].astype(F32)).astype(BF16)
    for i in range(8):
        dwx[i % 4, i // 4] = weight[64 * i : 64 * (i + 1)]
    for j in (2, 1, 3):
        xj = (x + j) % 4
        copy = remote(dwx.at[xj], dwxr.at[x], s_wx.at[0], r_wx.at[0], x_peer(j))
        copy.start()

    for s in (0, 1):
        home = add_share(0, s)
        arrived(fin.at[s], r_fin.at[s], "wait_home")
        home += fin[s, 0].astype(F32) + fin[s, 1].astype(F32)
        dqh[s] = (home * SCALE).astype(BF16)
        args = (s, dqh.at[s], dqf.at[e_mine], s_h.at[s], r_h.at[e_mine])
        start_to_owner(args)
        back.append(args)

    weight = dwx[x].astype(F32)
    arrived(dwxr.at[pl.ds(0, 3)], r_wx.at[0], "wait_weight")
    for j in (1, 3, 2):
        weight += dwxr[(x + j) % 4].astype(F32)
    dwz[...] = weight.astype(BF16)

    def weight_home(i):
        row_z = 2 * c + i
        own = (row_z == z) & (z // 2 == c)
        src, dst = dwz.at[i], dwf.at[z % 2]
        copy = remote(src, dst, s_wz.at[i], r_wz.at[z % 2], (4 * row_z + x, 2 * y + z // 2))
        return own, copy, pltpu.make_async_copy(src, dst, r_wz.at[z % 2])

    for i in (0, 1):
        own, copy, local = weight_home(i)

        @pl.when(own)
        def _():
            local.start()

        @pl.when(jnp.logical_not(own))
        def _():
            copy.start()

    for s in (0, 1):
        own = key_z(c, s) == z

        @pl.when(own)
        def _():
            left(gs.at[s, pl.ds(0, 7)], s_g.at[s])

        @pl.when(jnp.logical_not(own))
        def _():
            left(gs.at[s], s_g.at[s])

    left(wt.at[pl.ds(0, 7)], s_wt.at[0])
    left(xs, s_x.at[0])
    left(dwx.at[pl.ds(0, 3)], s_wx.at[0])

    for j in (1, 3, 2):
        i = 4 * c + (y + j) % 4
        arrived(ag.at[i], r_ag.at[i], "wait_chunk")
        remote(ag.at[i], ag_out.at[i], s_ag.at[0], r_ag.at[i], partner).start()
        to_hbm(i)

    for e in (0, 1):
        arrived(dwf.at[e], r_wz.at[e], "wait_weight")
        dwo[:, e * VDIM : (e + 1) * VDIM] = dwf[e].astype(F32)
    for e in (0, 1):
        arrived(dqf.at[e], r_h.at[e], "wait_queries")
    dqo[...] = jnp.concatenate([dqf[0], dqf[1]], axis=0).T
    stores = [pltpu.make_async_copy(dqo, dq_out, s_out.at[0]), pltpu.make_async_copy(dwo, dw_out, s_out.at[1])]
    for store in stores:
        store.start()
    for i in (0, 1):
        own, copy, _ = weight_home(i)

        @pl.when(jnp.logical_not(own))
        def _():
            copy.wait_send()

    for args in back:
        sent_to_owner(args)
    for j in (0, 1, 3, 2):
        i = 4 * (1 - c) + (y + j) % 4
        arrived(ag_out.at[i], r_ag.at[i], "wait_other_chunk")

    with jax.named_scope("last"):
        to_half.wait_send()
        left(ag.at[pl.ds(0, 7)], s_ag.at[0])
        for store in stores:
            store.wait()
        pltpu.make_async_copy(ag.at[pl.ds(0, 4)], ag_out.at[pl.ds(0, 4)], s_out.at[2]).wait()


def finish(ag_hbm, dq_hbm, dw_hbm, dlat_hbm, drope_hbm, dq_out, dw_out, ag, dq, dw, dlat, drope, s_in, s_out):
    loads = [pltpu.make_async_copy(ag_hbm.at[i], ag.at[i], s_in.at[i]) for i in range(8)]
    loads += [pltpu.make_async_copy(dq_hbm, dq, s_in.at[8]), pltpu.make_async_copy(dw_hbm, dw, s_in.at[9])]
    for load in loads:
        load.start()
    stores = []
    for i in range(8):
        loads[i].wait()
        rows = pl.ds(CHUNK * i, CHUNK)
        for j in range(8):
            dlat[rows, 128 * j : 128 * (j + 1)] = ag[i, CHUNK * j : CHUNK * (j + 1)].astype(F32)
        stores.append(pltpu.make_async_copy(dlat.at[rows], dlat_hbm.at[rows], s_out.at[i]))
        stores[-1].start()
    for i, src, dst in ((8, dq, dq_out), (9, dw, dw_out)):
        loads[i].wait()
        stores.append(pltpu.make_async_copy(src, dst, s_out.at[i]))
        stores[-1].start()
    ropes = []
    for i in range(8):
        pairs = ag[i, 8 * CHUNK : DONE].T.astype(F32)
        ropes += [pairs[0:ROPE], pairs[ROPE : 2 * ROPE]]
    drope[...] = jnp.concatenate(ropes, axis=1)
    stores.append(pltpu.make_async_copy(drope, drope_hbm, s_out.at[10]))
    stores[-1].start()
    for store in stores:
        store.wait()


def per_device(q, lat, rope, kw, vw, lse, ao, go):
    vmem = pl.BlockSpec(memory_space=pltpu.VMEM)
    anywhere = pl.BlockSpec(memory_space=pl.ANY)

    def buf(*shape, dtype=BF16):
        return pltpu.VMEM(shape, dtype)

    def sem(*shape):
        return pltpu.SemaphoreType.DMA(shape)

    scratch = [
        buf(ROWS, 2 * HEAD), buf(ROWS, LATENT), buf(ROPE, ROWS), buf(LATENT, 256), buf(LATENT, 256),
        buf(2, ROWS, dtype=F32), buf(ROWS, 256), buf(ROWS, 256),
        buf(16, PACK, ROWS), buf(2, PACK, ROWS), buf(2, HEAD, ROWS), buf(2, VDIM, ROWS),
        buf(2, KEY_PACK, ROWS), buf(2, ROWS, GRAD_AT), buf(2, ROWS, KEY_PACK - GRAD_AT),
        buf(2, ROWS, HEAD, dtype=F32), buf(2, ROWS, VDIM, dtype=F32), buf(16, HEAD, ROWS, dtype=F32),
        buf(8, HEAD, ROWS), buf(8, HEAD, ROWS), buf(6, HEAD, ROWS), buf(2, HEAD, ROWS), buf(2, 2, HEAD, ROWS),
        buf(2, HEAD, ROWS), buf(2, HEAD, ROWS), buf(2, 8, PIECE, 128), buf(16, PIECE, 128),
        buf(2, ROWS, LATENT), buf(8, 2, 256, LATENT),
        buf(2, 512, VDIM), buf(512, VDIM), buf(4, 2, 64, VDIM), buf(4, 2, 64, VDIM), buf(2, 64, VDIM), buf(2, 64, VDIM),
        buf(8, DONE, 128), buf(ROWS, 2 * HEAD), buf(64, 256, dtype=F32),
        sem(8), sem(2, 2), sem(2), sem(2), sem(16, 2), sem(2), sem(2), sem(3), sem(1), sem(8), sem(1), sem(2),
        sem(2), sem(2), sem(2), sem(2), sem(4),
        sem(2), sem(2), sem(1), sem(4), sem(1), sem(8), sem(1), sem(1), sem(1), sem(1), sem(2), sem(2), sem(3),
    ]
    ag, dq, dw = pl.pallas_call(
        kernel,
        in_specs=[anywhere] * 8,
        out_specs=[anywhere] * 3,
        out_shape=[
            jax.ShapeDtypeStruct((8, DONE, 128), BF16),
            jax.ShapeDtypeStruct((ROWS, 2 * HEAD), BF16),
            jax.ShapeDtypeStruct((64, 256), F32),
        ],
        scratch_shapes=scratch,
        compiler_params=pltpu.CompilerParams(
            collective_id=0, has_side_effects=True, vmem_limit_bytes=58000 * 1024
        ),
        name="latent_attention_backward",
    )(q, lat, rope.T, kw, vw, lse, ao, go)
    dlat, drope, dq, dw = pl.pallas_call(
        finish,
        in_specs=[anywhere] * 3,
        out_specs=[anywhere] * 4,
        out_shape=[
            jax.ShapeDtypeStruct((ROWS, LATENT), F32),
            jax.ShapeDtypeStruct((ROPE, ROWS), F32),
            jax.ShapeDtypeStruct((ROWS, 2 * HEAD), BF16),
            jax.ShapeDtypeStruct((64, 256), F32),
        ],
        scratch_shapes=[
            buf(8, DONE, 128), buf(ROWS, 2 * HEAD), buf(64, 256, dtype=F32),
            buf(ROWS, LATENT, dtype=F32), buf(ROPE, ROWS, dtype=F32), sem(10), sem(11),
        ],
        compiler_params=pltpu.CompilerParams(vmem_limit_bytes=58000 * 1024),
        name="finish",
    )(ag, dq, dw)
    return dq, dlat, drope.T, dw


def solution(mesh):
    placed = (
        P("sp", "tp"),
        P("sp", None),
        P("sp", None),
        P(None, "tp"),
        P(None, "tp"),
        P("tp", "sp"),
        P("sp", "tp"),
        P("sp", "tp"),
    )
    return jax.shard_map(
        per_device,
        mesh=mesh,
        in_specs=placed,
        out_specs=(P("sp", "tp"), P("sp", None), P("sp", None), P("sp", "tp")),
        check_vma=False,
    )
```

```python
import jax
import jax.numpy as jnp
from jax import lax
from jax.experimental import pallas as pl
from jax.experimental.pallas import tpu as pltpu
from jax.sharding import PartitionSpec as P

NOPE = 128
ROPE = 64
HEAD = NOPE + ROPE
VDIM = 128
ROWS = 512
LATENT = 1024
CHUNK = 64
PIECE = 160
DONE = 544
HALF = 256
SCALE = HEAD**-0.5
LOG2E = 1.4426950408889634
BF16 = jnp.bfloat16
F32 = jnp.float32
MESH = pl.DeviceIdType.MESH
NT = (((1,), (1,)), ((), ()))

LSE_AT, GRAD_AT, PACK = 192, 208, 336
ONES_AT, VALUE_AT, KEY_PACK = 192, 224, 352


def dot(a, b):
    return jnp.dot(a, b, preferred_element_type=F32)


def dot_nt(a, b):
    return lax.dot_general(a, b, NT, preferred_element_type=F32)


def in_three(row):
    high = row.astype(BF16).astype(F32)
    middle = (row - high).astype(BF16).astype(F32)
    return high, middle, row - high - middle


def six_rows(first, second):
    at = lax.broadcasted_iota(jnp.int32, (16, first.shape[1]), 0)
    rows = jnp.zeros(at.shape, F32)
    for i, part in enumerate(in_three(first) + in_three(second)):
        rows = jnp.where(at == i, part, rows)
    return rows.astype(BF16)


def ones_rows(first):
    at = lax.broadcasted_iota(jnp.int32, (16, ROWS), 0)
    return jnp.where((at >= first) & (at < first + 3), 1.0, 0.0).astype(BF16)


def kernel(
    q_hbm, lat_hbm, rope_hbm, kw_hbm, vw_hbm, lse_hbm, ao_hbm, go_hbm,
    ag_out, dq_out, dw_out,
    q, lat, rope, kw, vw, lse, ao, go,
    qb, pk, kts, vts, kv, kaug, vaug, dk, dv, dq,
    dqs, dqr, xs, rel, fin, dqh, dqf, gs, gf, lt, wt,
    dwh, dwhr, dwx, dwxr, dwz, dwf, ag, dqo, dwo,
    s_in, s_pk, s_kt, s_v, r_q, r_kt, r_v, s_fw, s_d, r_d, s_x, r_rel, r_fin, s_h, r_h, s_g, r_g,
    s_lt, r_lt, s_wt, r_wt, s_ag, r_ag, s_wh, r_wh, s_wx, r_wx, s_wz, r_wz, s_out,
):
    sp, tp = lax.axis_index("sp"), lax.axis_index("tp")
    z, x, y, c = sp // 4, sp % 4, tp // 2, tp % 2
    core_of_z = ((z + 1) // 2) % 2
    slot_of_z = z // 2
    partner = (sp, 2 * y + 1 - c)

    def key_z(core, slot):
        return core + slot * (3 - 2 * core)

    def x_peer(j):
        return (4 * z + (x + j) % 4, tp)

    def z_peer(j):
        return (4 * ((z + j) % 4) + x, tp)

    def y_peer(j):
        return (sp, 2 * ((y + j) % 4) + c)

    def remote(src, dst, send, recv, to):
        return pltpu.make_async_remote_copy(
            src_ref=src, dst_ref=dst, send_sem=send, recv_sem=recv, device_id=to, device_id_type=MESH
        )

    def arrived(ref, recv, name="wait"):
        with jax.named_scope(name):
            remote(ref, ref, s_in.at[0], recv, partner).wait_recv()

    def left(ref, send):
        remote(ref, ref, send, s_in.at[0], partner).wait_send()

    barrier = pltpu.get_barrier_semaphore()
    peers = [partner]
    for j in (1, 2, 3):
        peers += [x_peer(j)]
        peers += [(sp, 2 * ((y + j) % 4) + core) for core in (0, 1)]
        peers += [(4 * ((z + j) % 4) + x, 2 * y + core) for core in (0, 1)]
    for peer in peers:
        pl.semaphore_signal(barrier, inc=1, device_id=peer, device_id_type=MESH)

    def load(i):
        pairs = ((q_hbm, q), (go_hbm, go), (ao_hbm, ao), (lse_hbm, lse), (lat_hbm, lat), (kw_hbm, kw), (rope_hbm, rope), (vw_hbm, vw))
        return pltpu.make_async_copy(*pairs[i], s_in.at[i])

    @pl.when(z < 2)
    def _():
        for i in (4, 5, 6, 7, 0, 1, 2, 3):
            load(i).start()

    @pl.when(z >= 2)
    def _():
        for i in range(8):
            load(i).start()

    dk[...] = jnp.zeros_like(dk)
    dv[...] = jnp.zeros_like(dv)
    for s in (0, 1):
        kv[s, ONES_AT : ONES_AT + 16] = ones_rows(0)
        kv[s, ONES_AT + 16 : VALUE_AT] = ones_rows(3)

    def to_head(e, src, dst, send, recv):
        head_z = 2 * c + e
        own = (head_z == z) & (core_of_z == c)
        copy = remote(src, dst, send, recv, (4 * head_z + x, 2 * y + core_of_z))
        return own, copy, pltpu.make_async_copy(src, dst, recv)

    def start_to_head(args):
        own, copy, local = to_head(*args)

        @pl.when(own)
        def _():
            local.start()

        @pl.when(jnp.logical_not(own))
        def _():
            copy.start()

    def sent_to_head(args):
        own, copy, _ = to_head(*args)

        @pl.when(jnp.logical_not(own))
        def _():
            copy.wait_send()

    def half(ref, b, h):
        return ref.at[b, :, pl.ds(HALF * h, HALF)]

    pack_args = [
        (e, half(pk, e, h), half(qb, sp, h), s_pk.at[e, h], r_q.at[sp, h]) for h in (0, 1) for e in (0, 1)
    ]
    key_args = [
        (e, kts.at[e], kv.at[slot_of_z, pl.ds(0, HEAD)], s_kt.at[e], r_kt.at[slot_of_z]) for e in (0, 1)
    ]
    value_args = [
        (e, vts.at[e], kv.at[slot_of_z, pl.ds(VALUE_AT, VDIM)], s_v.at[e], r_v.at[slot_of_z]) for e in (0, 1)
    ]

    latent_args = [(e, lat, lt.at[slot_of_z], s_lt.at[e], r_lt.at[slot_of_z]) for e in (0, 1)]

    def pack_queries():
        for i in range(4):
            load(i).wait()
        qt = q[...].T
        got = go[...].T
        aot = ao[...].T
        for e in (0, 1):
            grad = got[e * VDIM : (e + 1) * VDIM]
            delta = jnp.sum(
                grad.astype(F32) * aot[e * VDIM : (e + 1) * VDIM].astype(F32), axis=0, keepdims=True
            )
            pk[e, 0:LSE_AT] = qt[e * HEAD : (e + 1) * HEAD]
            pk[e, LSE_AT:GRAD_AT] = six_rows(lse[e : e + 1, :] * (-1.0 / SCALE), -delta)
            pk[e, GRAD_AT:PACK] = grad

    def pack_keys():
        for i in range(4, 8):
            load(i).wait()
        keys = dot(lat[...], kw[...]).astype(BF16).T
        for e in (0, 1):
            kts[e, 0:NOPE] = keys[e * NOPE : (e + 1) * NOPE]
            kts[e, NOPE:HEAD] = rope[...]
        values = dot(lat[...], vw[...]).astype(BF16).T
        for e in (0, 1):
            vts[e] = values[e * VDIM : (e + 1) * VDIM]

    def send_queries():
        for args in pack_args:
            start_to_head(args)

    def send_keys():
        for args in key_args + value_args:
            start_to_head(args)

    def weight_copy(kind, dy, p):
        at = 2 * ((y + dy) % 4) + c
        to = (y_peer(1), y_peer(3), partner)[kind]
        return remote(wt.at[at, p], wt.at[at, p], s_wt.at[0], r_wt.at[3 if kind == 2 else 2 if dy else p], to)

    def send_weight(*args):
        copy = weight_copy(*args)
        copy.start()

    def take_weights(p):
        arrived(wt.at[0], r_wt.at[p], "wait_weights")
        for dy in (1, 3):
            send_weight(2, dy, p)
        send_weight(p, 3 - 2 * p, p)

    def send_own_weights(p):
        wt[tp, p] = (kw, vw)[p][...].T
        for kind in (0, 1, 2):
            send_weight(kind, 0, p)

    @pl.when(z < 2)
    def _():
        pack_keys()

    @pl.when(z >= 2)
    def _():
        pack_queries()

    with jax.named_scope("barrier"):
        pl.semaphore_wait(barrier, len(peers))

    @pl.when(z < 2)
    def _():
        send_keys()
        send_own_weights(0)
        pack_queries()
        send_queries()

    @pl.when(z >= 2)
    def _():
        send_queries()
        pack_keys()
        send_own_weights(0)
        send_own_weights(1)
        send_keys()

    @pl.when(z < 2)
    def _():
        send_own_weights(1)

    for args in latent_args:
        start_to_head(args)

    def zero(b, _):
        dq[b] = jnp.zeros((HEAD, ROWS), F32)
        return 0

    lax.fori_loop(0, 16, zero, 0)

    def step(t):
        near = t < 4
        far = t >= 12
        mid = jnp.logical_not(near | far)
        pair = t % 2
        slot = 1 - jnp.where(mid, (t - 4) // 4, (t % 4) // 2)
        other = jnp.where(mid, ((t - 4) // 2) % 2, pair)
        dx = jnp.where(near, 0, jnp.where(far, 2, jnp.where(pair == 0, 3, 1)))
        core = jnp.where(other == 0, c, 1 - c)
        block = 4 * key_z(core, slot) + (x + dx) % 4
        return block, dx, other, slot

    def forwards(t, h):
        b, dx, other, slot = step(t)
        block = half(qb, b, h)
        mine = other == 0
        plus = mine & ((dx == 0) | ((dx == 3) & (slot == 0)))
        minus = mine & ((dx == 0) | ((dx == 1) & (slot == 1)))
        return [
            (plus, remote(block, block, s_fw.at[0], r_q.at[b, h], x_peer(1))),
            (minus, remote(block, block, s_fw.at[1], r_q.at[b, h], x_peer(3))),
            (mine, remote(block, block, s_fw.at[2], r_q.at[b, h], partner)),
        ]

    def take(t):
        b = step(t)[0]
        for h in (0, 1):
            arrived(half(qb, b, h), r_q.at[b, h], "wait_query")
            for holds, copy in forwards(t, h):

                @pl.when(holds)
                def _():
                    copy.start()

    def tile(b, s, masked):
        raw = dot(kaug[s], qb[b, 0:GRAD_AT]) * (SCALE * LOG2E)
        if masked:
            key_row = lax.broadcasted_iota(jnp.int32, (ROWS, ROWS), 0)
            query_row = lax.broadcasted_iota(jnp.int32, (ROWS, ROWS), 1)
            raw = jnp.where(key_row <= query_row, raw, -1e30)
        probs = jnp.exp2(raw)
        diff = dot(vaug[s], qb[b, LSE_AT:PACK])
        grads = (probs * diff).astype(BF16)
        dv[s] += dot_nt(probs.astype(BF16), qb[b, GRAD_AT:PACK])
        dk[s] += dot_nt(grads, qb[b, 0:LSE_AT])
        dq[b] += dot(kv[s, 0:HEAD], grads)

    def to_partner(i):
        return remote(dqs.at[i], dqr.at[i], s_d.at[0], r_d.at[i], partner)

    def share(t):
        b, dx, other, slot = step(t)

        i = 2 * dx + slot
        dqs[i] = dq[b].astype(BF16)
        to_partner(i).start()

    def own_block(s):
        return 4 * key_z(c, s) + x

    def take_keys(s):
        arrived(kv.at[s, pl.ds(0, HEAD)], r_kt.at[s], "wait_keys")
        arrived(kv.at[s, pl.ds(VALUE_AT, VDIM)], r_v.at[s], "wait_values")
        kaug[s] = kv[s, 0:GRAD_AT].T
        vaug[s] = kv[s, GRAD_AT:KEY_PACK].T

    def both_tiles(b):
        probs = [jnp.exp2(dot(kaug[s], qb[b, 0:GRAD_AT]) * (SCALE * LOG2E)) for s in (0, 1)]
        grads = [(probs[s] * dot(vaug[s], qb[b, LSE_AT:PACK])).astype(BF16) for s in (0, 1)]
        for s in (0, 1):
            dv[s] += dot_nt(probs[s].astype(BF16), qb[b, GRAD_AT:PACK])
            dk[s] += dot_nt(grads[s], qb[b, 0:LSE_AT])
        dq[b] += dot(kv[0, 0:HEAD], grads[0]) + dot(kv[1, 0:HEAD], grads[1])

    def tiles(b):
        with jax.named_scope("pair"):

            @pl.when(b > own_block(1))
            def _():
                both_tiles(b)

            @pl.when((b > own_block(0)) & (b < own_block(1)))
            def _():
                tile(b, 0, False)

    def early(t, _):
        @pl.when(t > 0)
        def _():
            take(t)

        with jax.named_scope("early"):
            tile(step(t)[0], 0, False)
        return 0

    def later(p, _):
        far = p >= 6
        even = jnp.logical_not(far) & (p % 2 == 0)
        odd = jnp.logical_not(far) & (p % 2 == 1)
        slot = step(2 * p)[3]

        @pl.when(even)
        def _():
            for h in (0, 1):
                for i, back_slot in ((0, 0), (1, 1)):
                    b = step(2 * p + i)[0]
                    block = half(qb, b, h)
                    arrived(block, r_q.at[b, h], "wait_query")

                    @pl.when(slot == back_slot)
                    def _():
                        remote(block, block, s_fw.at[i], r_q.at[b, h], x_peer(1 + 2 * i)).start()

                    remote(block, block, s_fw.at[2], r_q.at[b, h], partner).start()

        @pl.when(odd)
        def _():
            for i in (0, 1):
                b = step(2 * p + i)[0]
                for h in (0, 1):
                    arrived(half(qb, b, h), r_q.at[b, h], "wait_query")

        @pl.when(far)
        def _():
            b = step(2 * p)[0]
            for h in (0, 1):
                block = half(qb, b, h)
                arrived(block, r_q.at[b, h], "wait_query")
                remote(block, block, s_fw.at[2], r_q.at[b, h], partner).start()

        @pl.when(p == 2)
        def _():
            take_weights(0)

        @pl.when(p == 4)
        def _():
            take_weights(1)

        def member(i, _):
            b = step(2 * p + i)[0]

            @pl.when(far & (i == 1))
            def _():
                for h in (0, 1):
                    arrived(half(qb, b, h), r_q.at[b, h], "wait_query")

            tiles(b)
            return 0

        lax.fori_loop(0, 2, member, 0)

        @pl.when(odd)
        def _():
            share(2 * p)

        @pl.when(odd | far)
        def _():
            share(2 * p + 1)

        return 0

    def own_tiles(s, _):
        @pl.when(s == 1)
        def _():
            take_keys(1)

        with jax.named_scope("diagonal"):
            tile(own_block(s), s, True)

        @pl.when(s == 0)
        def _():
            take(3)

        b = step(3 - 2 * s)[0]

        @pl.when(b > own_block(s))
        def _():
            tile(b, s, False)

        return 0

    def piece(s, j):
        i = (4 * c + y + j) % 8
        token_z = key_z(c, s)
        to = (4 * token_z + x, 2 * (i % 4) + i // 4)
        src, dst = gs.at[s, i], gf.at[4 * y + z]
        return (
            (token_z == z) if j == 0 else None,
            remote(src, dst, s_g.at[s], r_g.at[y], to),
            pltpu.make_async_copy(src, dst, r_g.at[y]),
        )

    def by_piece(s, j, local_op, remote_op):
        own, copy, local = piece(s, j)
        if own is None:
            remote_op(copy)
            return

        @pl.when(own)
        def _():
            local_op(local)

        @pl.when(jnp.logical_not(own))
        def _():
            remote_op(copy)

    def send_grads(s):
        gs[s, :, 0:CHUNK] = (dk[s, :, 0:NOPE] * SCALE).astype(BF16).reshape(8, CHUNK, NOPE)
        gs[s, :, CHUNK : 2 * CHUNK] = dv[s].astype(BF16).reshape(8, CHUNK, VDIM)
        ropes = (dk[s, :, NOPE:HEAD] * SCALE).astype(BF16).reshape(8, 2, 32, ROPE)
        gs[s, :, 2 * CHUNK : PIECE] = jnp.concatenate([ropes[:, 0], ropes[:, 1]], axis=2)
        for j in range(8):
            by_piece(s, j, lambda local: local.start(), lambda copy: copy.start())

    def to_owner(s, src, dst, send, recv):
        token_z = key_z(c, s)
        own = (token_z == z) & (z // 2 == c)
        copy = remote(src, dst, send, recv, (4 * token_z + x, 2 * y + z // 2))
        return own, copy, pltpu.make_async_copy(src, dst, recv)

    def start_to_owner(args):
        own, copy, local = to_owner(*args)

        @pl.when(own)
        def _():
            local.start()

        @pl.when(jnp.logical_not(own))
        def _():
            copy.start()

    def sent_to_owner(args):
        own, copy, _ = to_owner(*args)

        @pl.when(jnp.logical_not(own))
        def _():
            copy.wait_send()

    e_mine = z % 2
    back = []

    def add_share(dx, s):
        i = 2 * dx + s
        arrived(dqr.at[i], r_d.at[i], "wait_share")
        b = 4 * key_z(c, s) + (x + dx) % 4
        return dq[b] + dqr[i].astype(F32)

    def send_x(i, value, dst, recv, to):
        xs[i] = value.astype(BF16)
        copy = remote(xs.at[i], dst, s_x.at[0], recv, to)
        copy.start()

    def to_hbm(i):
        pltpu.make_async_copy(ag.at[i], ag_out.at[i], s_out.at[2]).start()

    take(0)
    take_keys(0)
    lax.fori_loop(0, 2, early, 0)
    take(2)
    lax.fori_loop(0, 2, own_tiles, 0)
    share(1)
    share(3)
    lax.fori_loop(2, 7, later, 0)

    send_grads(1)
    send_x(1, add_share(2, 1), rel.at[1], r_rel.at[1], x_peer(1))
    send_x(2, add_share(3, 1), fin.at[1, 1], r_fin.at[1], x_peer(3))
    send_x(3, add_share(1, 0), fin.at[0, 0], r_fin.at[0], x_peer(1))
    lax.fori_loop(7, 8, later, 0)
    send_grads(0)
    send_x(0, add_share(2, 0), rel.at[0], r_rel.at[0], x_peer(3))

    arrived(wt.at[0], r_wt.at[2], "wait_weights")
    for p in (0, 1):
        send_weight(2, 2, p)

    for args in pack_args + key_args + value_args + latent_args:
        sent_to_head(args)

    left(qb.at[pl.ds(0, 3)], s_fw.at[0])
    left(qb.at[pl.ds(0, 3)], s_fw.at[1])
    left(qb.at[pl.ds(0, 8)], s_fw.at[2])
    left(dqs, s_d.at[0])

    def relay_plus():
        value = add_share(1, 1)
        arrived(rel.at[1], r_rel.at[1], "wait_relay")
        send_x(5, value + rel[1].astype(F32), fin.at[1, 0], r_fin.at[1], x_peer(1))

    def relay_minus():
        value = add_share(3, 0)
        arrived(rel.at[0], r_rel.at[0], "wait_relay")
        send_x(4, value + rel[0].astype(F32), fin.at[0, 1], r_fin.at[0], x_peer(3))

    relay_plus()
    relay_minus()

    arrived(wt.at[pl.ds(0, 4)], r_wt.at[3], "wait_weights")
    latent = jnp.zeros((CHUNK, LATENT), F32)
    ropes = jnp.zeros((32, 2 * ROPE), F32)
    for j in (0, 1, 3, 2):
        yj = (y + j) % 4
        arrived(gf.at[pl.ds(4 * yj, 4)], r_g.at[yj], "wait_grads")
        for u in range(4):
            ropes += gf[4 * yj + u, 2 * CHUNK : PIECE].astype(F32)
        for core in (0, 1):
            first, second = 4 * yj + 2 * core, 4 * yj + 2 * core + 1
            for p in (0, 1):
                rows = slice(p * CHUNK, (p + 1) * CHUNK)
                grads = jnp.concatenate([gf[first, rows], gf[second, rows]], axis=1)
                latent += dot(grads, wt[2 * yj + core, p])
    mine = 4 * c + y
    for i in range(8):
        ag[mine, CHUNK * i : CHUNK * (i + 1)] = latent[:, 128 * i : 128 * (i + 1)].astype(BF16)
    ag[mine, 8 * CHUNK : DONE] = ropes.astype(BF16)
    for j in (2, 1, 3):
        remote(ag.at[mine], ag.at[mine], s_ag.at[0], r_ag.at[mine], y_peer(j)).start()
    remote(ag.at[mine], ag_out.at[mine], s_ag.at[0], r_ag.at[mine], partner).start()
    to_hbm(mine)

    for s in (0, 1):
        arrived(lt.at[s], r_lt.at[s], "wait_latent")
    weight = dot(gs[0, :, CHUNK : 2 * CHUNK].reshape(ROWS, VDIM).T, lt[0])
    weight += dot(gs[1, :, CHUNK : 2 * CHUNK].reshape(ROWS, VDIM).T, lt[1])
    for core in (0, 1):
        dwh[core] = weight[:, 512 * core : 512 * (core + 1)].astype(BF16).T
    to_half = remote(dwh.at[1 - c], dwhr, s_wh.at[0], r_wh.at[0], partner)
    to_half.start()

    arrived(dwhr, r_wh.at[0], "wait_weight")
    weight = (dwh[c].astype(F32) + dwhr[...].astype(F32)).astype(BF16)
    for i in range(8):
        dwx[i % 4, i // 4] = weight[64 * i : 64 * (i + 1)]
    for j in (2, 1, 3):
        xj = (x + j) % 4
        copy = remote(dwx.at[xj], dwxr.at[x], s_wx.at[0], r_wx.at[0], x_peer(j))
        copy.start()

    for s in (0, 1):
        home = add_share(0, s)
        arrived(fin.at[s], r_fin.at[s], "wait_home")
        home += fin[s, 0].astype(F32) + fin[s, 1].astype(F32)
        dqh[s] = (home * SCALE).astype(BF16)
        args = (s, dqh.at[s], dqf.at[e_mine], s_h.at[s], r_h.at[e_mine])
        start_to_owner(args)
        back.append(args)

    weight = dwx[x].astype(F32)
    arrived(dwxr.at[pl.ds(0, 3)], r_wx.at[0], "wait_weight")
    for j in (1, 3, 2):
        weight += dwxr[(x + j) % 4].astype(F32)
    dwz[...] = weight.astype(BF16)

    def weight_home(i):
        row_z = 2 * c + i
        own = (row_z == z) & (z // 2 == c)
        src, dst = dwz.at[i], dwf.at[z % 2]
        copy = remote(src, dst, s_wz.at[i], r_wz.at[z % 2], (4 * row_z + x, 2 * y + z // 2))
        return own, copy, pltpu.make_async_copy(src, dst, r_wz.at[z % 2])

    for i in (0, 1):
        own, copy, local = weight_home(i)

        @pl.when(own)
        def _():
            local.start()

        @pl.when(jnp.logical_not(own))
        def _():
            copy.start()

    for s in (0, 1):
        own = key_z(c, s) == z

        @pl.when(own)
        def _():
            left(gs.at[s, pl.ds(0, 7)], s_g.at[s])

        @pl.when(jnp.logical_not(own))
        def _():
            left(gs.at[s], s_g.at[s])

    left(wt.at[pl.ds(0, 7)], s_wt.at[0])
    left(xs, s_x.at[0])
    left(dwx.at[pl.ds(0, 3)], s_wx.at[0])

    for j in (1, 3, 2):
        i = 4 * c + (y + j) % 4
        arrived(ag.at[i], r_ag.at[i], "wait_chunk")
        remote(ag.at[i], ag_out.at[i], s_ag.at[0], r_ag.at[i], partner).start()
        to_hbm(i)

    for e in (0, 1):
        arrived(dwf.at[e], r_wz.at[e], "wait_weight")
        dwo[:, e * VDIM : (e + 1) * VDIM] = dwf[e].astype(F32)
    for e in (0, 1):
        arrived(dqf.at[e], r_h.at[e], "wait_queries")
    dqo[...] = jnp.concatenate([dqf[0], dqf[1]], axis=0).T
    stores = [pltpu.make_async_copy(dqo, dq_out, s_out.at[0]), pltpu.make_async_copy(dwo, dw_out, s_out.at[1])]
    for store in stores:
        store.start()
    for i in (0, 1):
        own, copy, _ = weight_home(i)

        @pl.when(jnp.logical_not(own))
        def _():
            copy.wait_send()

    for args in back:
        sent_to_owner(args)
    for j in (0, 1, 3, 2):
        i = 4 * (1 - c) + (y + j) % 4
        arrived(ag_out.at[i], r_ag.at[i], "wait_other_chunk")

    with jax.named_scope("last"):
        to_half.wait_send()
        left(ag.at[pl.ds(0, 7)], s_ag.at[0])
        for store in stores:
            store.wait()
        pltpu.make_async_copy(ag.at[pl.ds(0, 4)], ag_out.at[pl.ds(0, 4)], s_out.at[2]).wait()


def finish(ag_hbm, dq_hbm, dw_hbm, dlat_hbm, drope_hbm, dq_out, dw_out, ag, dq, dw, dlat, drope, s_in, s_out):
    pairs_of = [pl.ds(2 * i, 2) for i in range(4)]
    loads = [pltpu.make_async_copy(ag_hbm.at[two], ag.at[two], s_in.at[i]) for i, two in enumerate(pairs_of)]
    loads += [pltpu.make_async_copy(dq_hbm, dq, s_in.at[4]), pltpu.make_async_copy(dw_hbm, dw, s_in.at[5])]
    for load in loads:
        load.start()
    stores = []
    for i in range(8):
        if i % 2 == 0:
            loads[i // 2].wait()
        rows = pl.ds(CHUNK * i, CHUNK)
        for j in range(8):
            dlat[rows, 128 * j : 128 * (j + 1)] = ag[i, CHUNK * j : CHUNK * (j + 1)].astype(F32)
        pltpu.make_async_copy(dlat.at[rows], dlat_hbm.at[rows], s_out.at[0]).start()
    stores.append(pltpu.make_async_copy(dlat, dlat_hbm, s_out.at[0]))
    for i, src, dst in ((1, dq, dq_out), (2, dw, dw_out)):
        loads[3 + i].wait()
        stores.append(pltpu.make_async_copy(src, dst, s_out.at[i]))
        stores[-1].start()
    ropes = []
    for i in range(8):
        pairs = ag[i, 8 * CHUNK : DONE].T.astype(F32)
        ropes += [pairs[0:ROPE], pairs[ROPE : 2 * ROPE]]
    drope[...] = jnp.concatenate(ropes, axis=1)
    stores.append(pltpu.make_async_copy(drope, drope_hbm, s_out.at[3]))
    stores[-1].start()
    for store in stores:
        store.wait()


def per_device(q, lat, rope, kw, vw, lse, ao, go):
    vmem = pl.BlockSpec(memory_space=pltpu.VMEM)
    anywhere = pl.BlockSpec(memory_space=pl.ANY)

    def buf(*shape, dtype=BF16):
        return pltpu.VMEM(shape, dtype)

    def sem(*shape):
        return pltpu.SemaphoreType.DMA(shape)

    scratch = [
        buf(ROWS, 2 * HEAD), buf(ROWS, LATENT), buf(ROPE, ROWS), buf(LATENT, 256), buf(LATENT, 256),
        buf(2, ROWS, dtype=F32), buf(ROWS, 256), buf(ROWS, 256),
        buf(16, PACK, ROWS), buf(2, PACK, ROWS), buf(2, HEAD, ROWS), buf(2, VDIM, ROWS),
        buf(2, KEY_PACK, ROWS), buf(2, ROWS, GRAD_AT), buf(2, ROWS, KEY_PACK - GRAD_AT),
        buf(2, ROWS, HEAD, dtype=F32), buf(2, ROWS, VDIM, dtype=F32), buf(16, HEAD, ROWS, dtype=F32),
        buf(8, HEAD, ROWS), buf(8, HEAD, ROWS), buf(6, HEAD, ROWS), buf(2, HEAD, ROWS), buf(2, 2, HEAD, ROWS),
        buf(2, HEAD, ROWS), buf(2, HEAD, ROWS), buf(2, 8, PIECE, 128), buf(16, PIECE, 128),
        buf(2, ROWS, LATENT), buf(8, 2, 256, LATENT),
        buf(2, 512, VDIM), buf(512, VDIM), buf(4, 2, 64, VDIM), buf(4, 2, 64, VDIM), buf(2, 64, VDIM), buf(2, 64, VDIM),
        buf(8, DONE, 128), buf(ROWS, 2 * HEAD), buf(64, 256, dtype=F32),
        sem(8), sem(2, 2), sem(2), sem(2), sem(16, 2), sem(2), sem(2), sem(3), sem(1), sem(8), sem(1), sem(2),
        sem(2), sem(2), sem(2), sem(2), sem(4),
        sem(2), sem(2), sem(1), sem(4), sem(1), sem(8), sem(1), sem(1), sem(1), sem(1), sem(2), sem(2), sem(3),
    ]
    ag, dq, dw = pl.pallas_call(
        kernel,
        in_specs=[anywhere] * 8,
        out_specs=[anywhere] * 3,
        out_shape=[
            jax.ShapeDtypeStruct((8, DONE, 128), BF16),
            jax.ShapeDtypeStruct((ROWS, 2 * HEAD), BF16),
            jax.ShapeDtypeStruct((64, 256), F32),
        ],
        scratch_shapes=scratch,
        compiler_params=pltpu.CompilerParams(
            collective_id=0, has_side_effects=True, vmem_limit_bytes=58000 * 1024
        ),
        name="latent_attention_backward",
    )(q, lat, rope.T, kw, vw, lse, ao, go)
    dlat, drope, dq, dw = pl.pallas_call(
        finish,
        in_specs=[anywhere] * 3,
        out_specs=[anywhere] * 4,
        out_shape=[
            jax.ShapeDtypeStruct((ROWS, LATENT), F32),
            jax.ShapeDtypeStruct((ROPE, ROWS), F32),
            jax.ShapeDtypeStruct((ROWS, 2 * HEAD), BF16),
            jax.ShapeDtypeStruct((64, 256), F32),
        ],
        scratch_shapes=[
            buf(8, DONE, 128), buf(ROWS, 2 * HEAD), buf(64, 256, dtype=F32),
            buf(ROWS, LATENT, dtype=F32), buf(ROPE, ROWS, dtype=F32), sem(6), sem(4),
        ],
        compiler_params=pltpu.CompilerParams(vmem_limit_bytes=58000 * 1024),
        name="finish",
    )(ag, dq, dw)
    return dq, dlat, drope.T, dw


def solution(mesh):
    placed = (
        P("sp", "tp"),
        P("sp", None),
        P("sp", None),
        P(None, "tp"),
        P(None, "tp"),
        P("tp", "sp"),
        P("sp", "tp"),
        P("sp", "tp"),
    )
    return jax.shard_map(
        per_device,
        mesh=mesh,
        in_specs=placed,
        out_specs=(P("sp", "tp"), P("sp", None), P("sp", None), P("sp", "tp")),
        check_vma=False,
    )
```
